512 devices in a mesh: sp: 64 (over z, y), fs: 4 (over x), tp: 2 (over core).
Axes of the slice: x: 4, y: 8, z: 8, core: 2. Of those that a mesh axis runs over, the one named last changes fastest.
Arguments:
- tokens: bfloat16 [32768, 2048], P(('fs', 'sp')), parts along dimension 0, may hold values from -6 to 6
- norm_gain: bfloat16 [2048], replicated, may hold values from 0.099609375 to 1.8984375
- query_down: bfloat16 [2048, 512], P('sp'), may hold values from -0.125 to 0.125
- query_gain: bfloat16 [512], replicated, may hold values from 0.099609375 to 1.8984375
- latent_down: bfloat16 [2048, 256], replicated, may hold values from -0.125 to 0.125
- latent_gain: bfloat16 [256], replicated, may hold values from 0.099609375 to 1.8984375
- rope_down: bfloat16 [2048, 64], replicated, may hold values from -30 to 30
- query_up: bfloat16 [512, 1536], P(None, 'tp'), may hold values from -0.25 to 0.25
- key_up: bfloat16 [256, 1024], P(None, 'tp'), may hold values from -0.75 to 0.75
- value_up: bfloat16 [256, 1024], P(None, 'tp'), may hold values from -0.375 to 0.375
- glu_value: bfloat16 [2048, 1024], P('sp', 'tp'), may hold values from -0.125 to 0.125
- glu_gate: bfloat16 [2048, 1024], P('sp', 'tp'), may hold values from -0.125 to 0.125
- conv_taps: bfloat16 [31, 1024], P(None, 'tp'), may hold values from -1 to 1
- group_gain: bfloat16 [1024], P('tp'), may hold values from 0.099609375 to 1.8984375
- head_proj: bfloat16 [1024, 2048], P('tp', 'sp'), may hold values from -0.75 to 0.75
- channel_proj: bfloat16 [1024, 2048], P('tp', 'sp'), may hold values from -0.1875 to 0.1875
Outputs:
- mixed_out: bfloat16 [32768, 2048], P(('fs', 'sp'), 'tp'), parts along dimension 0
- log_weight: float32 [8, 32768], P('tp', ('fs', 'sp')), parts along dimension 1
The draws below stay inside these ranges and needn't reach their ends.
There are 4 independent parts, one for each index of `fs`. The reference program is written for one: setup_inputs(seed, part) draws one part's arguments, and reference() takes and returns one part's arrays. A program takes and returns all parts, laid end to end along the dimension named above; an argument that names none is the same for every part. Nothing has to cross between parts.
All inputs are finite; a program needn't handle non-finite values.
Results may differ from the reference program's by a relative error of at most 0.015.
The reference program's roundings to bfloat16 on the way count: a program that leaves them out, or rounds other values in their place, can miss the bound.
Values may be sent and summed in bfloat16 or wider, within the bound.
No kernel may reach another device: no remote copies, remote signals or barrier semaphores. Data moves between devices by JAX's collectives and lax.ppermute only.
A program may use at most 128 MiB of HBM per device.

```python
import jax
import jax.numpy as jnp
from jax import lax

D = 2048
HEADS = 8
NOPE = 128
ROPE = 64
VDIM = 128
QR = 512
KVR = 256
CH = 1024
GROUPS = 8
WIDTH = 31
GRID_W = 64
TOK_DEV = 128
LENGTH = 8192
N_TP = 2


def draw_rope_down(key, part):
    base_key = jax.random.fold_in(jax.random.fold_in(key, 11), 0)
    entries = jax.random.normal(base_key, (D, ROPE), jnp.float32) * D ** (-0.5)
    return jnp.clip(entries, -30.0, 30.0).astype(jnp.bfloat16)


def steps_of(key, extent, cuts, least, high):
    factor_of, own = 1.0, jax.random.fold_in(key, 6)
    for position, blocks in cuts:
        steps = jnp.exp(jax.random.uniform(jax.random.fold_in(own, position), (blocks,), jnp.float32, least / len(cuts), high / len(cuts)))
        factor_of = factor_of * jnp.repeat(steps, extent[position] // blocks).reshape([-1 if axis == position else 1 for axis in range(len(extent))])
    return factor_of


def bell_draw(stream_key, extent, width, bound, cuts=(), held_as=jnp.bfloat16):
    loudness = steps_of(stream_key, extent, cuts, -0.22, 0.18) if cuts else 1.0
    drawn = jax.random.normal(stream_key, extent, jnp.float32) * width * loudness
    return jnp.minimum(jnp.maximum(drawn, -bound), bound).astype(held_as)


def setup_inputs(seed: int = 0, part: int = 0) -> dict:
    arg_keys = jax.random.split(jax.random.key(seed), 17)
    part_splits = jax.random.split(jax.random.fold_in(arg_keys[16], part), 17)
    tokens = bell_draw(part_splits[0], (LENGTH, D), 1.0, 6.0, ((0, 64),))
    norm_gain = jnp.clip(1.0 + 0.18 * jax.random.normal(arg_keys[1], (D,), jnp.float32), 0.099609375, 1.8984375).astype(jnp.bfloat16)
    query_down = bell_draw(arg_keys[2], (D, QR), D ** -0.5, 0.125, ((0, 64),))
    query_gain = jnp.clip(1.0 + 0.18 * jax.random.normal(arg_keys[3], (QR,), jnp.float32), 0.099609375, 1.8984375).astype(jnp.bfloat16)
    latent_down = bell_draw(arg_keys[4], (D, KVR), D ** -0.5, 0.125)
    latent_gain = jnp.clip(1.0 + 0.18 * jax.random.normal(arg_keys[5], (KVR,), jnp.float32), 0.099609375, 1.8984375).astype(jnp.bfloat16)
    rope_down = draw_rope_down(jax.random.fold_in(arg_keys[16], 71), part)
    query_up = bell_draw(arg_keys[7], (QR, HEADS * (NOPE + ROPE)), QR ** -0.5, 0.25, ((1, 2),))
    key_up = bell_draw(arg_keys[8], (KVR, HEADS * NOPE), 0.125, 0.75, ((1, 2),))
    value_up = bell_draw(arg_keys[9], (KVR, HEADS * VDIM), KVR ** -0.5, 0.375, ((1, 2),))
    glu_value = bell_draw(arg_keys[10], (D, CH), D ** -0.5, 0.125, ((0, 64), (1, 2)))
    glu_gate = bell_draw(arg_keys[11], (D, CH), D ** -0.5, 0.125, ((0, 64), (1, 2)))
    conv_taps = bell_draw(arg_keys[12], (WIDTH, CH), WIDTH ** -0.5, 1.0, ((1, 2),))
    group_gain = jnp.clip(1.0 + 0.18 * jax.random.normal(arg_keys[13], (CH,), jnp.float32), 0.099609375, 1.8984375).astype(jnp.bfloat16)
    head_proj = bell_draw(arg_keys[14], (HEADS * VDIM, D), (HEADS * VDIM // 16) ** -0.5, 0.75, ((0, 2), (1, 64)))
    channel_proj = bell_draw(arg_keys[15], (CH, D), CH ** -0.5, 0.1875, ((0, 2), (1, 64)))
    return {"tokens": tokens, "norm_gain": norm_gain, "query_down": query_down, "query_gain": query_gain, "latent_down": latent_down, "latent_gain": latent_gain, "rope_down": rope_down, "query_up": query_up, "key_up": key_up, "value_up": value_up, "glu_value": glu_value, "glu_gate": glu_gate, "conv_taps": conv_taps, "group_gain": group_gain, "head_proj": head_proj, "channel_proj": channel_proj}


norm_eps = 1e-06
rope_base = 10000.0

def rounded(values):
    return lax.optimization_barrier(values.astype(jnp.bfloat16))

def rms_scale(values, scale_gain):
    inv_rms = lax.rsqrt(lax.optimization_barrier(jnp.mean(values * values, axis=-1, keepdims=True)) + norm_eps)
    return values * inv_rms * scale_gain.astype(jnp.float32)

def angles_for(positions, rope_size):
    quarter = rope_size // 4
    inverse = rope_base ** (-jnp.arange(quarter, dtype=jnp.float32) / quarter)
    grid_row = (positions // GRID_W).astype(jnp.float32)
    grid_col = (positions % GRID_W).astype(jnp.float32)
    return jnp.concatenate([grid_row[:, None] * inverse, grid_col[:, None] * inverse], axis=-1)

def rotate(values, angles):
    half_size = values.shape[-1] // 2
    front_half = values[..., :half_size]
    back_half = values[..., half_size:]
    cosine = jnp.cos(angles)
    sine_part = jnp.sin(angles)
    return jnp.concatenate([front_half * cosine - back_half * sine_part, back_half * cosine + front_half * sine_part], axis=-1)

def reference(tokens, norm_gain, query_down, query_gain, latent_down, latent_gain, rope_down, query_up, key_up, value_up, glu_value, glu_gate, conv_taps, group_gain, head_proj, channel_proj):
    normed = rounded(rms_scale(tokens.astype(jnp.float32), norm_gain))
    positions = jnp.arange(LENGTH, dtype=jnp.int32)
    angles = angles_for(positions, ROPE)
    latent_query = rounded(rms_scale(jnp.dot(normed, query_down, preferred_element_type=jnp.float32), query_gain))
    query_all = jnp.dot(latent_query, query_up, preferred_element_type=jnp.float32).reshape(LENGTH, HEADS, NOPE + ROPE)
    query_plain = rounded(query_all[:, :, :NOPE])
    query_rope = rounded(rotate(query_all[:, :, NOPE:], angles[:, None, :]))
    absorbed = rounded(jnp.einsum('thd,rhd->htr', query_plain.astype(jnp.float32), key_up.astype(jnp.float32).reshape(KVR, HEADS, NOPE)))
    queries = jnp.concatenate([absorbed, jnp.transpose(query_rope, (1, 0, 2))], axis=-1).astype(jnp.float32)
    latent = rounded(rms_scale(jnp.dot(normed, latent_down, preferred_element_type=jnp.float32), latent_gain))
    rope_key = rounded(rotate(jnp.dot(normed, rope_down, preferred_element_type=jnp.float32), angles))
    keys = jnp.concatenate([latent, rope_key], axis=1).astype(jnp.float32)
    latent_wide = latent.astype(jnp.float32)
    score_scale = (NOPE + ROPE) ** (-0.5)
    block_count = LENGTH // TOK_DEV
    query_blocks = jnp.transpose(queries.reshape(HEADS, block_count, TOK_DEV, KVR + ROPE), (1, 0, 2, 3))

    def attend_block(query_block):
        scores = jnp.einsum('hqc,kc->hqk', query_block, keys) * score_scale
        row_max = lax.optimization_barrier(jnp.max(scores, axis=-1))
        weights = jnp.exp(scores - row_max[:, :, None])
        row_sum = lax.optimization_barrier(jnp.sum(weights, axis=-1))
        summed = jnp.einsum('hqk,kr->hqr', rounded(weights).astype(jnp.float32), latent_wide)
        return (rounded(summed / row_sum[:, :, None]), row_max + jnp.log(row_sum))
    attended, log_blocks = lax.map(attend_block, query_blocks)
    attended = jnp.transpose(attended, (1, 0, 2, 3)).reshape(HEADS, LENGTH, KVR)
    log_weight = jnp.transpose(log_blocks, (1, 0, 2)).reshape(HEADS, LENGTH)
    head_out = jnp.einsum('htr,rhv->thv', attended.astype(jnp.float32), value_up.astype(jnp.float32).reshape(KVR, HEADS, VDIM))
    head_out = rounded(head_out.reshape(LENGTH, HEADS * VDIM))
    value_in = jnp.dot(normed, glu_value, preferred_element_type=jnp.float32)
    gate_in = jnp.dot(normed, glu_gate, preferred_element_type=jnp.float32)
    gated_rows = rounded(value_in * jax.nn.sigmoid(gate_in))
    reach_rows = WIDTH // 2
    padded = jnp.pad(gated_rows.astype(jnp.float32), ((reach_rows, reach_rows), (0, 0)))
    filtered = padded[0:LENGTH] * conv_taps[0].astype(jnp.float32)
    for tap_index in range(1, WIDTH):
        filtered = filtered + padded[tap_index:tap_index + LENGTH] * conv_taps[tap_index].astype(jnp.float32)
    grouped = filtered.reshape(LENGTH, GROUPS, CH // GROUPS)
    centred = grouped - lax.optimization_barrier(jnp.mean(grouped, axis=-1, keepdims=True))
    spread = lax.optimization_barrier(jnp.mean(centred * centred, axis=-1, keepdims=True))
    normal_groups = (centred * lax.rsqrt(spread + norm_eps)).reshape(LENGTH, CH)
    conv_branch = rounded(jax.nn.silu(normal_groups * group_gain.astype(jnp.float32)))
    head_part = HEADS * VDIM // N_TP
    channel_part = CH // N_TP
    mixed_total = jnp.zeros((LENGTH, D), jnp.float32)
    for group_index in range(N_TP):
        head_lo = group_index * head_part
        chan_lo = group_index * channel_part
        partial_value = jnp.dot(head_out[:, head_lo:head_lo + head_part], head_proj[head_lo:head_lo + head_part], preferred_element_type=jnp.float32)
        partial_value = partial_value + jnp.dot(conv_branch[:, chan_lo:chan_lo + channel_part], channel_proj[chan_lo:chan_lo + channel_part], preferred_element_type=jnp.float32)
        mixed_total = mixed_total + rounded(partial_value).astype(jnp.float32)
    return (mixed_total.astype(jnp.bfloat16), log_weight)
```

```python
import jax
import jax.numpy as jnp
from jax import lax
from jax.experimental import pallas as pl
from jax.experimental.pallas import tpu as pltpu
from jax.sharding import PartitionSpec as P

NOPE = 128
ROPE = 64
VDIM = 128
KVR = 256
GROUP = 128
GRID_W = 64
EDGE = 16
SIDE = 8
FS = 4
TP = 2
ROW = 32
OFFSETS = (0, -1, 1, -2, 2, -3, 3, -4)
FIRST = 5
KEY_ROWS = 160
PACK = 224
MESH_AXES = ("sp", "fs", "tp")

norm_eps = 1e-06
rope_base = 10000.0
far_below = -1e30
LOG2E = 1.4426950408889634
LN2 = 0.6931471805599453

f32 = jnp.float32
bf16 = jnp.bfloat16


def flat(z, y, x, c):
    return ((z * SIDE + y) * FS + x) * TP + c


def line_groups(phase):
    groups = []
    for x in range(FS):
        for c in range(TP):
            for o in range(SIDE):
                if (c == 0) == (phase == 0):
                    groups.append([flat(o, i, x, c) for i in range(SIDE)])
                else:
                    groups.append([flat(i, o, x, c) for i in range(SIDE)])
    return groups


def line_pairs(step, phase):
    pairs = []
    for group in line_groups(phase):
        pairs += [(group[i], group[(i + step) % SIDE]) for i in range(SIDE)]
    return pairs


def nt_dot(a, b):
    return lax.dot_general(a, b, (((1,), (1,)), ((), ())), preferred_element_type=f32)


def nn_dot(a, b):
    return jnp.dot(a, b, preferred_element_type=f32)


def scaled(values, gain):
    inv = lax.rsqrt(jnp.mean(values * values, axis=-1, keepdims=True) + norm_eps)
    return values * inv * gain.astype(f32)


def pre_kernel(where, tok, gain, ldown, lgain, rdown, cosv, sinv, normed, pack):
    half = tok.shape[0] // TP
    normed[...] = scaled(tok[...].astype(f32), gain[...]).astype(bf16)
    start = pl.multiple_of(where[2] * half, half)
    own = normed[pl.ds(start, half), :]
    latent = scaled(nn_dot(own, ldown[...]), lgain[...]).astype(bf16)
    pack[0:half, :] = latent[:, :128]
    pack[half : 2 * half, :] = latent[:, 128:]
    raw = nn_dot(own, rdown[...])
    turned = jnp.concatenate([raw[:, ROPE // 2 :], raw[:, : ROPE // 2]], axis=1)
    key = raw * cosv[pl.ds(start, half), :] + turned * sinv[pl.ds(start, half), :]
    pack[2 * half :, :] = jnp.concatenate([key[: half // 2], key[half // 2 :]], axis=1).astype(bf16)


def query_kernel(
    where, normed, g1, g2, t1, t2, qgain, qup, kup, cosv, sinv, queries, weight, lat
):
    z, y, c = where[0], where[1], where[2]
    count = SIDE * SIDE
    for theirs, parts in ((0, (g1, g2)), (1, (t1, t2))):
        kind = jnp.bitwise_xor(c, 1) if theirs else c
        base = jnp.where(kind == 0, z, y)
        for k, off in enumerate(OFFSETS):
            src, at = (parts[0], k) if k < FIRST else (parts[1], k - FIRST)
            far = jnp.bitwise_and(base + (off + SIDE), SIDE - 1)
            for o in range(SIDE):
                block = jnp.where(kind == 0, far * SIDE + o, o * SIDE + far)
                for h in range(2):
                    lo = KEY_ROWS + h * ROW
                    weight[kind * 2 + h, block] = src[at * SIDE + o, lo : lo + ROW, :]
    x = normed[...]
    for g in range(4):
        lat[:, g * 128 : (g + 1) * 128] = nn_dot(x, weight[g].reshape(count * ROW, 128))
    latent = scaled(lat[...], qgain[...]).astype(bf16)
    every = nn_dot(latent, qup[...])
    heads = kup.shape[1] // NOPE
    rows = normed.shape[0]
    for h in range(heads):
        lo = h * (NOPE + ROPE)
        plain = every[:, lo : lo + NOPE].astype(bf16)
        raw = every[:, lo + NOPE : lo + NOPE + ROPE]
        turned = jnp.concatenate([raw[:, ROPE // 2 :], raw[:, : ROPE // 2]], axis=1)
        rot = raw * cosv[...] + turned * sinv[...]
        rot = jnp.concatenate([rot, jnp.zeros_like(rot)], axis=1).astype(bf16)
        absorbed = nt_dot(plain, kup[:, h * NOPE : (h + 1) * NOPE]).astype(bf16)
        queries[h * rows : (h + 1) * rows, :KVR] = absorbed
        queries[h * rows : (h + 1) * rows, KVR:] = rot


def attend_kernel(queries, g1, g2, t1, t2, vup, head_out, logw, keys, top, low, acc):
    rows = head_out.shape[0]
    heads = queries.shape[0] // rows
    per = SIDE * 64
    base = 0
    for src in (g1, g2, t1, t2):
        count = src.shape[0] // SIDE

        def fill(i, carry, src=src, base=base):
            part = src[pl.ds(i * SIDE, SIDE)]
            keys[base + i, :, 0:128] = part[:, 0:64, :].reshape(per, 128)
            keys[base + i, :, 128:256] = part[:, 64:128, :].reshape(per, 128)
            near = part[:, 128:160, :].astype(f32)
            far = pltpu.roll(near.reshape(per // 2, 128), 64, 1).reshape(SIDE, 32, 128)
            both = jnp.concatenate([near, far], axis=1).reshape(per, 128)
            keys[base + i, :, 256:384] = both.astype(bf16)
            return carry

        lax.fori_loop(0, count, fill, 0)
        base += count
    top[...] = jnp.full_like(top, far_below)
    low[...] = jnp.zeros_like(low)
    acc[...] = jnp.zeros_like(acc)
    factor = LOG2E * (NOPE + ROPE) ** (-0.5)

    def step(j, carry):
        k = keys[j]
        v = k[:, :KVR]
        for h in range(heads):
            span = slice(h * rows, (h + 1) * rows)
            s = nt_dot(queries[span, :], k) * factor
            old = top[span, :]
            new = jnp.maximum(old, jnp.max(s, axis=1, keepdims=True))
            p = jnp.exp2(s - new[:, :1])
            fade = jnp.exp2(old - new)
            part = p[:, 0:128]
            for i in range(1, per // 128):
                part = part + p[:, i * 128 : (i + 1) * 128]
            low[span, :] = low[span, :] * fade + part
            top[span, :] = new
            add = nn_dot(p.astype(bf16), v)
            acc[span, :] = acc[span, :] * jnp.concatenate([fade, fade], axis=1) + add
        return carry

    lax.fori_loop(0, base, step, 0)
    for h in range(heads):
        span = slice(h * rows, (h + 1) * rows)
        total = jnp.sum(low[span, :], axis=1, keepdims=True)
        attended = (acc[span, :] / total).astype(bf16)
        out = nn_dot(attended, vup[:, h * VDIM : (h + 1) * VDIM])
        head_out[:, h * VDIM : (h + 1) * VDIM] = out.astype(bf16)
        logs = top[span, :] * LN2 + jnp.log(total)
        logw[h : h + 1, :] = jnp.transpose(logs)[0:1, :]


def post_kernel(
    where, normed, before, after, gain, w_any, taps, ggain, head_out, mine, other, w, wide, gated, sems
):
    c = where[2]
    rows = normed.shape[0]
    half = w.shape[3] // 2

    @pl.when(c == 0)
    def _():
        for p in range(2):
            for j in range(SIDE):
                pltpu.make_async_copy(
                    w_any.at[j, :, :, pl.ds(p * half, half)],
                    w.at[j, :, :, pl.ds(p * half, half)],
                    sems.at[p * SIDE + j],
                ).start()

    @pl.when(c != 0)
    def _():
        for p in range(2):
            for j in range(SIDE):
                pltpu.make_async_copy(
                    w_any.at[j, :, :, pl.ds(p * half, half)],
                    w.at[:, j, :, pl.ds(p * half, half)],
                    sems.at[p * SIDE + j],
                ).start()

    def arrive(p):
        for j in range(SIDE):
            pltpu.make_async_copy(
                w_any.at[j, :, :, pl.ds(p * half, half)],
                w.at[j, :, :, pl.ds(p * half, half)],
                sems.at[p * SIDE + j],
            ).wait()

    wide[0:EDGE, :] = scaled(before[...].astype(f32), gain[...]).astype(bf16)
    wide[EDGE : EDGE + rows, :] = normed[...]
    wide[EDGE + rows :, :] = scaled(after[...].astype(f32), gain[...]).astype(bf16)
    arrive(0)
    x = wide[...]
    ch = half // 2
    depth = SIDE * SIDE * ROW
    for g in range(ch // GROUP):
        lanes = slice(g * GROUP, (g + 1) * GROUP)
        value = nn_dot(x, w[:, :, :, lanes].reshape(depth, GROUP))
        gate = nn_dot(x, w[:, :, :, ch + g * GROUP : ch + (g + 1) * GROUP].reshape(depth, GROUP))
        gated[:, lanes] = (value * jax.nn.sigmoid(gate)).astype(bf16).astype(f32)
    mixed = []
    reach = taps.shape[0] // 2
    for g in range(ch // GROUP):
        lanes = slice(g * GROUP, (g + 1) * GROUP)
        tap = taps[:, lanes].astype(f32)
        lo = EDGE - reach
        total = gated[lo : lo + rows, lanes] * tap[0:1, :]
        for j in range(1, taps.shape[0]):
            total = total + gated[lo + j : lo + j + rows, lanes] * tap[j : j + 1, :]
        centred = total - jnp.mean(total, axis=-1, keepdims=True)
        spread = jnp.mean(centred * centred, axis=-1, keepdims=True)
        unit = centred * lax.rsqrt(spread + norm_eps) * ggain[:, lanes].astype(f32)
        mixed.append((unit * jax.nn.sigmoid(unit)).astype(bf16))
    mix = jnp.concatenate([head_out[...]] + mixed, axis=1)
    arrive(1)
    part = SIDE // TP
    for out, which in ((other, jnp.bitwise_xor(c, 1)), (mine, c)):
        wo = w[pl.ds(which * part, part), :, :, half:].reshape(depth // TP, half)
        out[...] = nt_dot(mix, wo).astype(bf16)


def per_device(
    tokens,
    norm_gain,
    query_down,
    query_gain,
    latent_down,
    latent_gain,
    rope_down,
    query_up,
    key_up,
    value_up,
    glu_value,
    glu_gate,
    conv_taps,
    group_gain,
    head_proj,
    channel_proj,
):
    tok = tokens.shape[0]
    sp = lax.axis_index("sp")
    core = lax.axis_index("tp")
    where = jnp.stack([sp // SIDE, sp % SIDE, core]).astype(jnp.int32)
    smem = pl.BlockSpec(memory_space=pltpu.SMEM)
    vmem = pl.BlockSpec(memory_space=pltpu.VMEM)
    hbm = pl.BlockSpec(memory_space=pltpu.HBM)
    first, second = line_groups(0), line_groups(1)

    rows_in = jnp.concatenate([glu_value, glu_gate, head_proj.T, channel_proj.T], axis=1)
    sent = jnp.broadcast_to(rows_in[None], (SIDE,) + rows_in.shape)
    near = lax.all_to_all(sent, MESH_AXES, 0, 0, axis_index_groups=first, tiled=True)
    weights = lax.all_gather(near, MESH_AXES, axis_index_groups=second, axis=0, tiled=False)

    sp_count = lax.axis_size("sp")
    forward = [(i, i + 1) for i in range(sp_count - 1)]
    backward = [(i + 1, i) for i in range(sp_count - 1)]
    before = lax.ppermute(tokens[tok - EDGE :], "sp", forward)
    after = lax.ppermute(tokens[:EDGE], "sp", backward)

    quarter = ROPE // 4
    inverse = rope_base ** (-jnp.arange(quarter, dtype=f32) / quarter)
    places = sp * tok + jnp.arange(tok, dtype=jnp.int32)
    grid_row = (places // GRID_W).astype(f32)
    grid_col = (places % GRID_W).astype(f32)
    angles = jnp.concatenate([grid_row[:, None] * inverse, grid_col[:, None] * inverse], axis=-1)
    cosine, sine = jnp.cos(angles), jnp.sin(angles)
    cosv = jnp.concatenate([cosine, cosine], axis=1)
    sinv = jnp.concatenate([-sine, sine], axis=1)

    gain2 = norm_gain[None]
    normed, pack = pl.pallas_call(
        pre_kernel,
        name="pre",
        out_shape=(
            jax.ShapeDtypeStruct(tokens.shape, bf16),
            jax.ShapeDtypeStruct((KEY_ROWS, 128), bf16),
        ),
        in_specs=[smem] + [vmem] * 7,
        out_specs=(vmem, vmem),
        cost_estimate=pl.CostEstimate(flops=int(2e9), bytes_accessed=3 * 2**20, transcendentals=0),
    )(where, tokens, gain2, latent_down, latent_gain[None], rope_down, cosv, sinv)

    own_half = lax.dynamic_slice_in_dim(query_down, core * 256, 256, 1)
    pack = jnp.concatenate([pack, own_half[:, :128], own_half[:, 128:]], axis=0)
    sent = jnp.broadcast_to(pack[None], (SIDE, PACK, 128))
    own = lax.all_to_all(sent, MESH_AXES, 0, 0, axis_index_groups=first, tiled=True)

    def move(block, step):
        return lax.ppermute(block, MESH_AXES, line_pairs(step, 1))

    up1, down1 = move(own, 1), move(own, -1)
    up2, down2 = move(own, 2), move(own, -2)
    up3, down3 = move(up2, 1), move(down2, -1)
    up4 = move(up2, 2)
    swap = [(0, 1), (1, 0)]
    g1 = jnp.concatenate([own, up1, down1, up2, down2], axis=0)
    t1 = lax.ppermute(g1, "tp", swap)
    g2 = jnp.concatenate([up3, down3, up4], axis=0)
    t2 = lax.ppermute(g2, "tp", swap)

    heads = key_up.shape[1] // NOPE
    queries = pl.pallas_call(
        query_kernel,
        name="query",
        out_shape=jax.ShapeDtypeStruct((heads * tok, KVR + 128), bf16),
        in_specs=[smem] + [vmem] * 10,
        out_specs=vmem,
        scratch_shapes=[
            pltpu.VMEM((4, SIDE * SIDE, ROW, 128), bf16),
            pltpu.VMEM((tok, 512), f32),
        ],
        cost_estimate=pl.CostEstimate(flops=int(2e9), bytes_accessed=8 * 2**20, transcendentals=0),
    )(where, normed, g1, g2, t1, t2, query_gain[None], query_up, key_up, cosv, sinv)

    chunks = 2 * SIDE
    head_out, log_weight = pl.pallas_call(
        attend_kernel,
        name="attend",
        out_shape=(
            jax.ShapeDtypeStruct((tok, heads * VDIM), bf16),
            jax.ShapeDtypeStruct((heads, tok), f32),
        ),
        in_specs=[vmem] * 6,
        out_specs=(vmem, vmem),
        scratch_shapes=[
            pltpu.VMEM((chunks, SIDE * 64, KVR + 128), bf16),
            pltpu.VMEM((heads * tok, 128), f32),
            pltpu.VMEM((heads * tok, 128), f32),
            pltpu.VMEM((heads * tok, KVR), f32),
        ],
        cost_estimate=pl.CostEstimate(flops=int(8e9), bytes_accessed=8 * 2**20, transcendentals=0),
    )(queries, g1, g2, t1, t2, value_up)

    width = rows_in.shape[1]
    mine, other = pl.pallas_call(
        post_kernel,
        name="post",
        out_shape=(jax.ShapeDtypeStruct((tok, width // 2), bf16),) * 2,
        in_specs=[smem] + [vmem] * 4 + [hbm] + [vmem] * 3,
        out_specs=(vmem, vmem),
        scratch_shapes=[
            pltpu.VMEM((SIDE, SIDE, ROW, width), bf16),
            pltpu.VMEM((tok + 2 * EDGE, tokens.shape[1]), bf16),
            pltpu.VMEM((tok + 2 * EDGE, width // 4), f32),
            pltpu.SemaphoreType.DMA((2 * SIDE,)),
        ],
        cost_estimate=pl.CostEstimate(flops=int(3e9), bytes_accessed=9 * 2**20, transcendentals=0),
    )(where, normed, before, after, gain2, weights, conv_taps, group_gain[None], head_out)
    arrived = lax.ppermute(other, "tp", swap)
    mixed_out = (mine.astype(f32) + arrived.astype(f32)).astype(bf16)
    return (mixed_out, log_weight)


def solution(mesh):
    in_specs = (
        P(("fs", "sp"), None),
        P(),
        P("sp", None),
        P(),
        P(),
        P(),
        P(),
        P(None, "tp"),
        P(None, "tp"),
        P(None, "tp"),
        P("sp", "tp"),
        P("sp", "tp"),
        P(None, "tp"),
        P("tp"),
        P("tp", "sp"),
        P("tp", "sp"),
    )
    out_specs = (P(("fs", "sp"), "tp"), P("tp", ("fs", "sp")))
    return jax.shard_map(
        per_device, mesh=mesh, in_specs=in_specs, out_specs=out_specs, check_vma=False
    )
```

```python
import jax
import jax.numpy as jnp
from jax import lax
from jax.experimental import pallas as pl
from jax.experimental.pallas import tpu as pltpu
from jax.sharding import PartitionSpec as P

NOPE = 128
ROPE = 64
VDIM = 128
KVR = 256
GROUP = 128
GRID_W = 64
EDGE = 16
SIDE = 8
FS = 4
TP = 2
ROW = 32
OFFSETS = (0, -1, 1, -2, 2, -3, 3, -4)
FIRST = 5
KEY_ROWS = 160
PACK = 224
MESH_AXES = ("sp", "fs", "tp")

norm_eps = 1e-06
rope_base = 10000.0
far_below = -1e30
LOG2E = 1.4426950408889634
LN2 = 0.6931471805599453

f32 = jnp.float32
bf16 = jnp.bfloat16


def flat(z, y, x, c):
    return ((z * SIDE + y) * FS + x) * TP + c


def line_groups(phase):
    groups = []
    for x in range(FS):
        for c in range(TP):
            for o in range(SIDE):
                if (c == 0) == (phase == 0):
                    groups.append([flat(o, i, x, c) for i in range(SIDE)])
                else:
                    groups.append([flat(i, o, x, c) for i in range(SIDE)])
    return groups


def line_pairs(step, phase):
    pairs = []
    for group in line_groups(phase):
        pairs += [(group[i], group[(i + step) % SIDE]) for i in range(SIDE)]
    return pairs


def nt_dot(a, b):
    return lax.dot_general(a, b, (((1,), (1,)), ((), ())), preferred_element_type=f32)


def nn_dot(a, b):
    return jnp.dot(a, b, preferred_element_type=f32)


def scaled(values, gain):
    inv = lax.rsqrt(jnp.mean(values * values, axis=-1, keepdims=True) + norm_eps)
    return values * inv * gain.astype(f32)


def turned_half(raw):
    return jnp.concatenate([raw[:, ROPE // 2 :], raw[:, : ROPE // 2]], axis=1)


def doubled(cosv, sinv):
    return jnp.concatenate([cosv, cosv], axis=1), jnp.concatenate([-sinv, sinv], axis=1)


def place():
    sp = lax.axis_index("sp")
    return lax.div(sp, SIDE), lax.rem(sp, SIDE), lax.axis_index("tp")


def pre_kernel(tok, gain, ldown, lgain, rdown, qdown, cosv, sinv, normed, pack):
    half = tok.shape[0] // TP
    c = place()[2]
    normed[...] = scaled(tok[...].astype(f32), gain[...]).astype(bf16)
    start = pl.multiple_of(c * half, half)
    own = normed[pl.ds(start, half), :]
    latent = scaled(nn_dot(own, ldown[...]), lgain[...]).astype(bf16)
    raw = nt_dot(own, rdown[...])
    cos2, sin2 = doubled(cosv[pl.ds(start, half), :], sinv[pl.ds(start, half), :])
    key = raw * cos2 + turned_half(raw) * sin2
    pair = jnp.concatenate([key[: half // 2], key[half // 2 :]], axis=1).astype(bf16)
    q0 = qdown[:, pl.ds(pl.multiple_of(c * 256, 128), 128)]
    q1 = qdown[:, pl.ds(pl.multiple_of(c * 256 + 128, 128), 128)]
    for i in range(SIDE):
        pack[i, 0:half, :] = latent[:, :128]
        pack[i, half : 2 * half, :] = latent[:, 128:]
        pack[i, 2 * half : KEY_ROWS, :] = pair
        pack[i, KEY_ROWS : KEY_ROWS + ROW, :] = q0
        pack[i, KEY_ROWS + ROW :, :] = q1


def attend_kernel(
    normed, g1, g2, t1, t2, qgain, qup, kup, vup, cosv, sinv, head_out, logw,
    weight, lat, queries, keys, sa, sb, p, top, low, acc
):
    z, y, c = place()
    blocks = SIDE * SIDE
    for theirs, parts in ((0, (g1, g2)), (1, (t1, t2))):
        kind = jnp.bitwise_xor(c, 1) if theirs else c
        base = jnp.where(kind == 0, z, y)
        for k, off in enumerate(OFFSETS):
            src, at = (parts[0], k) if k < FIRST else (parts[1], k - FIRST)
            far = jnp.bitwise_and(base + (off + SIDE), SIDE - 1)
            for o in range(SIDE):
                block = jnp.where(kind == 0, far * SIDE + o, o * SIDE + far)
                for h in range(2):
                    lo = KEY_ROWS + h * ROW
                    weight[kind * 2 + h, block] = src[at * SIDE + o, lo : lo + ROW, :]
    x = normed[...]
    for g in range(4):
        lat[:, g * 128 : (g + 1) * 128] = nn_dot(x, weight[g].reshape(blocks * ROW, 128))
    latent = scaled(lat[...], qgain[...]).astype(bf16)
    every = nn_dot(latent, qup[...])
    heads = kup.shape[1] // NOPE
    rows = normed.shape[0]
    cos2, sin2 = doubled(cosv[...], sinv[...])
    for h in range(heads):
        lo = h * (NOPE + ROPE)
        plain = every[:, lo : lo + NOPE].astype(bf16)
        raw = every[:, lo + NOPE : lo + NOPE + ROPE]
        rot = raw * cos2 + turned_half(raw) * sin2
        rot = jnp.concatenate([rot, jnp.zeros_like(rot)], axis=1).astype(bf16)
        absorbed = nt_dot(plain, kup[:, h * NOPE : (h + 1) * NOPE]).astype(bf16)
        queries[h * rows : (h + 1) * rows, :KVR] = absorbed
        queries[h * rows : (h + 1) * rows, KVR:] = rot

    per = SIDE * 64
    base = 0
    for src in (g1, g2, t1, t2):
        count = src.shape[0] // SIDE

        def fill(i, carry, src=src, base=base):
            part = src[pl.ds(i * SIDE, SIDE)]
            to = pl.ds(pl.multiple_of((base + i) * per, per), per)
            keys[to, 0:128] = part[:, 0:64, :].reshape(per, 128)
            keys[to, 128:256] = part[:, 64:128, :].reshape(per, 128)
            near = part[:, 128:160, :].astype(f32)
            far = pltpu.roll(near.reshape(per // 2, 128), 64, 1).reshape(SIDE, 32, 128)
            both = jnp.concatenate([near, far], axis=1).reshape(per, 128)
            keys[to, 256:384] = both.astype(bf16)
            return carry

        lax.fori_loop(0, count, fill, 0)
        base += count
    top[...] = jnp.full_like(top, far_below)
    low[...] = jnp.zeros_like(low)
    acc[...] = jnp.zeros_like(acc)
    factor = LOG2E * (NOPE + ROPE) ** (-0.5)
    wide = sa.shape[1]
    steps = keys.shape[0] // wide
    total_rows = heads * rows

    def span(j):
        return pl.ds(pl.multiple_of(j * wide, wide), wide)

    def score(j, s):
        s[...] = nt_dot(queries[...], keys[span(j), :])

    def soften(j, s):
        fades = []
        for r in range(0, total_rows, 32):
            at = slice(r, r + 32)
            v = s[at, :]
            most = v[:, 0:128]
            for i in range(1, wide // 128):
                most = jnp.maximum(most, v[:, i * 128 : (i + 1) * 128])
            old = top[at, :]
            new = jnp.maximum(old, jnp.max(most, axis=1, keepdims=True))
            fade = jnp.exp2((old - new) * factor)
            part = low[at, :] * fade
            for i in range(wide // 128):
                e = jnp.exp2((v[:, i * 128 : (i + 1) * 128] - new) * factor)
                part = part + e
                p[at, i * 128 : (i + 1) * 128] = e.astype(bf16)
            low[at, :] = part
            top[at, :] = new
            acc[at, 0:128] = acc[at, 0:128] * fade
            acc[at, 128:256] = acc[at, 128:256] * fade
        acc[...] += nn_dot(p[...], keys[span(j), 0:KVR])

    score(0, sa)

    def pair(i, carry):
        score(2 * i + 1, sb)
        soften(2 * i, sa)
        score(jnp.minimum(2 * i + 2, steps - 1), sa)
        soften(2 * i + 1, sb)
        return carry

    lax.fori_loop(0, steps // 2, pair, 0)
    for h in range(heads):
        at = slice(h * rows, (h + 1) * rows)
        total = jnp.sum(low[at, :], axis=1, keepdims=True)
        attended = (acc[at, :] / total).astype(bf16)
        out = nn_dot(attended, vup[:, h * VDIM : (h + 1) * VDIM])
        head_out[:, h * VDIM : (h + 1) * VDIM] = out.astype(bf16)
        logs = top[at, :] * (factor * LN2) + jnp.log(total)
        logw[h : h + 1, :] = jnp.transpose(logs)[0:1, :]


def post_kernel(
    normed, before, after, gain, w_any, taps, ggain, head_out, mine, other, w, wide, gated, sems
):
    c = place()[2]
    rows = normed.shape[0]
    depth, width = w.shape
    half = width // 2
    slab = depth // SIDE

    def piece(p, j):
        at = (pl.ds(j * slab, slab), pl.ds(p * half, half))
        return pltpu.make_async_copy(w_any.at[at], w.at[at], sems.at[p * SIDE + j])

    for p in range(2):
        for j in range(SIDE):
            piece(p, j).start()

    def arrive(p):
        for j in range(SIDE):
            piece(p, j).wait()

    wide[0:EDGE, :] = scaled(before[...].astype(f32), gain[...]).astype(bf16)
    wide[EDGE : EDGE + rows, :] = normed[...]
    wide[EDGE + rows :, :] = scaled(after[...].astype(f32), gain[...]).astype(bf16)
    arrive(0)
    x = wide[...]
    ch = half // 2
    for g in range(ch // GROUP):
        lanes = slice(g * GROUP, (g + 1) * GROUP)
        value = nn_dot(x, w[:, lanes])
        gate = nn_dot(x, w[:, ch + g * GROUP : ch + (g + 1) * GROUP])
        gated[:, lanes] = (value * jax.nn.sigmoid(gate)).astype(bf16).astype(f32)
    mixed = []
    reach = taps.shape[0] // 2
    for g in range(ch // GROUP):
        lanes = slice(g * GROUP, (g + 1) * GROUP)
        tap = taps[:, lanes].astype(f32)
        lo = EDGE - reach
        total = gated[lo : lo + rows, lanes] * tap[0:1, :]
        for j in range(1, taps.shape[0]):
            total = total + gated[lo + j : lo + j + rows, lanes] * tap[j : j + 1, :]
        centred = total - jnp.mean(total, axis=-1, keepdims=True)
        spread = jnp.mean(centred * centred, axis=-1, keepdims=True)
        unit = centred * lax.rsqrt(spread + norm_eps) * ggain[:, lanes].astype(f32)
        mixed.append((unit * jax.nn.sigmoid(unit)).astype(bf16))
    mix = jnp.concatenate([head_out[...]] + mixed, axis=1)
    arrive(1)
    part = depth // TP
    for out, which in ((other, jnp.bitwise_xor(c, 1)), (mine, c)):
        wo = w[pl.ds(pl.multiple_of(which * part, part), part), half:]
        out[...] = nt_dot(mix, wo).astype(bf16)


def per_device(
    tokens,
    norm_gain,
    query_down,
    query_gain,
    latent_down,
    latent_gain,
    rope_down,
    query_up,
    key_up,
    value_up,
    glu_value,
    glu_gate,
    conv_taps,
    group_gain,
    head_proj,
    channel_proj,
):
    tok = tokens.shape[0]
    sp = lax.axis_index("sp")
    vmem = pl.BlockSpec(memory_space=pltpu.VMEM)
    hbm = pl.BlockSpec(memory_space=pltpu.HBM)
    first = line_groups(0)

    rows_in = jnp.concatenate([glu_value, glu_gate, head_proj.T, channel_proj.T], axis=1)
    weights = lax.all_gather(rows_in, "sp", axis=0, tiled=True)

    quarter = ROPE // 4
    inverse = rope_base ** (-jnp.arange(quarter, dtype=f32) / quarter)
    places = sp * tok + jnp.arange(tok, dtype=jnp.int32)
    grid_row = (places // GRID_W).astype(f32)
    grid_col = (places % GRID_W).astype(f32)
    angles = jnp.concatenate([grid_row[:, None] * inverse, grid_col[:, None] * inverse], axis=-1)
    cosine, sine = jnp.cos(angles), jnp.sin(angles)
    gain2 = norm_gain[None]
    normed, sent = pl.pallas_call(
        pre_kernel,
        name="pre",
        out_shape=(
            jax.ShapeDtypeStruct(tokens.shape, bf16),
            jax.ShapeDtypeStruct((SIDE, PACK, 128), bf16),
        ),
        in_specs=[vmem] * 8,
        out_specs=(vmem, vmem),
        cost_estimate=pl.CostEstimate(flops=int(2e9), bytes_accessed=3 * 2**20, transcendentals=0),
    )(tokens, gain2, latent_down, latent_gain[None], rope_down.T, query_down, cosine, sine)
    own = lax.all_to_all(sent, MESH_AXES, 0, 0, axis_index_groups=first, tiled=True)

    def move(block, step):
        return lax.ppermute(block, MESH_AXES, line_pairs(step, 1))

    up1, down1 = move(own, 1), move(own, -1)
    up2, down2 = move(own, 2), move(own, -2)
    up3, down3 = move(up2, 1), move(down2, -1)
    up4 = move(up2, 2)
    swap = [(0, 1), (1, 0)]
    g1 = jnp.concatenate([own, up1, down1, up2, down2], axis=0)
    t1 = lax.ppermute(g1, "tp", swap)
    g2 = jnp.concatenate([up3, down3, up4], axis=0)
    t2 = lax.ppermute(g2, "tp", swap)

    heads = key_up.shape[1] // NOPE
    many = heads * tok
    total_keys = 2 * SIDE * SIDE * 64
    chunk = 1024
    head_out, log_weight = pl.pallas_call(
        attend_kernel,
        name="attend",
        out_shape=(
            jax.ShapeDtypeStruct((tok, heads * VDIM), bf16),
            jax.ShapeDtypeStruct((heads, tok), f32),
        ),
        in_specs=[vmem] * 11,
        out_specs=(vmem, vmem),
        scratch_shapes=[
            pltpu.VMEM((4, SIDE * SIDE, ROW, 128), bf16),
            pltpu.VMEM((tok, 512), f32),
            pltpu.VMEM((many, KVR + 128), bf16),
            pltpu.VMEM((total_keys, KVR + 128), bf16),
            pltpu.VMEM((many, chunk), f32),
            pltpu.VMEM((many, chunk), f32),
            pltpu.VMEM((many, chunk), bf16),
            pltpu.VMEM((many, 128), f32),
            pltpu.VMEM((many, 128), f32),
            pltpu.VMEM((many, KVR), f32),
        ],
        cost_estimate=pl.CostEstimate(flops=int(8e9), bytes_accessed=8 * 2**20, transcendentals=0),
    )(normed, g1, g2, t1, t2, query_gain[None], query_up, key_up, value_up, cosine, sine)

    sp_count = lax.axis_size("sp")
    forward = [(i, i + 1) for i in range(sp_count - 1)]
    backward = [(i + 1, i) for i in range(sp_count - 1)]
    last, front, head_out = lax.optimization_barrier(
        (tokens[tok - EDGE :], tokens[:EDGE], head_out)
    )
    before = lax.ppermute(last, "sp", forward)
    after = lax.ppermute(front, "sp", backward)

    width = rows_in.shape[1]
    mine, other = pl.pallas_call(
        post_kernel,
        name="post",
        out_shape=(jax.ShapeDtypeStruct((tok, width // 2), bf16),) * 2,
        in_specs=[vmem] * 4 + [hbm] + [vmem] * 3,
        out_specs=(vmem, vmem),
        scratch_shapes=[
            pltpu.VMEM(weights.shape, bf16),
            pltpu.VMEM((tok + 2 * EDGE, tokens.shape[1]), bf16),
            pltpu.VMEM((tok + 2 * EDGE, width // 4), f32),
            pltpu.SemaphoreType.DMA((2 * SIDE,)),
        ],
        cost_estimate=pl.CostEstimate(flops=int(3e9), bytes_accessed=9 * 2**20, transcendentals=0),
    )(normed, before, after, gain2, weights, conv_taps, group_gain[None], head_out)
    arrived = lax.ppermute(other, "tp", swap)
    mixed_out = (mine.astype(f32) + arrived.astype(f32)).astype(bf16)
    return (mixed_out, log_weight)


def solution(mesh):
    in_specs = (
        P(("fs", "sp"), None),
        P(),
        P("sp", None),
        P(),
        P(),
        P(),
        P(),
        P(None, "tp"),
        P(None, "tp"),
        P(None, "tp"),
        P("sp", "tp"),
        P("sp", "tp"),
        P(None, "tp"),
        P("tp"),
        P("tp", "sp"),
        P("tp", "sp"),
    )
    out_specs = (P(("fs", "sp"), "tp"), P("tp", ("fs", "sp")))
    return jax.shard_map(
        per_device, mesh=mesh, in_specs=in_specs, out_specs=out_specs, check_vma=False
    )
```

```python
import jax
import jax.numpy as jnp
from jax import lax
from jax.experimental import pallas as pl
from jax.experimental.pallas import tpu as pltpu
from jax.sharding import PartitionSpec as P

NOPE = 128
ROPE = 64
VDIM = 128
KVR = 256
GROUP = 128
GRID_W = 64
EDGE = 16
SIDE = 8
FS = 4
TP = 2
ROW = 32
KEY_ROWS = 160
PACK = 224
MESH_AXES = ("sp", "fs", "tp")

norm_eps = 1e-06
rope_base = 10000.0
far_below = -1e30
LOG2E = 1.4426950408889634
LN2 = 0.6931471805599453

f32 = jnp.float32
bf16 = jnp.bfloat16


def flat(z, y, x, c):
    return ((z * SIDE + y) * FS + x) * TP + c


def line_groups(phase):
    groups = []
    for x in range(FS):
        for c in range(TP):
            for o in range(SIDE):
                if (c == 0) == (phase == 0):
                    groups.append([flat(o, i, x, c) for i in range(SIDE)])
                else:
                    groups.append([flat(i, o, x, c) for i in range(SIDE)])
    return groups


def nt_dot(a, b):
    return lax.dot_general(a, b, (((1,), (1,)), ((), ())), preferred_element_type=f32)


def nn_dot(a, b):
    return jnp.dot(a, b, preferred_element_type=f32)


def scaled(values, gain):
    inv = lax.rsqrt(jnp.mean(values * values, axis=-1, keepdims=True) + norm_eps)
    return values * inv * gain.astype(f32)[None, :]


def turned_half(raw):
    return jnp.concatenate([raw[:, ROPE // 2 :], raw[:, : ROPE // 2]], axis=1)


def doubled(cosv, sinv):
    return jnp.concatenate([cosv, cosv], axis=1), jnp.concatenate([-sinv, sinv], axis=1)


def place():
    sp = lax.axis_index("sp")
    return lax.div(sp, SIDE), lax.rem(sp, SIDE), lax.axis_index("tp")


def pre_kernel(tok, gain, ldown, lgain, rdown, qdown, cosv, sinv, normed, pack):
    half = tok.shape[0] // TP
    c = place()[2]
    normed[...] = scaled(tok[...].astype(f32), gain[...]).astype(bf16)
    start = pl.multiple_of(c * half, half)
    own = normed[pl.ds(start, half), :]
    latent = scaled(nn_dot(own, ldown[...]), lgain[...]).astype(bf16)
    raw = nt_dot(own, rdown[...])
    cos2, sin2 = doubled(cosv[pl.ds(start, half), :], sinv[pl.ds(start, half), :])
    key = raw * cos2 + turned_half(raw) * sin2
    pair = jnp.concatenate([key[: half // 2], key[half // 2 :]], axis=1).astype(bf16)
    q0 = qdown[:, pl.ds(pl.multiple_of(c * 256, 128), 128)]
    q1 = qdown[:, pl.ds(pl.multiple_of(c * 256 + 128, 128), 128)]
    for i in range(SIDE):
        pack[i, 0:half, :] = latent[:, :128]
        pack[i, half : 2 * half, :] = latent[:, 128:]
        pack[i, 2 * half : KEY_ROWS, :] = pair
        pack[i, KEY_ROWS : KEY_ROWS + ROW, :] = q0
        pack[i, KEY_ROWS + ROW :, :] = q1


def attend_kernel(
    normed, mine, theirs, qgain, qup, kup, vup, cosv, sinv, head_out, logw,
    weight, lat, queries, keys, sa, sb, p, top, low, acc
):
    c = place()[2]
    blocks = SIDE * SIDE
    for src, kind in ((mine, c), (theirs, jnp.bitwise_xor(c, 1))):
        for b in range(SIDE):
            for o in range(SIDE):
                block = jnp.where(kind == 0, b * SIDE + o, o * SIDE + b)
                for h in range(2):
                    lo = KEY_ROWS + h * ROW
                    weight[kind * 2 + h, block] = src[b * SIDE + o, lo : lo + ROW, :]
    x = normed[...]
    for g in range(4):
        lat[:, g * 128 : (g + 1) * 128] = nn_dot(x, weight[g].reshape(blocks * ROW, 128))
    latent = scaled(lat[...], qgain[...]).astype(bf16)
    every = nn_dot(latent, qup[...])
    heads = kup.shape[1] // NOPE
    rows = normed.shape[0]
    cos2, sin2 = doubled(cosv[...], sinv[...])
    for h in range(heads):
        lo = h * (NOPE + ROPE)
        plain = every[:, lo : lo + NOPE].astype(bf16)
        raw = every[:, lo + NOPE : lo + NOPE + ROPE]
        rot = raw * cos2 + turned_half(raw) * sin2
        rot = jnp.concatenate([rot, jnp.zeros_like(rot)], axis=1).astype(bf16)
        absorbed = nt_dot(plain, kup[:, h * NOPE : (h + 1) * NOPE]).astype(bf16)
        queries[h * rows : (h + 1) * rows, :KVR] = absorbed
        queries[h * rows : (h + 1) * rows, KVR:] = rot

    per = SIDE * 64
    base = 0
    for src in (mine, theirs):
        count = src.shape[0] // SIDE

        def fill(i, carry, src=src, base=base):
            part = src[pl.ds(i * SIDE, SIDE)]
            to = pl.ds(pl.multiple_of((base + i) * per, per), per)
            keys[to, 0:128] = part[:, 0:64, :].reshape(per, 128)
            keys[to, 128:256] = part[:, 64:128, :].reshape(per, 128)
            near = part[:, 128:160, :].astype(f32)
            far = pltpu.roll(near.reshape(per // 2, 128), 64, 1).reshape(SIDE, 32, 128)
            both = jnp.concatenate([near, far], axis=1).reshape(per, 128)
            keys[to, 256:384] = both.astype(bf16)
            return carry

        lax.fori_loop(0, count, fill, 0)
        base += count
    top[...] = jnp.full_like(top, far_below)
    low[...] = jnp.zeros_like(low)
    acc[...] = jnp.zeros_like(acc)
    factor = LOG2E * (NOPE + ROPE) ** (-0.5)
    wide = sa.shape[1]
    steps = keys.shape[0] // wide
    total_rows = heads * rows

    def span(j):
        return pl.ds(pl.multiple_of(j * wide, wide), wide)

    def score(j, s):
        s[...] = nt_dot(queries[...], keys[span(j), :])

    def soften(j, s):
        fades = []
        for r in range(0, total_rows, 32):
            at = slice(r, r + 32)
            v = s[at, :]
            most = v[:, 0:128]
            for i in range(1, wide // 128):
                most = jnp.maximum(most, v[:, i * 128 : (i + 1) * 128])
            old = top[at, :]
            new = jnp.maximum(old, jnp.max(most, axis=1, keepdims=True))
            fade = jnp.exp2((old - new) * factor)
            part = low[at, :] * fade
            for i in range(wide // 128):
                e = jnp.exp2((v[:, i * 128 : (i + 1) * 128] - new) * factor)
                part = part + e
                p[at, i * 128 : (i + 1) * 128] = e.astype(bf16)
            low[at, :] = part
            top[at, :] = new
            acc[at, 0:128] = acc[at, 0:128] * fade
            acc[at, 128:256] = acc[at, 128:256] * fade
        acc[...] += nn_dot(p[...], keys[span(j), 0:KVR])

    score(0, sa)

    def pair(i, carry):
        score(2 * i + 1, sb)
        soften(2 * i, sa)
        score(jnp.minimum(2 * i + 2, steps - 1), sa)
        soften(2 * i + 1, sb)
        return carry

    lax.fori_loop(0, steps // 2, pair, 0)
    for h in range(heads):
        at = slice(h * rows, (h + 1) * rows)
        total = jnp.sum(low[at, :], axis=1, keepdims=True)
        attended = (acc[at, :] / total).astype(bf16)
        out = nn_dot(attended, vup[:, h * VDIM : (h + 1) * VDIM])
        head_out[:, h * VDIM : (h + 1) * VDIM] = out.astype(bf16)
        logs = top[at, :] * (factor * LN2) + jnp.log(total)
        logw[h : h + 1, :] = jnp.transpose(logs)[0:1, :]


def post_kernel(
    normed, before, after, gain, w_any, taps, ggain, head_out, mine, other, w, wide, gated, sems
):
    c = place()[2]
    rows = normed.shape[0]
    half = w.shape[3] // 2
    depth = SIDE * SIDE * ROW

    @pl.when(c == 0)
    def _():
        for p in range(2):
            for j in range(SIDE):
                pltpu.make_async_copy(
                    w_any.at[j, :, :, pl.ds(p * half, half)],
                    w.at[j, :, :, pl.ds(p * half, half)],
                    sems.at[p * SIDE + j],
                ).start()

    @pl.when(c != 0)
    def _():
        for p in range(2):
            for j in range(SIDE):
                pltpu.make_async_copy(
                    w_any.at[j, :, :, pl.ds(p * half, half)],
                    w.at[:, j, :, pl.ds(p * half, half)],
                    sems.at[p * SIDE + j],
                ).start()

    def arrive(p):
        for j in range(SIDE):
            pltpu.make_async_copy(
                w_any.at[j, :, :, pl.ds(p * half, half)],
                w.at[j, :, :, pl.ds(p * half, half)],
                sems.at[p * SIDE + j],
            ).wait()

    wide[0:EDGE, :] = scaled(before[...].astype(f32), gain[...]).astype(bf16)
    wide[EDGE : EDGE + rows, :] = normed[...]
    wide[EDGE + rows :, :] = scaled(after[...].astype(f32), gain[...]).astype(bf16)
    arrive(0)
    x = wide[...]
    ch = half // 2
    for g in range(ch // GROUP):
        lanes = slice(g * GROUP, (g + 1) * GROUP)
        value = nn_dot(x, w[:, :, :, lanes].reshape(depth, GROUP))
        gate = nn_dot(x, w[:, :, :, ch + g * GROUP : ch + (g + 1) * GROUP].reshape(depth, GROUP))
        gated[:, lanes] = (value * jax.nn.sigmoid(gate)).astype(bf16).astype(f32)
    mixed = []
    reach = taps.shape[0] // 2
    for g in range(ch // GROUP):
        lanes = slice(g * GROUP, (g + 1) * GROUP)
        tap = taps[:, lanes].astype(f32)
        lo = EDGE - reach
        total = gated[lo : lo + rows, lanes] * tap[0:1, :]
        for j in range(1, taps.shape[0]):
            total = total + gated[lo + j : lo + j + rows, lanes] * tap[j : j + 1, :]
        centred = total - jnp.mean(total, axis=-1, keepdims=True)
        spread = jnp.mean(centred * centred, axis=-1, keepdims=True)
        unit = centred * lax.rsqrt(spread + norm_eps) * ggain[lanes].astype(f32)[None, :]
        mixed.append((unit * jax.nn.sigmoid(unit)).astype(bf16))
    mix = jnp.concatenate([head_out[...]] + mixed, axis=1)
    arrive(1)
    part = SIDE // TP
    for out, which in ((other, jnp.bitwise_xor(c, 1)), (mine, c)):
        wo = w[pl.ds(which * part, part), :, :, half:].reshape(depth // TP, half)
        out[...] = nt_dot(mix, wo).astype(bf16)


def per_device(
    tokens,
    norm_gain,
    query_down,
    query_gain,
    latent_down,
    latent_gain,
    rope_down,
    query_up,
    key_up,
    value_up,
    glu_value,
    glu_gate,
    conv_taps,
    group_gain,
    head_proj,
    channel_proj,
):
    tok = tokens.shape[0]
    sp = lax.axis_index("sp")
    vmem = pl.BlockSpec(memory_space=pltpu.VMEM)
    hbm = pl.BlockSpec(memory_space=pltpu.HBM)
    first, second = line_groups(0), line_groups(1)

    quarter = ROPE // 4
    inverse = rope_base ** (-jnp.arange(quarter, dtype=f32) / quarter)
    places = sp * tok + jnp.arange(tok, dtype=jnp.int32)
    grid_row = (places // GRID_W).astype(f32)
    grid_col = (places % GRID_W).astype(f32)
    angles = jnp.concatenate([grid_row[:, None] * inverse, grid_col[:, None] * inverse], axis=-1)
    cosine, sine = jnp.cos(angles), jnp.sin(angles)
    normed, sent = pl.pallas_call(
        pre_kernel,
        name="pre",
        out_shape=(
            jax.ShapeDtypeStruct(tokens.shape, bf16),
            jax.ShapeDtypeStruct((SIDE, PACK, 128), bf16),
        ),
        in_specs=[vmem] * 8,
        out_specs=(vmem, vmem),
        cost_estimate=pl.CostEstimate(flops=int(2e9), bytes_accessed=3 * 2**20, transcendentals=0),
    )(tokens, norm_gain, latent_down, latent_gain, rope_down.T, query_down, cosine, sine)
    own = lax.all_to_all(sent, MESH_AXES, 0, 0, axis_index_groups=first, tiled=True)

    spread = lax.all_gather(own, MESH_AXES, axis_index_groups=second, axis=0, tiled=True)

    rows_in = jnp.concatenate([glu_value, glu_gate, head_proj.T, channel_proj.T], axis=1)
    rows_in, own = lax.optimization_barrier((rows_in, own))
    sent = jnp.broadcast_to(rows_in[None], (SIDE,) + rows_in.shape)
    near = lax.all_to_all(sent, MESH_AXES, 0, 0, axis_index_groups=first, tiled=True)
    weights = lax.all_gather(near, MESH_AXES, axis_index_groups=second, axis=0, tiled=False)

    swap = [(0, 1), (1, 0)]
    theirs = lax.ppermute(spread, "tp", swap)

    heads = key_up.shape[1] // NOPE
    many = heads * tok
    total_keys = 2 * SIDE * SIDE * 64
    chunk = 1024
    head_out, log_weight = pl.pallas_call(
        attend_kernel,
        name="attend",
        out_shape=(
            jax.ShapeDtypeStruct((tok, heads * VDIM), bf16),
            jax.ShapeDtypeStruct((heads, tok), f32),
        ),
        in_specs=[vmem] * 9,
        out_specs=(vmem, vmem),
        scratch_shapes=[
            pltpu.VMEM((4, SIDE * SIDE, ROW, 128), bf16),
            pltpu.VMEM((tok, 512), f32),
            pltpu.VMEM((many, KVR + 128), bf16),
            pltpu.VMEM((total_keys, KVR + 128), bf16),
            pltpu.VMEM((many, chunk), f32),
            pltpu.VMEM((many, chunk), f32),
            pltpu.VMEM((many, chunk), bf16),
            pltpu.VMEM((many, 128), f32),
            pltpu.VMEM((many, 128), f32),
            pltpu.VMEM((many, KVR), f32),
        ],
        cost_estimate=pl.CostEstimate(flops=int(8e9), bytes_accessed=8 * 2**20, transcendentals=0),
    )(normed, spread, theirs, query_gain, query_up, key_up, value_up, cosine, sine)

    sp_count = lax.axis_size("sp")
    forward = [(i, i + 1) for i in range(sp_count - 1)]
    backward = [(i + 1, i) for i in range(sp_count - 1)]
    last, front, head_out = lax.optimization_barrier(
        (tokens[tok - EDGE :], tokens[:EDGE], head_out)
    )
    before = lax.ppermute(last, "sp", forward)
    after = lax.ppermute(front, "sp", backward)

    width = rows_in.shape[1]
    mine, other = pl.pallas_call(
        post_kernel,
        name="post",
        out_shape=(jax.ShapeDtypeStruct((tok, width // 2), bf16),) * 2,
        in_specs=[vmem] * 4 + [hbm] + [vmem] * 3,
        out_specs=(vmem, vmem),
        scratch_shapes=[
            pltpu.VMEM((SIDE, SIDE, ROW, width), bf16),
            pltpu.VMEM((tok + 2 * EDGE, tokens.shape[1]), bf16),
            pltpu.VMEM((tok + 2 * EDGE, width // 4), f32),
            pltpu.SemaphoreType.DMA((2 * SIDE,)),
        ],
        cost_estimate=pl.CostEstimate(flops=int(3e9), bytes_accessed=9 * 2**20, transcendentals=0),
    )(normed, before, after, norm_gain, weights, conv_taps, group_gain, head_out)
    arrived = lax.ppermute(other, "tp", swap)
    mixed_out = (mine.astype(f32) + arrived.astype(f32)).astype(bf16)
    return (mixed_out, log_weight)


def solution(mesh):
    in_specs = (
        P(("fs", "sp"), None),
        P(),
        P("sp", None),
        P(),
        P(),
        P(),
        P(),
        P(None, "tp"),
        P(None, "tp"),
        P(None, "tp"),
        P("sp", "tp"),
        P("sp", "tp"),
        P(None, "tp"),
        P("tp"),
        P("tp", "sp"),
        P("tp", "sp"),
    )
    out_specs = (P(("fs", "sp"), "tp"), P("tp", ("fs", "sp")))
    return jax.shard_map(
        per_device, mesh=mesh, in_specs=in_specs, out_specs=out_specs, check_vma=False
    )
```

```python
import jax
import jax.numpy as jnp
from jax import lax
from jax.experimental import pallas as pl
from jax.experimental.pallas import tpu as pltpu
from jax.sharding import PartitionSpec as P

NOPE = 128
ROPE = 64
VDIM = 128
KVR = 256
GROUP = 128
GRID_W = 64
EDGE = 16
SIDE = 8
FS = 4
TP = 2
ROW = 32
KEY_ROWS = 160
PACK = 224
FULL = 288
QUART = 256
MESH_AXES = ("sp", "fs", "tp")

norm_eps = 1e-06
rope_base = 10000.0
far_below = -1e30
LOG2E = 1.4426950408889634
LN2 = 0.6931471805599453

f32 = jnp.float32
bf16 = jnp.bfloat16


def flat(z, y, x, c):
    return ((z * SIDE + y) * FS + x) * TP + c


def line_groups(phase):
    groups = []
    for x in range(FS):
        for c in range(TP):
            for o in range(SIDE):
                if (c == 0) == (phase == 0):
                    groups.append([flat(o, i, x, c) for i in range(SIDE)])
                else:
                    groups.append([flat(i, o, x, c) for i in range(SIDE)])
    return groups


def nt_dot(a, b):
    return lax.dot_general(a, b, (((1,), (1,)), ((), ())), preferred_element_type=f32)


def nn_dot(a, b):
    return jnp.dot(a, b, preferred_element_type=f32)


def scaled(values, gain):
    inv = lax.rsqrt(jnp.mean(values * values, axis=-1, keepdims=True) + norm_eps)
    return values * inv * gain.astype(f32)[None, :]


def turned_half(raw):
    return jnp.concatenate([raw[:, ROPE // 2 :], raw[:, : ROPE // 2]], axis=1)


def doubled(cosv, sinv):
    return jnp.concatenate([cosv, cosv], axis=1), jnp.concatenate([-sinv, sinv], axis=1)


def place():
    sp = lax.axis_index("sp")
    return lax.div(sp, SIDE), lax.rem(sp, SIDE), lax.axis_index("tp")


def quarter_of(head, chan, q, h):
    at = pl.ds(pl.multiple_of(lax.rem(q, 2) * QUART + h * 128, 128), 128)
    return jnp.where(q < 2, head[:, at], chan[:, at])


def pre_kernel(
    tok, gain, ldown, lgain, rdown, qdown, head, chan, cosv, sinv, normed, pack
):
    half = tok.shape[0] // TP
    c = place()[2]
    normed[...] = scaled(tok[...].astype(f32), gain[...]).astype(bf16)
    start = pl.multiple_of(c * half, half)
    own = normed[pl.ds(start, half), :]
    latent = scaled(nn_dot(own, ldown[...]), lgain[...]).astype(bf16)
    raw = nt_dot(own, rdown[...])
    cos2, sin2 = doubled(cosv[pl.ds(start, half), :], sinv[pl.ds(start, half), :])
    key = raw * cos2 + turned_half(raw) * sin2
    pair = jnp.concatenate([key[: half // 2], key[half // 2 :]], axis=1).astype(bf16)
    q0 = qdown[:, pl.ds(pl.multiple_of(c * 256, 128), 128)]
    q1 = qdown[:, pl.ds(pl.multiple_of(c * 256 + 128, 128), 128)]
    x = lax.axis_index("fs")
    o0, o1 = (quarter_of(head, chan, x, h) for h in range(2))
    for i in range(SIDE):
        pack[i, 0:half, :] = latent[:, :128]
        pack[i, half : 2 * half, :] = latent[:, 128:]
        pack[i, 2 * half : KEY_ROWS, :] = pair
        pack[i, KEY_ROWS : KEY_ROWS + ROW, :] = q0
        pack[i, KEY_ROWS + ROW : PACK, :] = q1
        pack[i, PACK : PACK + ROW, :] = o0
        pack[i, PACK + ROW :, :] = o1


def pack_kernel(value, gate, head, chan, pack):
    far = lax.rem(lax.axis_index("fs") + 2, FS)
    ch = value.shape[1]
    parts = []
    for g in range(ch // GROUP):
        lanes = slice(g * GROUP, (g + 1) * GROUP)
        parts += [value[:, lanes], gate[:, lanes]]
    parts += [quarter_of(head, chan, far, h) for h in range(2)]
    row = jnp.concatenate(parts, axis=1)
    for i in range(SIDE):
        pack[i] = row


def attend_kernel(
    normed, mine, theirs, qgain, qup, kup, vup, cosv, sinv, head_out, logw,
    weight, lat, queries, keys, sa, sb, p, top, low, acc
):
    c = place()[2]
    blocks = SIDE * SIDE
    for src, kind in ((mine, c), (theirs, jnp.bitwise_xor(c, 1))):
        for b in range(SIDE):
            for o in range(SIDE):
                block = jnp.where(kind == 0, b * SIDE + o, o * SIDE + b)
                for h in range(2):
                    lo = KEY_ROWS + h * ROW
                    weight[kind * 2 + h, block] = src[b * SIDE + o, lo : lo + ROW, :]
    x = normed[...]
    for g in range(4):
        lat[:, g * 128 : (g + 1) * 128] = nn_dot(x, weight[g].reshape(blocks * ROW, 128))
    latent = scaled(lat[...], qgain[...]).astype(bf16)
    every = nn_dot(latent, qup[...])
    heads = kup.shape[1] // NOPE
    rows = normed.shape[0]
    cos2, sin2 = doubled(cosv[...], sinv[...])
    for h in range(heads):
        lo = h * (NOPE + ROPE)
        plain = every[:, lo : lo + NOPE].astype(bf16)
        raw = every[:, lo + NOPE : lo + NOPE + ROPE]
        rot = raw * cos2 + turned_half(raw) * sin2
        rot = jnp.concatenate([rot, jnp.zeros_like(rot)], axis=1).astype(bf16)
        absorbed = nt_dot(plain, kup[:, h * NOPE : (h + 1) * NOPE]).astype(bf16)
        queries[h * rows : (h + 1) * rows, :KVR] = absorbed
        queries[h * rows : (h + 1) * rows, KVR:] = rot

    per = SIDE * 64
    base = 0
    for src in (mine, theirs):
        count = src.shape[0] // SIDE

        def fill(i, carry, src=src, base=base):
            part = src[pl.ds(i * SIDE, SIDE)]
            to = pl.ds(pl.multiple_of((base + i) * per, per), per)
            keys[to, 0:128] = part[:, 0:64, :].reshape(per, 128)
            keys[to, 128:256] = part[:, 64:128, :].reshape(per, 128)
            near = part[:, 128:160, :].astype(f32)
            far = pltpu.roll(near.reshape(per // 2, 128), 64, 1).reshape(SIDE, 32, 128)
            both = jnp.concatenate([near, far], axis=1).reshape(per, 128)
            keys[to, 256:384] = both.astype(bf16)
            return carry

        lax.fori_loop(0, count, fill, 0)
        base += count
    top[...] = jnp.full_like(top, far_below)
    low[...] = jnp.zeros_like(low)
    acc[...] = jnp.zeros_like(acc)
    factor = LOG2E * (NOPE + ROPE) ** (-0.5)
    wide = sa.shape[1]
    steps = keys.shape[0] // wide
    total_rows = heads * rows

    def span(j):
        return pl.ds(pl.multiple_of(j * wide, wide), wide)

    def score(j, s):
        s[...] = nt_dot(queries[...], keys[span(j), :])

    def soften(j, s):
        fades = []
        for r in range(0, total_rows, 32):
            at = slice(r, r + 32)
            v = s[at, :]
            most = v[:, 0:128]
            for i in range(1, wide // 128):
                most = jnp.maximum(most, v[:, i * 128 : (i + 1) * 128])
            old = top[at, :]
            new = jnp.maximum(old, jnp.max(most, axis=1, keepdims=True))
            fade = jnp.exp2((old - new) * factor)
            part = low[at, :] * fade
            for i in range(wide // 128):
                e = jnp.exp2((v[:, i * 128 : (i + 1) * 128] - new) * factor)
                part = part + e
                p[at, i * 128 : (i + 1) * 128] = e.astype(bf16)
            low[at, :] = part
            top[at, :] = new
            acc[at, 0:128] = acc[at, 0:128] * fade
            acc[at, 128:256] = acc[at, 128:256] * fade
        acc[...] += nn_dot(p[...], keys[span(j), 0:KVR])

    score(0, sa)

    def pair(i, carry):
        score(2 * i + 1, sb)
        soften(2 * i, sa)
        score(jnp.minimum(2 * i + 2, steps - 1), sa)
        soften(2 * i + 1, sb)
        return carry

    lax.fori_loop(0, steps // 2, pair, 0)
    for h in range(heads):
        at = slice(h * rows, (h + 1) * rows)
        total = jnp.sum(low[at, :], axis=1, keepdims=True)
        attended = (acc[at, :] / total).astype(bf16)
        out = nn_dot(attended, vup[:, h * VDIM : (h + 1) * VDIM])
        head_out[:, h * VDIM : (h + 1) * VDIM] = out.astype(bf16)
        logs = top[at, :] * (factor * LN2) + jnp.log(total)
        logw[h : h + 1, :] = jnp.transpose(logs)[0:1, :]


def post_kernel(
    normed, before, after, gain, w_any, own_any, up_any, down_any, taps, ggain, head_out,
    mine, other, w, wo, wide, gated, sems
):
    c = place()[2]
    x = lax.axis_index("fs")
    rows = normed.shape[0]
    groups = gated.shape[1] // GROUP
    depth = SIDE * SIDE * ROW

    def copies(core):
        made = []

        def add(src, to):
            made.append(pltpu.make_async_copy(src, to, sems.at[len(made)]))

        def spot(ref, j, lanes):
            return ref.at[j, :, :, lanes] if core == 0 else ref.at[:, j, :, lanes]

        for g in range(groups):
            lanes = pl.ds(2 * GROUP * g, 2 * GROUP)
            for j in range(SIDE):
                add(w_any.at[j, :, :, lanes], spot(w, j, lanes))
        for step, src, lo in ((0, own_any, PACK), (3, up_any, 0), (1, down_any, 0)):
            to = wo.at[lax.rem(x + step, FS)]
            for h in range(2):
                for j in range(SIDE):
                    part = src.at[pl.ds(j * SIDE, SIDE), pl.ds(lo + h * ROW, ROW), :]
                    add(part, spot(to, j, pl.ds(h * 128, 128)))
        to = wo.at[lax.rem(x + 2, FS)]
        for j in range(SIDE):
            part = w_any.at[j, :, :, pl.ds(2 * GROUP * groups, QUART)]
            add(part, spot(to, j, pl.ds(0, QUART)))
        return made

    for core in range(TP):

        @pl.when(c == core)
        def _(core=core):
            for copy in copies(core):
                copy.start()

    pending = copies(0)

    wide[0:EDGE, :] = scaled(before[...].astype(f32), gain[...]).astype(bf16)
    wide[EDGE : EDGE + rows, :] = normed[...]
    wide[EDGE + rows :, :] = scaled(after[...].astype(f32), gain[...]).astype(bf16)
    full = wide[...]
    for g in range(groups):
        lanes = pl.ds(2 * GROUP * g, 2 * GROUP)
        for j in range(SIDE):
            pending[g * SIDE + j].wait()
        both = nn_dot(full, w[:, :, :, lanes].reshape(depth, 2 * GROUP))
        value, gate = both[:, :GROUP], both[:, GROUP:]
        spot = slice(g * GROUP, (g + 1) * GROUP)
        gated[:, spot] = (value * jax.nn.sigmoid(gate)).astype(bf16).astype(f32)
    mixed = []
    reach = taps.shape[0] // 2
    for g in range(groups):
        lanes = slice(g * GROUP, (g + 1) * GROUP)
        tap = taps[:, lanes].astype(f32)
        lo = EDGE - reach
        total = gated[lo : lo + rows, lanes] * tap[0:1, :]
        for j in range(1, taps.shape[0]):
            total = total + gated[lo + j : lo + j + rows, lanes] * tap[j : j + 1, :]
        centred = total - jnp.mean(total, axis=-1, keepdims=True)
        spread = jnp.mean(centred * centred, axis=-1, keepdims=True)
        unit = centred * lax.rsqrt(spread + norm_eps) * ggain[lanes].astype(f32)[None, :]
        mixed.append((unit * jax.nn.sigmoid(unit)).astype(bf16))
    mix = jnp.concatenate([head_out[...]] + mixed, axis=1)
    for copy in pending[groups * SIDE :]:
        copy.wait()
    part = SIDE // TP
    for out, which in ((other, jnp.bitwise_xor(c, 1)), (mine, c)):
        total = None
        for q in range(FS):
            wq = wo[q, pl.ds(which * part, part)].reshape(depth // TP, QUART)
            term = nt_dot(mix[:, q * QUART : (q + 1) * QUART], wq)
            total = term if total is None else total + term
        out[...] = total.astype(bf16)


def per_device(
    tokens,
    norm_gain,
    query_down,
    query_gain,
    latent_down,
    latent_gain,
    rope_down,
    query_up,
    key_up,
    value_up,
    glu_value,
    glu_gate,
    conv_taps,
    group_gain,
    head_proj,
    channel_proj,
):
    tok = tokens.shape[0]
    sp = lax.axis_index("sp")
    vmem = pl.BlockSpec(memory_space=pltpu.VMEM)
    hbm = pl.BlockSpec(memory_space=pltpu.HBM)
    first, second = line_groups(0), line_groups(1)
    head_t, chan_t = head_proj.T, channel_proj.T

    quarter = ROPE // 4
    inverse = rope_base ** (-jnp.arange(quarter, dtype=f32) / quarter)
    places = sp * tok + jnp.arange(tok, dtype=jnp.int32)
    grid_row = (places // GRID_W).astype(f32)
    grid_col = (places % GRID_W).astype(f32)
    angles = jnp.concatenate([grid_row[:, None] * inverse, grid_col[:, None] * inverse], axis=-1)
    cosine, sine = jnp.cos(angles), jnp.sin(angles)
    normed, sent = pl.pallas_call(
        pre_kernel,
        name="pre",
        out_shape=(
            jax.ShapeDtypeStruct(tokens.shape, bf16),
            jax.ShapeDtypeStruct((SIDE, FULL, 128), bf16),
        ),
        in_specs=[vmem] * 10,
        out_specs=(vmem, vmem),
        cost_estimate=pl.CostEstimate(flops=int(2e9), bytes_accessed=3 * 2**20, transcendentals=0),
    )(tokens, norm_gain, latent_down, latent_gain, rope_down.T, query_down, head_t, chan_t, cosine, sine)
    own = lax.all_to_all(sent, MESH_AXES, 0, 0, axis_index_groups=first, tiled=True)

    spread = lax.all_gather(own, MESH_AXES, axis_index_groups=second, axis=0, tiled=True)

    value, gate, own = lax.optimization_barrier((glu_value, glu_gate, own))
    width = 2 * glu_value.shape[1] + QUART
    sent = pl.pallas_call(
        pack_kernel,
        name="pack",
        out_shape=jax.ShapeDtypeStruct((SIDE, ROW, width), bf16),
        in_specs=[vmem] * 4,
        out_specs=vmem,
    )(value, gate, head_t, chan_t)
    near = lax.all_to_all(sent, MESH_AXES, 0, 0, axis_index_groups=first, tiled=True)
    weights = lax.all_gather(near, MESH_AXES, axis_index_groups=second, axis=0, tiled=False)

    swap = [(0, 1), (1, 0)]
    theirs = lax.ppermute(spread, "tp", swap)
    fourth = spread[:, PACK:, :]
    up = lax.ppermute(fourth, "fs", [(i, (i + 1) % FS) for i in range(FS)])
    down = lax.ppermute(fourth, "fs", [((i + 1) % FS, i) for i in range(FS)])

    heads = key_up.shape[1] // NOPE
    many = heads * tok
    total_keys = 2 * SIDE * SIDE * 64
    chunk = 1024
    head_out, log_weight = pl.pallas_call(
        attend_kernel,
        name="attend",
        out_shape=(
            jax.ShapeDtypeStruct((tok, heads * VDIM), bf16),
            jax.ShapeDtypeStruct((heads, tok), f32),
        ),
        in_specs=[vmem] * 9,
        out_specs=(vmem, vmem),
        scratch_shapes=[
            pltpu.VMEM((4, SIDE * SIDE, ROW, 128), bf16),
            pltpu.VMEM((tok, 512), f32),
            pltpu.VMEM((many, KVR + 128), bf16),
            pltpu.VMEM((total_keys, KVR + 128), bf16),
            pltpu.VMEM((many, chunk), f32),
            pltpu.VMEM((many, chunk), f32),
            pltpu.VMEM((many, chunk), bf16),
            pltpu.VMEM((many, 128), f32),
            pltpu.VMEM((many, 128), f32),
            pltpu.VMEM((many, KVR), f32),
        ],
        cost_estimate=pl.CostEstimate(flops=int(8e9), bytes_accessed=8 * 2**20, transcendentals=0),
    )(normed, spread, theirs, query_gain, query_up, key_up, value_up, cosine, sine)

    sp_count = lax.axis_size("sp")
    forward = [(i, i + 1) for i in range(sp_count - 1)]
    backward = [(i + 1, i) for i in range(sp_count - 1)]
    last, front, head_out = lax.optimization_barrier(
        (tokens[tok - EDGE :], tokens[:EDGE], head_out)
    )
    before = lax.ppermute(last, "sp", forward)
    after = lax.ppermute(front, "sp", backward)

    ch = glu_value.shape[1]
    half_out = tokens.shape[1] // TP
    mine, other = pl.pallas_call(
        post_kernel,
        name="post",
        out_shape=(jax.ShapeDtypeStruct((tok, half_out), bf16),) * 2,
        in_specs=[vmem] * 4 + [hbm] * 4 + [vmem] * 3,
        out_specs=(vmem, vmem),
        scratch_shapes=[
            pltpu.VMEM((SIDE, SIDE, ROW, 2 * ch), bf16),
            pltpu.VMEM((FS, SIDE, SIDE, ROW, QUART), bf16),
            pltpu.VMEM((tok + 2 * EDGE, tokens.shape[1]), bf16),
            pltpu.VMEM((tok + 2 * EDGE, ch), f32),
            pltpu.SemaphoreType.DMA((128,)),
        ],
        cost_estimate=pl.CostEstimate(flops=int(3e9), bytes_accessed=9 * 2**20, transcendentals=0),
    )(
        normed, before, after, norm_gain, weights, spread, up, down, conv_taps, group_gain, head_out
    )
    arrived = lax.ppermute(other, "tp", swap)
    mixed_out = (mine.astype(f32) + arrived.astype(f32)).astype(bf16)
    return (mixed_out, log_weight)


def solution(mesh):
    in_specs = (
        P(("fs", "sp"), None),
        P(),
        P("sp", None),
        P(),
        P(),
        P(),
        P(),
        P(None, "tp"),
        P(None, "tp"),
        P(None, "tp"),
        P("sp", "tp"),
        P("sp", "tp"),
        P(None, "tp"),
        P("tp"),
        P("tp", "sp"),
        P("tp", "sp"),
    )
    out_specs = (P(("fs", "sp"), "tp"), P("tp", ("fs", "sp")))
    return jax.shard_map(
        per_device, mesh=mesh, in_specs=in_specs, out_specs=out_specs, check_vma=False
    )
```

```python
import jax
import jax.numpy as jnp
from jax import lax
from jax.experimental import pallas as pl
from jax.experimental.pallas import tpu as pltpu
from jax.sharding import PartitionSpec as P

NOPE = 128
ROPE = 64
VDIM = 128
KVR = 256
GROUP = 128
GRID_W = 64
EDGE = 16
SIDE = 8
FS = 4
TP = 2
ROW = 32
KEY_ROWS = 160
PACK = 224
FULL = 288
QUART = 256
MESH_AXES = ("sp", "fs", "tp")

norm_eps = 1e-06
rope_base = 10000.0
far_below = -1e30
LOG2E = 1.4426950408889634
LN2 = 0.6931471805599453

f32 = jnp.float32
bf16 = jnp.bfloat16


def flat(z, y, x, c):
    return ((z * SIDE + y) * FS + x) * TP + c


def line_groups(phase):
    groups = []
    for x in range(FS):
        for c in range(TP):
            for o in range(SIDE):
                if (c == 0) == (phase == 0):
                    groups.append([flat(o, i, x, c) for i in range(SIDE)])
                else:
                    groups.append([flat(i, o, x, c) for i in range(SIDE)])
    return groups


def nt_dot(a, b):
    return lax.dot_general(a, b, (((1,), (1,)), ((), ())), preferred_element_type=f32)


def nn_dot(a, b):
    return jnp.dot(a, b, preferred_element_type=f32)


def scaled(values, gain):
    inv = lax.rsqrt(jnp.mean(values * values, axis=-1, keepdims=True) + norm_eps)
    return values * inv * gain.astype(f32)[None, :]


def turned_half(raw):
    return jnp.concatenate([raw[:, ROPE // 2 :], raw[:, : ROPE // 2]], axis=1)


def doubled(cosv, sinv):
    return jnp.concatenate([cosv, cosv], axis=1), jnp.concatenate([-sinv, sinv], axis=1)


def place():
    sp = lax.axis_index("sp")
    return lax.div(sp, SIDE), lax.rem(sp, SIDE), lax.axis_index("tp")


def quarter_of(head, chan, q, h):
    at = pl.ds(pl.multiple_of(lax.rem(q, 2) * QUART + h * 128, 128), 128)
    return jnp.where(q < 2, head[:, at], chan[:, at])


def pre_kernel(
    tok, gain, ldown, lgain, rdown, qdown, head, chan, cosv, sinv, normed, pack
):
    half = tok.shape[0] // TP
    c = place()[2]
    normed[...] = scaled(tok[...].astype(f32), gain[...]).astype(bf16)
    start = pl.multiple_of(c * half, half)
    own = normed[pl.ds(start, half), :]
    latent = scaled(nn_dot(own, ldown[...]), lgain[...]).astype(bf16)
    raw = nt_dot(own, rdown[...])
    cos2, sin2 = doubled(cosv[pl.ds(start, half), :], sinv[pl.ds(start, half), :])
    key = raw * cos2 + turned_half(raw) * sin2
    pair = jnp.concatenate([key[: half // 2], key[half // 2 :]], axis=1).astype(bf16)
    q0 = qdown[:, pl.ds(pl.multiple_of(c * 256, 128), 128)]
    q1 = qdown[:, pl.ds(pl.multiple_of(c * 256 + 128, 128), 128)]
    x = lax.axis_index("fs")
    o0, o1 = (quarter_of(head, chan, x, h) for h in range(2))
    for i in range(SIDE):
        pack[i, 0:half, :] = latent[:, :128]
        pack[i, half : 2 * half, :] = latent[:, 128:]
        pack[i, 2 * half : KEY_ROWS, :] = pair
        pack[i, KEY_ROWS : KEY_ROWS + ROW, :] = q0
        pack[i, KEY_ROWS + ROW : PACK, :] = q1
        pack[i, PACK : PACK + ROW, :] = o0
        pack[i, PACK + ROW :, :] = o1


def pack_kernel(value, gate, head, chan, pack):
    far = lax.rem(lax.axis_index("fs") + 2, FS)
    at = pl.ds(pl.multiple_of(lax.axis_index("fs") * GROUP, GROUP), GROUP)
    parts = [value[:, at], gate[:, at]]
    parts += [quarter_of(head, chan, far, h) for h in range(2)]
    row = jnp.concatenate(parts, axis=1)
    for i in range(SIDE):
        pack[i] = row


def edge_kernel(normed, before, after, gain, spread):
    c = place()[2]
    half = normed.shape[0] // TP
    edge = jnp.where(c == 0, before[...], after[...]).astype(f32)
    edge = scaled(edge, gain[...]).astype(bf16)
    main = normed[pl.ds(pl.multiple_of(c * half, half), half), :]
    for i in range(FS):
        spread[i, :half, :] = main
        spread[i, half:, :] = edge


def attend_kernel(
    normed, mine, theirs, qgain, qup, kup, vup, cosv, sinv, head_out, logw,
    weight, lat, queries, keys, sa, sb, p, top, low, acc
):
    c = place()[2]
    blocks = SIDE * SIDE
    for src, kind in ((mine, c), (theirs, jnp.bitwise_xor(c, 1))):
        for b in range(SIDE):
            for o in range(SIDE):
                block = jnp.where(kind == 0, b * SIDE + o, o * SIDE + b)
                for h in range(2):
                    lo = KEY_ROWS + h * ROW
                    weight[kind * 2 + h, block] = src[b * SIDE + o, lo : lo + ROW, :]
    x = normed[...]
    for g in range(4):
        lat[:, g * 128 : (g + 1) * 128] = nn_dot(x, weight[g].reshape(blocks * ROW, 128))
    latent = scaled(lat[...], qgain[...]).astype(bf16)
    every = nn_dot(latent, qup[...])
    heads = kup.shape[1] // NOPE
    rows = normed.shape[0]
    cos2, sin2 = doubled(cosv[...], sinv[...])
    for h in range(heads):
        lo = h * (NOPE + ROPE)
        plain = every[:, lo : lo + NOPE].astype(bf16)
        raw = every[:, lo + NOPE : lo + NOPE + ROPE]
        rot = raw * cos2 + turned_half(raw) * sin2
        rot = jnp.concatenate([rot, jnp.zeros_like(rot)], axis=1).astype(bf16)
        absorbed = nt_dot(plain, kup[:, h * NOPE : (h + 1) * NOPE]).astype(bf16)
        queries[h * rows : (h + 1) * rows, :KVR] = absorbed
        queries[h * rows : (h + 1) * rows, KVR:] = rot

    per = SIDE * 64
    base = 0
    for src in (mine, theirs):
        count = src.shape[0] // SIDE

        def fill(i, carry, src=src, base=base):
            part = src[pl.ds(i * SIDE, SIDE)]
            to = pl.ds(pl.multiple_of((base + i) * per, per), per)
            keys[to, 0:128] = part[:, 0:64, :].reshape(per, 128)
            keys[to, 128:256] = part[:, 64:128, :].reshape(per, 128)
            near = part[:, 128:160, :].astype(f32)
            far = pltpu.roll(near.reshape(per // 2, 128), 64, 1).reshape(SIDE, 32, 128)
            both = jnp.concatenate([near, far], axis=1).reshape(per, 128)
            keys[to, 256:384] = both.astype(bf16)
            return carry

        lax.fori_loop(0, count, fill, 0)
        base += count
    top[...] = jnp.full_like(top, far_below)
    low[...] = jnp.zeros_like(low)
    acc[...] = jnp.zeros_like(acc)
    factor = LOG2E * (NOPE + ROPE) ** (-0.5)
    wide = sa.shape[1]
    steps = keys.shape[0] // wide
    total_rows = heads * rows

    def span(j):
        return pl.ds(pl.multiple_of(j * wide, wide), wide)

    def score(j, s):
        s[...] = nt_dot(queries[...], keys[span(j), :])

    def soften(j, s):
        fades = []
        for r in range(0, total_rows, 32):
            at = slice(r, r + 32)
            v = s[at, :]
            most = v[:, 0:128]
            for i in range(1, wide // 128):
                most = jnp.maximum(most, v[:, i * 128 : (i + 1) * 128])
            old = top[at, :]
            new = jnp.maximum(old, jnp.max(most, axis=1, keepdims=True))
            fade = jnp.exp2((old - new) * factor)
            part = low[at, :] * fade
            for i in range(wide // 128):
                e = jnp.exp2((v[:, i * 128 : (i + 1) * 128] - new) * factor)
                part = part + e
                p[at, i * 128 : (i + 1) * 128] = e.astype(bf16)
            low[at, :] = part
            top[at, :] = new
            acc[at, 0:128] = acc[at, 0:128] * fade
            acc[at, 128:256] = acc[at, 128:256] * fade
        acc[...] += nn_dot(p[...], keys[span(j), 0:KVR])

    score(0, sa)

    def pair(i, carry):
        score(2 * i + 1, sb)
        soften(2 * i, sa)
        score(jnp.minimum(2 * i + 2, steps - 1), sa)
        soften(2 * i + 1, sb)
        return carry

    lax.fori_loop(0, steps // 2, pair, 0)
    for h in range(heads):
        at = slice(h * rows, (h + 1) * rows)
        total = jnp.sum(low[at, :], axis=1, keepdims=True)
        attended = (acc[at, :] / total).astype(bf16)
        out = nn_dot(attended, vup[:, h * VDIM : (h + 1) * VDIM])
        head_out[:, h * VDIM : (h + 1) * VDIM] = out.astype(bf16)
        logs = top[at, :] * (factor * LN2) + jnp.log(total)
        logw[h : h + 1, :] = jnp.transpose(logs)[0:1, :]


def spot(core, ref, j, lanes):
    return ref.at[j, :, :, lanes] if core == 0 else ref.at[:, j, :, lanes]


def launch(c, copies):
    for core in range(TP):

        @pl.when(c == core)
        def _(core=core):
            for copy in copies(core):
                copy.start()

    return copies(0)


def conv_kernel(x_own, x_other, w_any, taps, ggain, out, w, gated, sems):
    c = place()[2]
    x = lax.axis_index("fs")
    wide = 2 * GROUP
    depth = SIDE * SIDE * ROW
    parts, rows, _ = x_own.shape
    half = rows - EDGE

    def copies(core):
        lanes = pl.ds(0, wide)
        return [
            pltpu.make_async_copy(w_any.at[j, :, :, lanes], spot(core, w, j, lanes), sems.at[j])
            for j in range(SIDE)
        ]

    for copy in launch(c, copies):
        copy.wait()
    weight = w[...].reshape(depth, wide)
    for src, owner in ((x_own, c), (x_other, jnp.bitwise_xor(c, 1))):
        both = nn_dot(src[...].reshape(parts * rows, src.shape[2]), weight)
        value = both[:, :GROUP] * jax.nn.sigmoid(both[:, GROUP:])
        value = value.astype(bf16).astype(f32).reshape(parts, rows, GROUP)
        main = pl.multiple_of(EDGE + owner * half, 8)
        side = pl.multiple_of(owner * (EDGE + 2 * half), 8)
        gated[:, pl.ds(main, half), :] = value[:, :half, :]
        gated[:, pl.ds(side, EDGE), :] = value[:, half:, :]
    lanes = pl.ds(pl.multiple_of(x * GROUP, GROUP), GROUP)
    tap = taps[:, lanes].astype(f32)
    gain = ggain[:, lanes].astype(f32)
    lo = EDGE - taps.shape[0] // 2
    tok = 2 * half
    for p in range(parts):
        total = gated[p, lo : lo + tok, :] * tap[0:1, :]
        for j in range(1, taps.shape[0]):
            total = total + gated[p, lo + j : lo + j + tok, :] * tap[j : j + 1, :]
        centred = total - jnp.mean(total, axis=-1, keepdims=True)
        spread = jnp.mean(centred * centred, axis=-1, keepdims=True)
        unit = centred * lax.rsqrt(spread + norm_eps) * gain
        out[p] = (unit * jax.nn.sigmoid(unit)).astype(bf16)


def post_kernel(head_out, conv, w_any, own_any, up_any, down_any, mine, other, wo, sems):
    c = place()[2]
    x = lax.axis_index("fs")
    depth = SIDE * SIDE * ROW

    def copies(core):
        made = []

        def add(src, to):
            made.append(pltpu.make_async_copy(src, to, sems.at[len(made)]))

        for step, src, lo in ((0, own_any, PACK), (3, up_any, 0), (1, down_any, 0)):
            to = wo.at[lax.rem(x + step, FS)]
            for h in range(2):
                for j in range(SIDE):
                    part = src.at[pl.ds(j * SIDE, SIDE), pl.ds(lo + h * ROW, ROW), :]
                    add(part, spot(core, to, j, pl.ds(h * 128, 128)))
        to = wo.at[lax.rem(x + 2, FS)]
        for j in range(SIDE):
            part = w_any.at[j, :, :, pl.ds(2 * GROUP, QUART)]
            add(part, spot(core, to, j, pl.ds(0, QUART)))
        return made

    pending = launch(c, copies)
    mix = [head_out[:, :QUART], head_out[:, QUART:]]
    mix += [jnp.concatenate([conv[2 * i], conv[2 * i + 1]], axis=1) for i in range(2)]
    for copy in pending:
        copy.wait()
    part = SIDE // TP
    for out, which in ((other, jnp.bitwise_xor(c, 1)), (mine, c)):
        total = None
        for q in range(FS):
            wq = wo[q, pl.ds(which * part, part)].reshape(depth // TP, QUART)
            term = nt_dot(mix[q], wq)
            total = term if total is None else total + term
        out[...] = total.astype(bf16)


def per_device(
    tokens,
    norm_gain,
    query_down,
    query_gain,
    latent_down,
    latent_gain,
    rope_down,
    query_up,
    key_up,
    value_up,
    glu_value,
    glu_gate,
    conv_taps,
    group_gain,
    head_proj,
    channel_proj,
):
    tok = tokens.shape[0]
    sp = lax.axis_index("sp")
    vmem = pl.BlockSpec(memory_space=pltpu.VMEM)
    hbm = pl.BlockSpec(memory_space=pltpu.HBM)
    first, second = line_groups(0), line_groups(1)
    head_t, chan_t = head_proj.T, channel_proj.T

    quarter = ROPE // 4
    inverse = rope_base ** (-jnp.arange(quarter, dtype=f32) / quarter)
    places = sp * tok + jnp.arange(tok, dtype=jnp.int32)
    grid_row = (places // GRID_W).astype(f32)
    grid_col = (places % GRID_W).astype(f32)
    angles = jnp.concatenate([grid_row[:, None] * inverse, grid_col[:, None] * inverse], axis=-1)
    cosine, sine = jnp.cos(angles), jnp.sin(angles)
    normed, sent = pl.pallas_call(
        pre_kernel,
        name="pre",
        out_shape=(
            jax.ShapeDtypeStruct(tokens.shape, bf16),
            jax.ShapeDtypeStruct((SIDE, FULL, 128), bf16),
        ),
        in_specs=[vmem] * 10,
        out_specs=(vmem, vmem),
        cost_estimate=pl.CostEstimate(flops=int(2e9), bytes_accessed=3 * 2**20, transcendentals=0),
    )(tokens, norm_gain, latent_down, latent_gain, rope_down.T, query_down, head_t, chan_t, cosine, sine)
    own = lax.all_to_all(sent, MESH_AXES, 0, 0, axis_index_groups=first, tiled=True)

    spread = lax.all_gather(own, MESH_AXES, axis_index_groups=second, axis=0, tiled=True)

    value, gate, own = lax.optimization_barrier((glu_value, glu_gate, own))
    width = 2 * GROUP + QUART
    sent = pl.pallas_call(
        pack_kernel,
        name="pack",
        out_shape=jax.ShapeDtypeStruct((SIDE, ROW, width), bf16),
        in_specs=[vmem] * 4,
        out_specs=vmem,
    )(value, gate, head_t, chan_t)
    near = lax.all_to_all(sent, MESH_AXES, 0, 0, axis_index_groups=first, tiled=True)
    last, front, near = lax.optimization_barrier((tokens[tok - EDGE :], tokens[:EDGE], near))
    weights = lax.all_gather(near, MESH_AXES, axis_index_groups=second, axis=0, tiled=False)

    swap = [(0, 1), (1, 0)]
    sp_count = lax.axis_size("sp")
    before = lax.ppermute(last, "sp", [(i, i + 1) for i in range(sp_count - 1)])
    after = lax.ppermute(front, "sp", [(i + 1, i) for i in range(sp_count - 1)])
    rows_x = tok // TP + EDGE
    spread_x = pl.pallas_call(
        edge_kernel,
        name="edge",
        out_shape=jax.ShapeDtypeStruct((FS, rows_x, tokens.shape[1]), bf16),
        in_specs=[vmem] * 4,
        out_specs=vmem,
    )(normed, before, after, norm_gain)
    x_own = lax.all_to_all(spread_x, "fs", 0, 0, tiled=True)
    spread, x_own = lax.optimization_barrier((spread, x_own))
    theirs = lax.ppermute(spread, "tp", swap)
    x_other = lax.ppermute(x_own, "tp", swap)
    fourth = spread[:, PACK:, :]
    up = lax.ppermute(fourth, "fs", [(i, (i + 1) % FS) for i in range(FS)])
    down = lax.ppermute(fourth, "fs", [((i + 1) % FS, i) for i in range(FS)])

    heads = key_up.shape[1] // NOPE
    many = heads * tok
    total_keys = 2 * SIDE * SIDE * 64
    chunk = 1024
    head_out, log_weight = pl.pallas_call(
        attend_kernel,
        name="attend",
        out_shape=(
            jax.ShapeDtypeStruct((tok, heads * VDIM), bf16),
            jax.ShapeDtypeStruct((heads, tok), f32),
        ),
        in_specs=[vmem] * 9,
        out_specs=(vmem, vmem),
        scratch_shapes=[
            pltpu.VMEM((4, SIDE * SIDE, ROW, 128), bf16),
            pltpu.VMEM((tok, 512), f32),
            pltpu.VMEM((many, KVR + 128), bf16),
            pltpu.VMEM((total_keys, KVR + 128), bf16),
            pltpu.VMEM((many, chunk), f32),
            pltpu.VMEM((many, chunk), f32),
            pltpu.VMEM((many, chunk), bf16),
            pltpu.VMEM((many, 128), f32),
            pltpu.VMEM((many, 128), f32),
            pltpu.VMEM((many, KVR), f32),
        ],
        cost_estimate=pl.CostEstimate(flops=int(8e9), bytes_accessed=8 * 2**20, transcendentals=0),
    )(normed, spread, theirs, query_gain, query_up, key_up, value_up, cosine, sine)

    x_own, x_other, head_out = lax.optimization_barrier((x_own, x_other, head_out))
    conv = pl.pallas_call(
        conv_kernel,
        name="conv",
        out_shape=jax.ShapeDtypeStruct((FS, tok, GROUP), bf16),
        in_specs=[vmem, vmem, hbm, vmem, vmem],
        out_specs=vmem,
        scratch_shapes=[
            pltpu.VMEM((SIDE, SIDE, ROW, 2 * GROUP), bf16),
            pltpu.VMEM((FS, tok + 2 * EDGE, GROUP), f32),
            pltpu.SemaphoreType.DMA((SIDE,)),
        ],
        cost_estimate=pl.CostEstimate(flops=int(3e9), bytes_accessed=9 * 2**20, transcendentals=0),
    )(x_own, x_other, weights, conv_taps, group_gain[None])
    conv = lax.all_to_all(conv, "fs", 0, 0, tiled=True)

    half_out = tokens.shape[1] // TP
    mine, other = pl.pallas_call(
        post_kernel,
        name="post",
        out_shape=(jax.ShapeDtypeStruct((tok, half_out), bf16),) * 2,
        in_specs=[vmem] * 2 + [hbm] * 4,
        out_specs=(vmem, vmem),
        scratch_shapes=[
            pltpu.VMEM((FS, SIDE, SIDE, ROW, QUART), bf16),
            pltpu.SemaphoreType.DMA((64,)),
        ],
        cost_estimate=pl.CostEstimate(flops=int(3e9), bytes_accessed=9 * 2**20, transcendentals=0),
    )(head_out, conv, weights, spread, up, down)
    arrived = lax.ppermute(other, "tp", swap)
    mixed_out = (mine.astype(f32) + arrived.astype(f32)).astype(bf16)
    return (mixed_out, log_weight)


def solution(mesh):
    in_specs = (
        P(("fs", "sp"), None),
        P(),
        P("sp", None),
        P(),
        P(),
        P(),
        P(),
        P(None, "tp"),
        P(None, "tp"),
        P(None, "tp"),
        P("sp", "tp"),
        P("sp", "tp"),
        P(None, "tp"),
        P("tp"),
        P("tp", "sp"),
        P("tp", "sp"),
    )
    out_specs = (P(("fs", "sp"), "tp"), P("tp", ("fs", "sp")))
    return jax.shard_map(
        per_device, mesh=mesh, in_specs=in_specs, out_specs=out_specs, check_vma=False
    )
```

```python
import jax
import jax.numpy as jnp
from jax import lax
from jax.experimental import pallas as pl
from jax.experimental.pallas import tpu as pltpu
from jax.sharding import PartitionSpec as P

NOPE = 128
ROPE = 64
VDIM = 128
KVR = 256
GROUP = 128
GRID_W = 64
EDGE = 16
SIDE = 8
FS = 4
TP = 2
ROW = 32
QUERY_AT = 5
OUT_AT = 7
KEY_TILES = 9
GLU_TILES = 8
TILES = 19
QUART = 256
OFFSETS = (0, -1, 1, -2, 2, -3, 3, -4)
MESH_AXES = ("sp", "fs", "tp")

norm_eps = 1e-06
rope_base = 10000.0
far_below = -1e30
LOG2E = 1.4426950408889634
LN2 = 0.6931471805599453

f32 = jnp.float32
bf16 = jnp.bfloat16


def flat(z, y, x, c):
    return ((z * SIDE + y) * FS + x) * TP + c


def line_groups(phase):
    groups = []
    for x in range(FS):
        for c in range(TP):
            for o in range(SIDE):
                if (c == 0) == (phase == 0):
                    groups.append([flat(o, i, x, c) for i in range(SIDE)])
                else:
                    groups.append([flat(i, o, x, c) for i in range(SIDE)])
    return groups


def line_pairs(step):
    pairs = []
    for group in line_groups(1):
        pairs += [(group[i], group[(i + step) % SIDE]) for i in range(SIDE)]
    return pairs


def hop(block, step):
    return lax.ppermute(block, MESH_AXES, line_pairs(step))


def rings(owns):
    ups, downs = list(owns), list(owns)
    got = [[own] for own in owns]
    half = SIDE // 2
    for step in range(1, half + 1):
        for i in range(len(owns)):
            last = step == half
            ups[i] = hop(ups[i][:half] if last else ups[i], 1)
            downs[i] = hop(downs[i][half:] if last else downs[i], -1)
            got[i] += [ups[i], downs[i]]
    return [jnp.concatenate(g, axis=0) for g in got]


def nt_dot(a, b):
    return lax.dot_general(a, b, (((1,), (1,)), ((), ())), preferred_element_type=f32)


def nn_dot(a, b):
    return jnp.dot(a, b, preferred_element_type=f32)


def scaled(values, gain):
    inv = lax.rsqrt(jnp.mean(values * values, axis=-1, keepdims=True) + norm_eps)
    return values * inv * gain.astype(f32)[None, :]


def turned_half(raw):
    return jnp.concatenate([raw[:, ROPE // 2 :], raw[:, : ROPE // 2]], axis=1)


def doubled(cosv, sinv):
    return jnp.concatenate([cosv, cosv], axis=1), jnp.concatenate([-sinv, sinv], axis=1)


def place():
    sp = lax.axis_index("sp")
    return lax.div(sp, SIDE), lax.rem(sp, SIDE), lax.axis_index("tp")


def quarter_of(head, chan, q, h):
    at = pl.ds(pl.multiple_of(lax.rem(q, 2) * QUART + h * 128, 128), 128)
    return jnp.where(q < 2, head[:, at], chan[:, at])


def pre_kernel(
    tok, gain, ldown, lgain, rdown, qdown, value, gate, head, chan, cosv, sinv, normed, pack
):
    half = tok.shape[0] // TP
    c = place()[2]
    normed[...] = scaled(tok[...].astype(f32), gain[...]).astype(bf16)
    start = pl.multiple_of(c * half, half)
    own = normed[pl.ds(start, half), :]
    latent = scaled(nn_dot(own, ldown[...]), lgain[...]).astype(bf16)
    raw = nt_dot(own, rdown[...])
    cos2, sin2 = doubled(cosv[pl.ds(start, half), :], sinv[pl.ds(start, half), :])
    key = raw * cos2 + turned_half(raw) * sin2
    pair = jnp.concatenate([key[: half // 2], key[half // 2 :]], axis=1).astype(bf16)
    x = lax.axis_index("fs")
    tiles = []
    for j in range(2):
        for i in range(2):
            tiles.append(latent[i * ROW : (i + 1) * ROW, j * 128 : (j + 1) * 128])
    tiles.append(pair)
    tiles += [qdown[:, pl.ds(pl.multiple_of(c * 256 + h * 128, 128), 128)] for h in range(2)]
    tiles += [quarter_of(head, chan, x, h) for h in range(2)]
    for g in range(value.shape[1] // GROUP):
        lanes = slice(g * GROUP, (g + 1) * GROUP)
        tiles += [value[:, lanes], gate[:, lanes]]
    tiles += [quarter_of(head, chan, lax.rem(x + 2, FS), h) for h in range(2)]
    for i in range(SIDE):
        for t, tile in enumerate(tiles):
            pack[i, t] = tile


def attend_kernel(
    normed, mine, theirs, qgain, qup, kup, vup, cosv, sinv, head_out, logw,
    weight, lat, queries, keys, sa, sb, p, top, low, acc
):
    z, y, c = place()
    blocks = SIDE * SIDE
    for src, kind in ((mine, c), (theirs, jnp.bitwise_xor(c, 1))):
        base = jnp.where(kind == 0, z, y)
        for k, off in enumerate(OFFSETS):
            far = jnp.bitwise_and(base + (off + SIDE), SIDE - 1)
            for o in range(SIDE):
                block = jnp.where(kind == 0, far * SIDE + o, o * SIDE + far)
                for h in range(2):
                    weight[kind * 2 + h, block] = src[k * SIDE + o, QUERY_AT + h]
    x = normed[...]
    for g in range(4):
        lat[:, g * 128 : (g + 1) * 128] = nn_dot(x, weight[g].reshape(blocks * ROW, 128))
    latent = scaled(lat[...], qgain[...]).astype(bf16)
    every = nn_dot(latent, qup[...])
    heads = kup.shape[1] // NOPE
    rows = normed.shape[0]
    cos2, sin2 = doubled(cosv[...], sinv[...])
    for h in range(heads):
        lo = h * (NOPE + ROPE)
        plain = every[:, lo : lo + NOPE].astype(bf16)
        raw = every[:, lo + NOPE : lo + NOPE + ROPE]
        rot = raw * cos2 + turned_half(raw) * sin2
        rot = jnp.concatenate([rot, jnp.zeros_like(rot)], axis=1).astype(bf16)
        absorbed = nt_dot(plain, kup[:, h * NOPE : (h + 1) * NOPE]).astype(bf16)
        queries[h * rows : (h + 1) * rows, :KVR] = absorbed
        queries[h * rows : (h + 1) * rows, KVR:] = rot

    per = SIDE * 64
    base = 0
    for src in (mine, theirs):
        count = src.shape[0] // SIDE

        def fill(i, carry, src=src, base=base):
            part = src[pl.ds(i * SIDE, SIDE)]
            to = pl.ds(pl.multiple_of((base + i) * per, per), per)
            keys[to, 0:128] = part[:, 0:2].reshape(per, 128)
            keys[to, 128:256] = part[:, 2:4].reshape(per, 128)
            near = part[:, 4].astype(f32)
            far = pltpu.roll(near.reshape(per // 2, 128), 64, 1).reshape(SIDE, 32, 128)
            both = jnp.concatenate([near, far], axis=1).reshape(per, 128)
            keys[to, 256:384] = both.astype(bf16)
            return carry

        lax.fori_loop(0, count, fill, 0)
        base += count
    top[...] = jnp.full_like(top, far_below)
    low[...] = jnp.zeros_like(low)
    acc[...] = jnp.zeros_like(acc)
    factor = LOG2E * (NOPE + ROPE) ** (-0.5)
    wide = sa.shape[1]
    steps = keys.shape[0] // wide
    total_rows = heads * rows

    def span(j):
        return pl.ds(pl.multiple_of(j * wide, wide), wide)

    def score(j, s):
        s[...] = nt_dot(queries[...], keys[span(j), :])

    def soften(j, s):
        for r in range(0, total_rows, 32):
            at = slice(r, r + 32)
            v = s[at, :]
            most = v[:, 0:128]
            for i in range(1, wide // 128):
                most = jnp.maximum(most, v[:, i * 128 : (i + 1) * 128])
            old = top[at, :]
            new = jnp.maximum(old, jnp.max(most, axis=1, keepdims=True))
            fade = jnp.exp2((old - new) * factor)
            part = low[at, :] * fade
            for i in range(wide // 128):
                e = jnp.exp2((v[:, i * 128 : (i + 1) * 128] - new) * factor)
                part = part + e
                p[at, i * 128 : (i + 1) * 128] = e.astype(bf16)
            low[at, :] = part
            top[at, :] = new
            acc[at, 0:128] = acc[at, 0:128] * fade
            acc[at, 128:256] = acc[at, 128:256] * fade
        acc[...] += nn_dot(p[...], keys[span(j), 0:KVR])

    score(0, sa)

    def pair(i, carry):
        score(2 * i + 1, sb)
        soften(2 * i, sa)
        score(jnp.minimum(2 * i + 2, steps - 1), sa)
        soften(2 * i + 1, sb)
        return carry

    lax.fori_loop(0, steps // 2, pair, 0)
    for h in range(heads):
        at = slice(h * rows, (h + 1) * rows)
        total = jnp.sum(low[at, :], axis=1, keepdims=True)
        attended = (acc[at, :] / total).astype(bf16)
        out = nn_dot(attended, vup[:, h * VDIM : (h + 1) * VDIM])
        head_out[:, h * VDIM : (h + 1) * VDIM] = out.astype(bf16)
        logs = top[at, :] * (factor * LN2) + jnp.log(total)
        logw[h : h + 1, :] = jnp.transpose(logs)[0:1, :]


def post_kernel(
    normed, before, after, gain, w_any, own_any, up_any, down_any, taps, ggain, head_out,
    mine, other, w, wo, wide, gated, sems
):
    c = place()[2]
    x = lax.axis_index("fs")
    rows = normed.shape[0]
    groups = gated.shape[1] // GROUP

    def copies(core):
        made = []
        base = place()[core]

        def add(src, lo, count, to):
            for k, off in enumerate(OFFSETS):
                far = jnp.bitwise_and(base + (off + SIDE), SIDE - 1)
                at = src.at[pl.ds(k * SIDE, SIDE), pl.ds(lo, count)]
                spot = to.at[far] if core == 0 else to.at[:, far]
                made.append(pltpu.make_async_copy(at, spot, sems.at[len(made)]))

        add(w_any, 0, GLU_TILES, w)
        for step, src, lo in ((0, own_any, OUT_AT), (3, up_any, 0), (1, down_any, 0)):
            add(src, lo, 2, wo.at[lax.rem(x + step, FS)])
        add(w_any, GLU_TILES, 2, wo.at[lax.rem(x + 2, FS)])
        return made

    for core in range(TP):

        @pl.when(c == core)
        def _(core=core):
            for copy in copies(core):
                copy.start()

    pending = copies(0)

    wide[0:EDGE, :] = scaled(before[...].astype(f32), gain[...]).astype(bf16)
    wide[EDGE : EDGE + rows, :] = normed[...]
    wide[EDGE + rows :, :] = scaled(after[...].astype(f32), gain[...]).astype(bf16)
    full = wide[...]
    for copy in pending[:SIDE]:
        copy.wait()

    def pair_of(ref, t):
        return jnp.concatenate([ref[:, :, t + i].reshape(-1, 128) for i in range(2)], axis=1)

    for g in range(groups):
        both = nn_dot(full, pair_of(w, 2 * g))
        value, gate = both[:, :GROUP], both[:, GROUP:]
        spot = slice(g * GROUP, (g + 1) * GROUP)
        gated[:, spot] = (value * jax.nn.sigmoid(gate)).astype(bf16).astype(f32)
    mixed = []
    reach = taps.shape[0] // 2
    for g in range(groups):
        lanes = slice(g * GROUP, (g + 1) * GROUP)
        tap = taps[:, lanes].astype(f32)
        lo = EDGE - reach
        total = gated[lo : lo + rows, lanes] * tap[0:1, :]
        for j in range(1, taps.shape[0]):
            total = total + gated[lo + j : lo + j + rows, lanes] * tap[j : j + 1, :]
        centred = total - jnp.mean(total, axis=-1, keepdims=True)
        spread = jnp.mean(centred * centred, axis=-1, keepdims=True)
        unit = centred * lax.rsqrt(spread + norm_eps) * ggain[lanes].astype(f32)[None, :]
        mixed.append((unit * jax.nn.sigmoid(unit)).astype(bf16))
    mix = jnp.concatenate([head_out[...]] + mixed, axis=1)
    for copy in pending[SIDE:]:
        copy.wait()
    part = SIDE // TP
    for out, which in ((other, jnp.bitwise_xor(c, 1)), (mine, c)):
        total = None
        for q in range(FS):
            wq = pair_of(wo.at[q, pl.ds(which * part, part)], 0)
            term = nt_dot(mix[:, q * QUART : (q + 1) * QUART], wq)
            total = term if total is None else total + term
        out[...] = total.astype(bf16)


def on_device(
    tokens,
    norm_gain,
    query_down,
    query_gain,
    latent_down,
    latent_gain,
    rope_down,
    query_up,
    key_up,
    value_up,
    glu_value,
    glu_gate,
    conv_taps,
    group_gain,
    head_proj,
    channel_proj,
):
    tok = tokens.shape[0]
    sp = lax.axis_index("sp")
    vmem = pl.BlockSpec(memory_space=pltpu.VMEM)
    hbm = pl.BlockSpec(memory_space=pltpu.HBM)
    first = line_groups(0)
    head_t, chan_t = head_proj.T, channel_proj.T

    quarter = ROPE // 4
    inverse = rope_base ** (-jnp.arange(quarter, dtype=f32) / quarter)
    places = sp * tok + jnp.arange(tok, dtype=jnp.int32)
    grid_row = (places // GRID_W).astype(f32)
    grid_col = (places % GRID_W).astype(f32)
    angles = jnp.concatenate([grid_row[:, None] * inverse, grid_col[:, None] * inverse], axis=-1)
    cosine, sine = jnp.cos(angles), jnp.sin(angles)
    normed, sent = pl.pallas_call(
        pre_kernel,
        name="pre",
        out_shape=(
            jax.ShapeDtypeStruct(tokens.shape, bf16),
            jax.ShapeDtypeStruct((SIDE, TILES, ROW, 128), bf16),
        ),
        in_specs=[vmem] * 12,
        out_specs=(vmem, vmem),
        cost_estimate=pl.CostEstimate(flops=int(2e9), bytes_accessed=3 * 2**20, transcendentals=0),
    )(tokens, norm_gain, latent_down, latent_gain, rope_down.T, query_down, glu_value, glu_gate, head_t, chan_t, cosine, sine)
    own = lax.all_to_all(sent, MESH_AXES, 0, 0, axis_index_groups=first, tiled=True)

    spread, weights = rings([own[:, :KEY_TILES], own[:, KEY_TILES:]])

    swap = [(0, 1), (1, 0)]
    theirs = lax.ppermute(spread, "tp", swap)
    fourth = spread[:, OUT_AT:]
    up = lax.ppermute(fourth, "fs", [(i, (i + 1) % FS) for i in range(FS)])
    down = lax.ppermute(fourth, "fs", [((i + 1) % FS, i) for i in range(FS)])

    heads = key_up.shape[1] // NOPE
    many = heads * tok
    total_keys = 2 * SIDE * SIDE * 64
    chunk = 1024
    head_out, log_weight = pl.pallas_call(
        attend_kernel,
        name="attend",
        out_shape=(
            jax.ShapeDtypeStruct((tok, heads * VDIM), bf16),
            jax.ShapeDtypeStruct((heads, tok), f32),
        ),
        in_specs=[vmem] * 9,
        out_specs=(vmem, vmem),
        scratch_shapes=[
            pltpu.VMEM((4, SIDE * SIDE, ROW, 128), bf16),
            pltpu.VMEM((tok, 512), f32),
            pltpu.VMEM((many, KVR + 128), bf16),
            pltpu.VMEM((total_keys, KVR + 128), bf16),
            pltpu.VMEM((many, chunk), f32),
            pltpu.VMEM((many, chunk), f32),
            pltpu.VMEM((many, chunk), bf16),
            pltpu.VMEM((many, 128), f32),
            pltpu.VMEM((many, 128), f32),
            pltpu.VMEM((many, KVR), f32),
        ],
        cost_estimate=pl.CostEstimate(flops=int(8e9), bytes_accessed=8 * 2**20, transcendentals=0),
    )(normed, spread, theirs, query_gain, query_up, key_up, value_up, cosine, sine)

    sp_count = lax.axis_size("sp")
    forward = [(i, i + 1) for i in range(sp_count - 1)]
    backward = [(i + 1, i) for i in range(sp_count - 1)]
    last, front, head_out = lax.optimization_barrier(
        (tokens[tok - EDGE :], tokens[:EDGE], head_out)
    )
    before = lax.ppermute(last, "sp", forward)
    after = lax.ppermute(front, "sp", backward)

    ch = glu_value.shape[1]
    half_out = tokens.shape[1] // TP
    mine, other = pl.pallas_call(
        post_kernel,
        name="post",
        out_shape=(jax.ShapeDtypeStruct((tok, half_out), bf16),) * 2,
        in_specs=[vmem] * 4 + [hbm] * 4 + [vmem] * 3,
        out_specs=(vmem, vmem),
        scratch_shapes=[
            pltpu.VMEM((SIDE, SIDE, GLU_TILES, ROW, 128), bf16),
            pltpu.VMEM((FS, SIDE, SIDE, 2, ROW, 128), bf16),
            pltpu.VMEM((tok + 2 * EDGE, tokens.shape[1]), bf16),
            pltpu.VMEM((tok + 2 * EDGE, ch), f32),
            pltpu.SemaphoreType.DMA((5 * SIDE,)),
        ],
        cost_estimate=pl.CostEstimate(flops=int(3e9), bytes_accessed=9 * 2**20, transcendentals=0),
    )(
        normed, before, after, norm_gain, weights, spread, up, down, conv_taps, group_gain, head_out
    )
    arrived = lax.ppermute(other, "tp", swap)
    mixed_out = (mine.astype(f32) + arrived.astype(f32)).astype(bf16)
    return (mixed_out, log_weight)


def solution(mesh):
    in_specs = (
        P(("fs", "sp"), None),
        P(),
        P("sp", None),
        P(),
        P(),
        P(),
        P(),
        P(None, "tp"),
        P(None, "tp"),
        P(None, "tp"),
        P("sp", "tp"),
        P("sp", "tp"),
        P(None, "tp"),
        P("tp"),
        P("tp", "sp"),
        P("tp", "sp"),
    )
    out_specs = (P(("fs", "sp"), "tp"), P("tp", ("fs", "sp")))
    return jax.shard_map(
        on_device, mesh=mesh, in_specs=in_specs, out_specs=out_specs, check_vma=False
    )
```

```python
import jax
import jax.numpy as jnp
from jax import lax
from jax.experimental import pallas as pl
from jax.experimental.pallas import tpu as pltpu
from jax.sharding import PartitionSpec as P

NOPE = 128
ROPE = 64
VDIM = 128
KVR = 256
GROUP = 128
GRID_W = 64
EDGE = 16
SIDE = 8
FS = 4
TP = 2
ROW = 32
QUERY_AT = 5
OUT_AT = 7
KEY_TILES = 9
GLU_TILES = 8
WEIGHT_TILES = 10
QUART = 256
MESH_AXES = ("sp", "fs", "tp")

norm_eps = 1e-06
rope_base = 10000.0
far_below = -1e30
LOG2E = 1.4426950408889634
LN2 = 0.6931471805599453

f32 = jnp.float32
bf16 = jnp.bfloat16


def flat(z, y, x, c):
    return ((z * SIDE + y) * FS + x) * TP + c


def line_groups(phase):
    groups = []
    for x in range(FS):
        for c in range(TP):
            for o in range(SIDE):
                if (c == 0) == (phase == 0):
                    groups.append([flat(o, i, x, c) for i in range(SIDE)])
                else:
                    groups.append([flat(i, o, x, c) for i in range(SIDE)])
    return groups


def nt_dot(a, b):
    return lax.dot_general(a, b, (((1,), (1,)), ((), ())), preferred_element_type=f32)


def nn_dot(a, b):
    return jnp.dot(a, b, preferred_element_type=f32)


def scaled(values, gain):
    inv = lax.rsqrt(jnp.mean(values * values, axis=-1, keepdims=True) + norm_eps)
    return values * inv * gain.astype(f32)[None, :]


def turned_half(raw):
    return jnp.concatenate([raw[:, ROPE // 2 :], raw[:, : ROPE // 2]], axis=1)


def doubled(cosv, sinv):
    return jnp.concatenate([cosv, cosv], axis=1), jnp.concatenate([-sinv, sinv], axis=1)


def place():
    sp = lax.axis_index("sp")
    return lax.div(sp, SIDE), lax.rem(sp, SIDE), lax.axis_index("tp")


def quarter_of(head, chan, q, h):
    at = pl.ds(pl.multiple_of(lax.rem(q, 2) * QUART + h * 128, 128), 128)
    return jnp.where(q < 2, head[:, at], chan[:, at])


def pre_kernel(
    tok, gain, ldown, lgain, rdown, qdown, head, chan, cosv, sinv, normed, pack
):
    half = tok.shape[0] // TP
    c = place()[2]
    normed[...] = scaled(tok[...].astype(f32), gain[...]).astype(bf16)
    start = pl.multiple_of(c * half, half)
    own = normed[pl.ds(start, half), :]
    latent = scaled(nn_dot(own, ldown[...]), lgain[...]).astype(bf16)
    raw = nt_dot(own, rdown[...])
    cos2, sin2 = doubled(cosv[pl.ds(start, half), :], sinv[pl.ds(start, half), :])
    key = raw * cos2 + turned_half(raw) * sin2
    pair = jnp.concatenate([key[: half // 2], key[half // 2 :]], axis=1).astype(bf16)
    x = lax.axis_index("fs")
    tiles = []
    for j in range(2):
        for i in range(2):
            tiles.append(latent[i * ROW : (i + 1) * ROW, j * 128 : (j + 1) * 128])
    tiles.append(pair)
    tiles += [qdown[:, pl.ds(pl.multiple_of(c * 256 + h * 128, 128), 128)] for h in range(2)]
    tiles += [quarter_of(head, chan, x, h) for h in range(2)]
    for i in range(SIDE):
        for t, tile in enumerate(tiles):
            pack[i, t] = tile


def pack_kernel(value, gate, head, chan, pack):
    far = lax.rem(lax.axis_index("fs") + 2, FS)
    tiles = []
    for g in range(value.shape[1] // GROUP):
        lanes = slice(g * GROUP, (g + 1) * GROUP)
        tiles += [value[:, lanes], gate[:, lanes]]
    tiles += [quarter_of(head, chan, far, h) for h in range(2)]
    for i in range(SIDE):
        for t, tile in enumerate(tiles):
            pack[i, t] = tile


def attend_kernel(
    normed, mine, theirs, qgain, qup, kup, vup, cosv, sinv, head_out, logw,
    weight, lat, queries, keys, sa, sb, p, top, low, acc
):
    c = place()[2]
    blocks = SIDE * SIDE
    for src, kind in ((mine, c), (theirs, jnp.bitwise_xor(c, 1))):
        for b in range(SIDE):
            for o in range(SIDE):
                block = jnp.where(kind == 0, b * SIDE + o, o * SIDE + b)
                for h in range(2):
                    weight[kind * 2 + h, block] = src[b * SIDE + o, QUERY_AT + h]
    x = normed[...]
    for g in range(4):
        lat[:, g * 128 : (g + 1) * 128] = nn_dot(x, weight[g].reshape(blocks * ROW, 128))
    latent = scaled(lat[...], qgain[...]).astype(bf16)
    every = nn_dot(latent, qup[...])
    heads = kup.shape[1] // NOPE
    rows = normed.shape[0]
    cos2, sin2 = doubled(cosv[...], sinv[...])
    for h in range(heads):
        lo = h * (NOPE + ROPE)
        plain = every[:, lo : lo + NOPE].astype(bf16)
        raw = every[:, lo + NOPE : lo + NOPE + ROPE]
        rot = raw * cos2 + turned_half(raw) * sin2
        rot = jnp.concatenate([rot, jnp.zeros_like(rot)], axis=1).astype(bf16)
        absorbed = nt_dot(plain, kup[:, h * NOPE : (h + 1) * NOPE]).astype(bf16)
        queries[h * rows : (h + 1) * rows, :KVR] = absorbed
        queries[h * rows : (h + 1) * rows, KVR:] = rot

    per = SIDE * 64
    base = 0
    for src in (mine, theirs):
        count = src.shape[0] // SIDE

        def fill(i, carry, src=src, base=base):
            part = src[pl.ds(i * SIDE, SIDE)]
            to = pl.ds(pl.multiple_of((base + i) * per, per), per)
            keys[to, 0:128] = part[:, 0:2].reshape(per, 128)
            keys[to, 128:256] = part[:, 2:4].reshape(per, 128)
            near = part[:, 4].astype(f32)
            far = pltpu.roll(near.reshape(per // 2, 128), 64, 1).reshape(SIDE, 32, 128)
            both = jnp.concatenate([near, far], axis=1).reshape(per, 128)
            keys[to, 256:384] = both.astype(bf16)
            return carry

        lax.fori_loop(0, count, fill, 0)
        base += count
    top[...] = jnp.full_like(top, far_below)
    low[...] = jnp.zeros_like(low)
    acc[...] = jnp.zeros_like(acc)
    factor = LOG2E * (NOPE + ROPE) ** (-0.5)
    wide = sa.shape[1]
    steps = keys.shape[0] // wide
    total_rows = heads * rows

    def span(j):
        return pl.ds(pl.multiple_of(j * wide, wide), wide)

    def score(j, s):
        s[...] = nt_dot(queries[...], keys[span(j), :])

    def soften(j, s):
        fades = []
        for r in range(0, total_rows, 32):
            at = slice(r, r + 32)
            v = s[at, :]
            most = v[:, 0:128]
            for i in range(1, wide // 128):
                most = jnp.maximum(most, v[:, i * 128 : (i + 1) * 128])
            old = top[at, :]
            new = jnp.maximum(old, jnp.max(most, axis=1, keepdims=True))
            fade = jnp.exp2((old - new) * factor)
            part = low[at, :] * fade
            for i in range(wide // 128):
                e = jnp.exp2((v[:, i * 128 : (i + 1) * 128] - new) * factor)
                part = part + e
                p[at, i * 128 : (i + 1) * 128] = e.astype(bf16)
            low[at, :] = part
            top[at, :] = new
            acc[at, 0:128] = acc[at, 0:128] * fade
            acc[at, 128:256] = acc[at, 128:256] * fade
        acc[...] += nn_dot(p[...], keys[span(j), 0:KVR])

    score(0, sa)

    def pair(i, carry):
        score(2 * i + 1, sb)
        soften(2 * i, sa)
        score(jnp.minimum(2 * i + 2, steps - 1), sa)
        soften(2 * i + 1, sb)
        return carry

    lax.fori_loop(0, steps // 2, pair, 0)
    for h in range(heads):
        at = slice(h * rows, (h + 1) * rows)
        total = jnp.sum(low[at, :], axis=1, keepdims=True)
        attended = (acc[at, :] / total).astype(bf16)
        out = nn_dot(attended, vup[:, h * VDIM : (h + 1) * VDIM])
        head_out[:, h * VDIM : (h + 1) * VDIM] = out.astype(bf16)
        logs = top[at, :] * (factor * LN2) + jnp.log(total)
        logw[h : h + 1, :] = jnp.transpose(logs)[0:1, :]


def edge_kernel(normed, before, after, gain, wide):
    rows = normed.shape[0]
    wide[0:EDGE, :] = scaled(before[...].astype(f32), gain[...]).astype(bf16)
    wide[EDGE : EDGE + rows, :] = normed[...]
    wide[EDGE + rows :, :] = scaled(after[...].astype(f32), gain[...]).astype(bf16)


def post_kernel(
    w_any, own_any, up_any, down_any, wide_any, taps, ggain, head_out,
    mine, other, w, wo, wide, taps_v, ggain_v, head_v, gated, outs, sems
):
    c = place()[2]
    x = lax.axis_index("fs")
    rows = head_out.shape[0]
    ch = gated.shape[1]
    groups = ch // GROUP

    def copies(core):
        made = []

        def add(src, to):
            made.append(pltpu.make_async_copy(src, to, sems.at[len(made)]))

        def tiles(src, lo, count, to):
            for j in range(SIDE):
                at = src.at[pl.ds(j * SIDE, SIDE), pl.ds(lo, count)]
                add(at, to.at[j] if core == 0 else to.at[:, j])

        tiles(w_any, 0, GLU_TILES, w)
        add(wide_any, wide)
        add(taps, taps_v)
        add(ggain, ggain_v)
        add(head_out, head_v)
        first = len(made)
        for step, src, lo in ((0, own_any, OUT_AT), (3, up_any, 0), (1, down_any, 0)):
            tiles(src, lo, 2, wo.at[lax.rem(x + step, FS)])
        tiles(w_any, GLU_TILES, 2, wo.at[lax.rem(x + 2, FS)])
        return made, first

    for core in range(TP):

        @pl.when(c == core)
        def _(core=core):
            for copy in copies(core)[0]:
                copy.start()

    pending, first = copies(0)
    for copy in pending[:first]:
        copy.wait()
    full = wide[...]

    def pair_of(ref, t):
        return jnp.concatenate([ref[:, :, t + i].reshape(-1, 128) for i in range(2)], axis=1)

    for g in range(groups):
        both = nn_dot(full, pair_of(w, 2 * g))
        value = both[:, :GROUP] * jax.nn.sigmoid(both[:, GROUP:])
        gated[:, g * GROUP : (g + 1) * GROUP] = value.astype(bf16).astype(f32)
    mixed = []
    count = taps_v.shape[0]
    lo = EDGE - count // 2
    for g in range(groups):
        lanes = slice(g * GROUP, (g + 1) * GROUP)
        tap = taps_v[:, lanes].astype(f32)
        total = None
        for r in range(8):
            reach = [s for s in range(lo, lo + count) if s % 8 == r]
            top = reach[-1] - r
            shifted = gated[r : r + top + rows, lanes]
            for s in reach:
                term = shifted[s - r : s - r + rows] * tap[s - lo : s - lo + 1, :]
                total = term if total is None else total + term
        centred = total - jnp.mean(total, axis=-1, keepdims=True)
        spread = jnp.mean(centred * centred, axis=-1, keepdims=True)
        unit = centred * lax.rsqrt(spread + norm_eps) * ggain_v[lanes].astype(f32)[None, :]
        mixed.append((unit * jax.nn.sigmoid(unit)).astype(bf16))
    mix = jnp.concatenate([head_v[...]] + mixed, axis=1)
    for copy in pending[first:]:
        copy.wait()
    part = SIDE // TP
    sent = []
    for i, (out, which) in enumerate(((other, jnp.bitwise_xor(c, 1)), (mine, c))):
        total = None
        for q in range(FS):
            wq = pair_of(wo.at[q, pl.ds(which * part, part)], 0)
            term = nt_dot(mix[:, q * QUART : (q + 1) * QUART], wq)
            total = term if total is None else total + term
        outs[i] = total.astype(bf16)
        sent.append(pltpu.make_async_copy(outs.at[i], out, sems.at[len(pending) + i]))
        sent[i].start()
    for copy in sent:
        copy.wait()


def per_device(
    tokens,
    norm_gain,
    query_down,
    query_gain,
    latent_down,
    latent_gain,
    rope_down,
    query_up,
    key_up,
    value_up,
    glu_value,
    glu_gate,
    conv_taps,
    group_gain,
    head_proj,
    channel_proj,
):
    tok = tokens.shape[0]
    sp = lax.axis_index("sp")
    vmem = pl.BlockSpec(memory_space=pltpu.VMEM)
    hbm = pl.BlockSpec(memory_space=pltpu.HBM)
    first, second = line_groups(0), line_groups(1)
    head_t, chan_t = head_proj.T, channel_proj.T

    quarter = ROPE // 4
    inverse = rope_base ** (-jnp.arange(quarter, dtype=f32) / quarter)
    places = sp * tok + jnp.arange(tok, dtype=jnp.int32)
    grid_row = (places // GRID_W).astype(f32)
    grid_col = (places % GRID_W).astype(f32)
    angles = jnp.concatenate([grid_row[:, None] * inverse, grid_col[:, None] * inverse], axis=-1)
    cosine, sine = jnp.cos(angles), jnp.sin(angles)
    normed, sent = pl.pallas_call(
        pre_kernel,
        name="pre",
        out_shape=(
            jax.ShapeDtypeStruct(tokens.shape, bf16),
            jax.ShapeDtypeStruct((SIDE, KEY_TILES, ROW, 128), bf16),
        ),
        in_specs=[vmem] * 10,
        out_specs=(vmem, vmem),
        cost_estimate=pl.CostEstimate(flops=int(2e9), bytes_accessed=3 * 2**20, transcendentals=0),
    )(tokens, norm_gain, latent_down, latent_gain, rope_down.T, query_down, head_t, chan_t, cosine, sine)
    own = lax.all_to_all(sent, MESH_AXES, 0, 0, axis_index_groups=first, tiled=True)

    spread = lax.all_gather(own, MESH_AXES, axis_index_groups=second, axis=0, tiled=True)

    value, gate, own = lax.optimization_barrier((glu_value, glu_gate, own))
    sent = pl.pallas_call(
        pack_kernel,
        name="pack",
        out_shape=jax.ShapeDtypeStruct((SIDE, WEIGHT_TILES, ROW, 128), bf16),
        in_specs=[vmem] * 4,
        out_specs=vmem,
    )(value, gate, head_t, chan_t)
    near = lax.all_to_all(sent, MESH_AXES, 0, 0, axis_index_groups=first, tiled=True)
    weights = lax.all_gather(near, MESH_AXES, axis_index_groups=second, axis=0, tiled=True)

    swap = [(0, 1), (1, 0)]
    theirs = lax.ppermute(spread, "tp", swap)
    fourth = spread[:, OUT_AT:]
    up = lax.ppermute(fourth, "fs", [(i, (i + 1) % FS) for i in range(FS)])
    down = lax.ppermute(fourth, "fs", [((i + 1) % FS, i) for i in range(FS)])

    heads = key_up.shape[1] // NOPE
    many = heads * tok
    total_keys = 2 * SIDE * SIDE * 64
    chunk = 1024
    head_out, log_weight = pl.pallas_call(
        attend_kernel,
        name="attend",
        out_shape=(
            jax.ShapeDtypeStruct((tok, heads * VDIM), bf16),
            jax.ShapeDtypeStruct((heads, tok), f32),
        ),
        in_specs=[vmem] * 9,
        out_specs=(vmem, vmem),
        scratch_shapes=[
            pltpu.VMEM((4, SIDE * SIDE, ROW, 128), bf16),
            pltpu.VMEM((tok, 512), f32),
            pltpu.VMEM((many, KVR + 128), bf16),
            pltpu.VMEM((total_keys, KVR + 128), bf16),
            pltpu.VMEM((many, chunk), f32),
            pltpu.VMEM((many, chunk), f32),
            pltpu.VMEM((many, chunk), bf16),
            pltpu.VMEM((many, 128), f32),
            pltpu.VMEM((many, 128), f32),
            pltpu.VMEM((many, KVR), f32),
        ],
        cost_estimate=pl.CostEstimate(flops=int(8e9), bytes_accessed=8 * 2**20, transcendentals=0),
    )(normed, spread, theirs, query_gain, query_up, key_up, value_up, cosine, sine)

    sp_count = lax.axis_size("sp")
    forward = [(i, i + 1) for i in range(sp_count - 1)]
    backward = [(i + 1, i) for i in range(sp_count - 1)]
    last, front, head_out = lax.optimization_barrier(
        (tokens[tok - EDGE :], tokens[:EDGE], head_out)
    )
    before = lax.ppermute(last, "sp", forward)
    after = lax.ppermute(front, "sp", backward)
    wide = pl.pallas_call(
        edge_kernel,
        name="edge",
        out_shape=jax.ShapeDtypeStruct((tok + 2 * EDGE, tokens.shape[1]), bf16),
        in_specs=[vmem] * 4,
        out_specs=vmem,
    )(normed, before, after, norm_gain)

    ch = glu_value.shape[1]
    half_out = tokens.shape[1] // TP
    mine, other = pl.pallas_call(
        post_kernel,
        name="post",
        out_shape=(jax.ShapeDtypeStruct((tok, half_out), bf16),) * 2,
        in_specs=[hbm] * 8,
        out_specs=(hbm, hbm),
        scratch_shapes=[
            pltpu.VMEM((SIDE, SIDE, GLU_TILES, ROW, 128), bf16),
            pltpu.VMEM((FS, SIDE, SIDE, 2, ROW, 128), bf16),
            pltpu.VMEM((tok + 2 * EDGE, tokens.shape[1]), bf16),
            pltpu.VMEM(conv_taps.shape, bf16),
            pltpu.VMEM(group_gain.shape, bf16),
            pltpu.VMEM(head_out.shape, bf16),
            pltpu.VMEM((tok + 2 * EDGE, ch), f32),
            pltpu.VMEM((TP, tok, half_out), bf16),
            pltpu.SemaphoreType.DMA((64,)),
        ],
        cost_estimate=pl.CostEstimate(flops=int(3e9), bytes_accessed=9 * 2**20, transcendentals=0),
    )(
        weights, spread, up, down, wide, conv_taps, group_gain, head_out
    )
    arrived = lax.ppermute(other, "tp", swap)
    mixed_out = (mine.astype(f32) + arrived.astype(f32)).astype(bf16)
    return (mixed_out, log_weight)


def solution(mesh):
    in_specs = (
        P(("fs", "sp"), None),
        P(),
        P("sp", None),
        P(),
        P(),
        P(),
        P(),
        P(None, "tp"),
        P(None, "tp"),
        P(None, "tp"),
        P("sp", "tp"),
        P("sp", "tp"),
        P(None, "tp"),
        P("tp"),
        P("tp", "sp"),
        P("tp", "sp"),
    )
    out_specs = (P(("fs", "sp"), "tp"), P("tp", ("fs", "sp")))
    return jax.shard_map(
        per_device, mesh=mesh, in_specs=in_specs, out_specs=out_specs, check_vma=False
    )
```

```python
import jax
import jax.numpy as jnp
from jax import lax
from jax.experimental import pallas as pl
from jax.experimental.pallas import tpu as pltpu
from jax.sharding import PartitionSpec as P

NOPE = 128
ROPE = 64
VDIM = 128
KVR = 256
GROUP = 128
GRID_W = 64
EDGE = 16
SIDE = 8
FS = 4
TP = 2
ROW = 32
QUERY_AT = 5
OUT_AT = 7
KEY_TILES = 9
GLU_TILES = 8
WEIGHT_TILES = 10
QUART = 256
MESH_AXES = ("sp", "fs", "tp")

norm_eps = 1e-06
rope_base = 10000.0
far_below = -1e30
LOG2E = 1.4426950408889634
LN2 = 0.6931471805599453

f32 = jnp.float32
bf16 = jnp.bfloat16


def flat(z, y, x, c):
    return ((z * SIDE + y) * FS + x) * TP + c


def line_groups(phase):
    groups = []
    for x in range(FS):
        for c in range(TP):
            for o in range(SIDE):
                if (c == 0) == (phase == 0):
                    groups.append([flat(o, i, x, c) for i in range(SIDE)])
                else:
                    groups.append([flat(i, o, x, c) for i in range(SIDE)])
    return groups


def nt_dot(a, b):
    return lax.dot_general(a, b, (((1,), (1,)), ((), ())), preferred_element_type=f32)


def nn_dot(a, b):
    return jnp.dot(a, b, preferred_element_type=f32)


def scaled(values, gain):
    inv = lax.rsqrt(jnp.mean(values * values, axis=-1, keepdims=True) + norm_eps)
    return values * inv * gain.astype(f32)[None, :]


def turned_half(raw):
    return jnp.concatenate([raw[:, ROPE // 2 :], raw[:, : ROPE // 2]], axis=1)


def turns(inverse, first, count):
    spot = first + lax.broadcasted_iota(jnp.int32, (count, ROPE), 0)
    lane = lax.broadcasted_iota(jnp.int32, (count, ROPE), 1)
    row = lax.shift_right_logical(spot, GRID_W.bit_length() - 1)
    col = jnp.bitwise_and(spot, GRID_W - 1)
    on_row = jnp.bitwise_and(lane, ROPE // 2 - 1) < ROPE // 4
    angles = jnp.where(on_row, row, col).astype(f32) * inverse[...]
    sine = jnp.sin(angles)
    return jnp.cos(angles), jnp.where(lane < ROPE // 2, -sine, sine)


def place():
    sp = lax.axis_index("sp")
    return lax.div(sp, SIDE), lax.rem(sp, SIDE), lax.axis_index("tp")


def quarter_of(head, chan, q, h):
    at = pl.ds(pl.multiple_of(lax.rem(q, 2) * QUART + h * 128, 128), 128)
    return jnp.where(q < 2, head[:, at], chan[:, at])


def pre_kernel(
    tok, gain, ldown, lgain, rdown, qdown, head, chan, inverse, normed, pack
):
    half = tok.shape[0] // TP
    c = place()[2]
    normed[...] = scaled(tok[...].astype(f32), gain[...]).astype(bf16)
    start = pl.multiple_of(c * half, half)
    own = normed[pl.ds(start, half), :]
    latent = scaled(nn_dot(own, ldown[...]), lgain[...]).astype(bf16)
    raw = nt_dot(own, rdown[...])
    first = lax.axis_index("sp") * tok.shape[0] + start
    cos2, sin2 = turns(inverse, first, half)
    key = raw * cos2 + turned_half(raw) * sin2
    pair = jnp.concatenate([key[: half // 2], key[half // 2 :]], axis=1).astype(bf16)
    x = lax.axis_index("fs")
    tiles = []
    for j in range(2):
        for i in range(2):
            tiles.append(latent[i * ROW : (i + 1) * ROW, j * 128 : (j + 1) * 128])
    tiles.append(pair)
    tiles += [qdown[:, pl.ds(pl.multiple_of(c * 256 + h * 128, 128), 128)] for h in range(2)]
    tiles += [quarter_of(head, chan, x, h) for h in range(2)]
    for i in range(SIDE):
        for t, tile in enumerate(tiles):
            pack[i, t] = tile


def pack_kernel(value, gate, head, chan, pack):
    far = lax.rem(lax.axis_index("fs") + 2, FS)
    tiles = []
    for g in range(value.shape[1] // GROUP):
        lanes = slice(g * GROUP, (g + 1) * GROUP)
        tiles += [value[:, lanes], gate[:, lanes]]
    tiles += [quarter_of(head, chan, far, h) for h in range(2)]
    for i in range(SIDE):
        for t, tile in enumerate(tiles):
            pack[i, t] = tile


def attend_kernel(
    normed, mine, theirs, qgain, qup, kup, vup, inverse, head_out, logw,
    weight, lat, queries, keys, sa, sb, p, top, low, acc
):
    c = place()[2]
    blocks = SIDE * SIDE
    for src, kind in ((mine, c), (theirs, jnp.bitwise_xor(c, 1))):
        for b in range(SIDE):
            for o in range(SIDE):
                block = jnp.where(kind == 0, b * SIDE + o, o * SIDE + b)
                for h in range(2):
                    weight[kind * 2 + h, block] = src[b * SIDE + o, QUERY_AT + h]
    x = normed[...]
    for g in range(4):
        lat[:, g * 128 : (g + 1) * 128] = nn_dot(x, weight[g].reshape(blocks * ROW, 128))
    latent = scaled(lat[...], qgain[...]).astype(bf16)
    every = nn_dot(latent, qup[...])
    heads = kup.shape[1] // NOPE
    rows = normed.shape[0]
    cos2, sin2 = turns(inverse, lax.axis_index("sp") * rows, rows)
    for h in range(heads):
        lo = h * (NOPE + ROPE)
        plain = every[:, lo : lo + NOPE].astype(bf16)
        raw = every[:, lo + NOPE : lo + NOPE + ROPE]
        rot = raw * cos2 + turned_half(raw) * sin2
        rot = jnp.concatenate([rot, jnp.zeros_like(rot)], axis=1).astype(bf16)
        absorbed = nt_dot(plain, kup[:, h * NOPE : (h + 1) * NOPE]).astype(bf16)
        queries[h * rows : (h + 1) * rows, :KVR] = absorbed
        queries[h * rows : (h + 1) * rows, KVR:] = rot

    per = SIDE * 64
    base = 0
    for src in (mine, theirs):
        count = src.shape[0] // SIDE

        def fill(i, carry, src=src, base=base):
            part = src[pl.ds(i * SIDE, SIDE)]
            to = pl.ds(pl.multiple_of((base + i) * per, per), per)
            keys[to, 0:128] = part[:, 0:2].reshape(per, 128)
            keys[to, 128:256] = part[:, 2:4].reshape(per, 128)
            near = part[:, 4].astype(f32)
            far = pltpu.roll(near.reshape(per // 2, 128), 64, 1).reshape(SIDE, 32, 128)
            both = jnp.concatenate([near, far], axis=1).reshape(per, 128)
            keys[to, 256:384] = both.astype(bf16)
            return carry

        lax.fori_loop(0, count, fill, 0)
        base += count
    top[...] = jnp.full_like(top, far_below)
    low[...] = jnp.zeros_like(low)
    acc[...] = jnp.zeros_like(acc)
    factor = LOG2E * (NOPE + ROPE) ** (-0.5)
    wide = sa.shape[1]
    steps = keys.shape[0] // wide
    total_rows = heads * rows

    def span(j):
        return pl.ds(pl.multiple_of(j * wide, wide), wide)

    def score(j, s):
        s[...] = nt_dot(queries[...], keys[span(j), :])

    def soften(j, s):
        fades = []
        for r in range(0, total_rows, 32):
            at = slice(r, r + 32)
            v = s[at, :]
            most = v[:, 0:128]
            for i in range(1, wide // 128):
                most = jnp.maximum(most, v[:, i * 128 : (i + 1) * 128])
            old = top[at, :]
            new = jnp.maximum(old, jnp.max(most, axis=1, keepdims=True))
            fade = jnp.exp2((old - new) * factor)
            part = low[at, :] * fade
            for i in range(wide // 128):
                e = jnp.exp2((v[:, i * 128 : (i + 1) * 128] - new) * factor)
                part = part + e
                p[at, i * 128 : (i + 1) * 128] = e.astype(bf16)
            low[at, :] = part
            top[at, :] = new
            acc[at, 0:128] = acc[at, 0:128] * fade
            acc[at, 128:256] = acc[at, 128:256] * fade
        acc[...] += nn_dot(p[...], keys[span(j), 0:KVR])

    score(0, sa)

    def pair(i, carry):
        score(2 * i + 1, sb)
        soften(2 * i, sa)
        score(jnp.minimum(2 * i + 2, steps - 1), sa)
        soften(2 * i + 1, sb)
        return carry

    lax.fori_loop(0, steps // 2, pair, 0)
    for h in range(heads):
        at = slice(h * rows, (h + 1) * rows)
        total = jnp.sum(low[at, :], axis=1, keepdims=True)
        attended = (acc[at, :] / total).astype(bf16)
        out = nn_dot(attended, vup[:, h * VDIM : (h + 1) * VDIM])
        head_out[:, h * VDIM : (h + 1) * VDIM] = out.astype(bf16)
        logs = top[at, :] * (factor * LN2) + jnp.log(total)
        logw[h : h + 1, :] = jnp.transpose(logs)[0:1, :]


def edge_kernel(normed, before, after, gain, wide):
    rows = normed.shape[0]
    wide[0:EDGE, :] = scaled(before[...].astype(f32), gain[...]).astype(bf16)
    wide[EDGE : EDGE + rows, :] = normed[...]
    wide[EDGE + rows :, :] = scaled(after[...].astype(f32), gain[...]).astype(bf16)


def post_kernel(
    w_any, own_any, up_any, down_any, wide_any, taps, ggain, head_out,
    mine, other, w, wo, wide, taps_v, ggain_v, head_v, gated, outs, sems
):
    c = place()[2]
    x = lax.axis_index("fs")
    rows = head_out.shape[0]
    ch = gated.shape[1]
    groups = ch // GROUP

    def copies(core):
        made = []

        def add(src, to):
            made.append(pltpu.make_async_copy(src, to, sems.at[len(made)]))

        def tiles(src, lo, count, to):
            for j in range(SIDE):
                at = src.at[pl.ds(j * SIDE, SIDE), pl.ds(lo, count)]
                add(at, to.at[j] if core == 0 else to.at[:, j])

        tiles(w_any, 0, GLU_TILES, w)
        add(wide_any, wide)
        add(taps, taps_v)
        add(ggain, ggain_v)
        add(head_out, head_v)
        first = len(made)
        for step, src, lo in ((0, own_any, OUT_AT), (3, up_any, 0), (1, down_any, 0)):
            tiles(src, lo, 2, wo.at[lax.rem(x + step, FS)])
        tiles(w_any, GLU_TILES, 2, wo.at[lax.rem(x + 2, FS)])
        return made, first

    pending, first = copies(0)

    def launch(span):
        for core in range(TP):

            @pl.when(c == core)
            def _(core=core):
                for copy in copies(core)[0][span]:
                    copy.start()

    launch(slice(0, first))
    for copy in pending[:first]:
        copy.wait()
    launch(slice(first, None))
    full = wide[...]

    def pair_of(ref, t):
        return jnp.concatenate([ref[:, :, t + i].reshape(-1, 128) for i in range(2)], axis=1)

    for g in range(groups):
        both = nn_dot(full, pair_of(w, 2 * g))
        value = both[:, :GROUP] * jax.nn.sigmoid(both[:, GROUP:])
        gated[:, g * GROUP : (g + 1) * GROUP] = value.astype(bf16).astype(f32)
    mixed = []
    count = taps_v.shape[0]
    lo = EDGE - count // 2
    for g in range(groups):
        lanes = slice(g * GROUP, (g + 1) * GROUP)
        tap = taps_v[:, lanes].astype(f32)
        total = None
        for r in range(8):
            reach = [s for s in range(lo, lo + count) if s % 8 == r]
            top = reach[-1] - r
            shifted = gated[r : r + top + rows, lanes]
            for s in reach:
                term = shifted[s - r : s - r + rows] * tap[s - lo : s - lo + 1, :]
                total = term if total is None else total + term
        centred = total - jnp.mean(total, axis=-1, keepdims=True)
        spread = jnp.mean(centred * centred, axis=-1, keepdims=True)
        unit = centred * lax.rsqrt(spread + norm_eps) * ggain_v[lanes].astype(f32)[None, :]
        mixed.append((unit * jax.nn.sigmoid(unit)).astype(bf16))
    mix = jnp.concatenate([head_v[...]] + mixed, axis=1)
    for copy in pending[first:]:
        copy.wait()
    part = SIDE // TP
    sent = []
    for i, (out, which) in enumerate(((other, jnp.bitwise_xor(c, 1)), (mine, c))):
        total = None
        for q in range(FS):
            wq = pair_of(wo.at[q, pl.ds(which * part, part)], 0)
            term = nt_dot(mix[:, q * QUART : (q + 1) * QUART], wq)
            total = term if total is None else total + term
        outs[i] = total.astype(bf16)
        sent.append(pltpu.make_async_copy(outs.at[i], out, sems.at[len(pending) + i]))
        sent[i].start()
    for copy in sent:
        copy.wait()


def per_device(
    tokens,
    norm_gain,
    query_down,
    query_gain,
    latent_down,
    latent_gain,
    rope_down,
    query_up,
    key_up,
    value_up,
    glu_value,
    glu_gate,
    conv_taps,
    group_gain,
    head_proj,
    channel_proj,
):
    tok = tokens.shape[0]
    vmem = pl.BlockSpec(memory_space=pltpu.VMEM)
    hbm = pl.BlockSpec(memory_space=pltpu.HBM)
    first, second = line_groups(0), line_groups(1)
    head_t, chan_t = head_proj.T, channel_proj.T

    quarter = ROPE // 4
    inverse = rope_base ** (-jnp.arange(quarter, dtype=f32) / quarter)
    inverse = jnp.tile(inverse, 4)[None]
    normed, sent = pl.pallas_call(
        pre_kernel,
        name="pre",
        out_shape=(
            jax.ShapeDtypeStruct(tokens.shape, bf16),
            jax.ShapeDtypeStruct((SIDE, KEY_TILES, ROW, 128), bf16),
        ),
        in_specs=[vmem] * 9,
        out_specs=(vmem, vmem),
        cost_estimate=pl.CostEstimate(flops=int(2e9), bytes_accessed=3 * 2**20, transcendentals=0),
    )(tokens, norm_gain, latent_down, latent_gain, rope_down.T, query_down, head_t, chan_t, inverse)
    own = lax.all_to_all(sent, MESH_AXES, 0, 0, axis_index_groups=first, tiled=True)

    spread = lax.all_gather(own, MESH_AXES, axis_index_groups=second, axis=0, tiled=True)

    value, gate, own = lax.optimization_barrier((glu_value, glu_gate, own))
    sent = pl.pallas_call(
        pack_kernel,
        name="pack",
        out_shape=jax.ShapeDtypeStruct((SIDE, WEIGHT_TILES, ROW, 128), bf16),
        in_specs=[vmem] * 4,
        out_specs=vmem,
    )(value, gate, head_t, chan_t)
    near = lax.all_to_all(sent, MESH_AXES, 0, 0, axis_index_groups=first, tiled=True)
    weights = lax.all_gather(near, MESH_AXES, axis_index_groups=second, axis=0, tiled=True)

    swap = [(0, 1), (1, 0)]
    theirs = lax.ppermute(spread, "tp", swap)
    fourth = spread[:, OUT_AT:]
    up = lax.ppermute(fourth, "fs", [(i, (i + 1) % FS) for i in range(FS)])
    down = lax.ppermute(fourth, "fs", [((i + 1) % FS, i) for i in range(FS)])

    heads = key_up.shape[1] // NOPE
    many = heads * tok
    total_keys = 2 * SIDE * SIDE * 64
    chunk = 1024
    head_out, log_weight = pl.pallas_call(
        attend_kernel,
        name="attend",
        out_shape=(
            jax.ShapeDtypeStruct((tok, heads * VDIM), bf16),
            jax.ShapeDtypeStruct((heads, tok), f32),
        ),
        in_specs=[vmem] * 8,
        out_specs=(vmem, vmem),
        scratch_shapes=[
            pltpu.VMEM((4, SIDE * SIDE, ROW, 128), bf16),
            pltpu.VMEM((tok, 512), f32),
            pltpu.VMEM((many, KVR + 128), bf16),
            pltpu.VMEM((total_keys, KVR + 128), bf16),
            pltpu.VMEM((many, chunk), f32),
            pltpu.VMEM((many, chunk), f32),
            pltpu.VMEM((many, chunk), bf16),
            pltpu.VMEM((many, 128), f32),
            pltpu.VMEM((many, 128), f32),
            pltpu.VMEM((many, KVR), f32),
        ],
        cost_estimate=pl.CostEstimate(flops=int(8e9), bytes_accessed=8 * 2**20, transcendentals=0),
    )(normed, spread, theirs, query_gain, query_up, key_up, value_up, inverse)

    sp_count = lax.axis_size("sp")
    forward = [(i, i + 1) for i in range(sp_count - 1)]
    backward = [(i + 1, i) for i in range(sp_count - 1)]
    last, front, head_out = lax.optimization_barrier(
        (tokens[tok - EDGE :], tokens[:EDGE], head_out)
    )
    before = lax.ppermute(last, "sp", forward)
    after = lax.ppermute(front, "sp", backward)
    wide = pl.pallas_call(
        edge_kernel,
        name="edge",
        out_shape=jax.ShapeDtypeStruct((tok + 2 * EDGE, tokens.shape[1]), bf16),
        in_specs=[vmem] * 4,
        out_specs=vmem,
    )(normed, before, after, norm_gain)

    ch = glu_value.shape[1]
    half_out = tokens.shape[1] // TP
    mine, other = pl.pallas_call(
        post_kernel,
        name="post",
        out_shape=(jax.ShapeDtypeStruct((tok, half_out), bf16),) * 2,
        in_specs=[hbm] * 8,
        out_specs=(hbm, hbm),
        scratch_shapes=[
            pltpu.VMEM((SIDE, SIDE, GLU_TILES, ROW, 128), bf16),
            pltpu.VMEM((FS, SIDE, SIDE, 2, ROW, 128), bf16),
            pltpu.VMEM((tok + 2 * EDGE, tokens.shape[1]), bf16),
            pltpu.VMEM(conv_taps.shape, bf16),
            pltpu.VMEM(group_gain.shape, bf16),
            pltpu.VMEM(head_out.shape, bf16),
            pltpu.VMEM((tok + 2 * EDGE, ch), f32),
            pltpu.VMEM((TP, tok, half_out), bf16),
            pltpu.SemaphoreType.DMA((64,)),
        ],
        cost_estimate=pl.CostEstimate(flops=int(3e9), bytes_accessed=9 * 2**20, transcendentals=0),
    )(
        weights, spread, up, down, wide, conv_taps, group_gain, head_out
    )
    arrived = lax.ppermute(other, "tp", swap)
    mixed_out = (mine.astype(f32) + arrived.astype(f32)).astype(bf16)
    return (mixed_out, log_weight)


def solution(mesh):
    in_specs = (
        P(("fs", "sp"), None),
        P(),
        P("sp", None),
        P(),
        P(),
        P(),
        P(),
        P(None, "tp"),
        P(None, "tp"),
        P(None, "tp"),
        P("sp", "tp"),
        P("sp", "tp"),
        P(None, "tp"),
        P("tp"),
        P("tp", "sp"),
        P("tp", "sp"),
    )
    out_specs = (P(("fs", "sp"), "tp"), P("tp", ("fs", "sp")))
    return jax.shard_map(
        per_device, mesh=mesh, in_specs=in_specs, out_specs=out_specs, check_vma=False
    )
```

```python
import jax
import jax.numpy as jnp
from jax import lax
from jax.experimental import pallas as pl
from jax.experimental.pallas import tpu as pltpu
from jax.sharding import PartitionSpec as P

NOPE = 128
ROPE = 64
VDIM = 128
KVR = 256
GROUP = 128
GRID_W = 64
EDGE = 16
SIDE = 8
FS = 4
TP = 2
ROW = 32
QUERY_AT = 5
OUT_AT = 7
KEY_TILES = 9
GLU_TILES = 8
WEIGHT_TILES = 10
QUART = 256
OFFSETS = (0, -1, 1, -2, 2, -3, 3, -4)
MESH_AXES = ("sp", "fs", "tp")

norm_eps = 1e-06
rope_base = 10000.0
far_below = -1e30
LOG2E = 1.4426950408889634
LN2 = 0.6931471805599453

f32 = jnp.float32
bf16 = jnp.bfloat16


def flat(z, y, x, c):
    return ((z * SIDE + y) * FS + x) * TP + c


def line_groups(phase):
    groups = []
    for x in range(FS):
        for c in range(TP):
            for o in range(SIDE):
                if (c == 0) == (phase == 0):
                    groups.append([flat(o, i, x, c) for i in range(SIDE)])
                else:
                    groups.append([flat(i, o, x, c) for i in range(SIDE)])
    return groups


def line_pairs(step):
    pairs = []
    for group in line_groups(1):
        pairs += [(group[i], group[(i + step) % SIDE]) for i in range(SIDE)]
    return pairs


def spread_line(own):
    def hop(block, step):
        return lax.ppermute(block, MESH_AXES, line_pairs(step))

    half = SIDE // 2
    up1, down1 = hop(own, 1), hop(own, -1)
    up2, down2 = hop(own, 2), hop(own, -2)
    up3, down3 = hop(up2, 1), hop(down2, -1)
    up4, down4 = hop(up2[:half], 2), hop(down2[half:], -2)
    return jnp.concatenate([own, up1, down1, up2, down2, up3, down3, up4, down4], axis=0)


def nt_dot(a, b):
    return lax.dot_general(a, b, (((1,), (1,)), ((), ())), preferred_element_type=f32)


def nn_dot(a, b):
    return jnp.dot(a, b, preferred_element_type=f32)


def scaled(values, gain):
    inv = lax.rsqrt(jnp.mean(values * values, axis=-1, keepdims=True) + norm_eps)
    return values * inv * gain.astype(f32)[None, :]


def turned_half(raw):
    return jnp.concatenate([raw[:, ROPE // 2 :], raw[:, : ROPE // 2]], axis=1)


def turns(inverse, first, count):
    spot = first + lax.broadcasted_iota(jnp.int32, (count, ROPE), 0)
    lane = lax.broadcasted_iota(jnp.int32, (count, ROPE), 1)
    row = lax.shift_right_logical(spot, GRID_W.bit_length() - 1)
    col = jnp.bitwise_and(spot, GRID_W - 1)
    on_row = jnp.bitwise_and(lane, ROPE // 2 - 1) < ROPE // 4
    angles = jnp.where(on_row, row, col).astype(f32) * inverse[...]
    sine = jnp.sin(angles)
    return jnp.cos(angles), jnp.where(lane < ROPE // 2, -sine, sine)


def place():
    sp = lax.axis_index("sp")
    return lax.div(sp, SIDE), lax.rem(sp, SIDE), lax.axis_index("tp")


def quarter_of(head, chan, q, h):
    at = pl.ds(pl.multiple_of(lax.rem(q, 2) * QUART + h * 128, 128), 128)
    return jnp.where(q < 2, head[:, at], chan[:, at])


def pre_kernel(
    tok, gain, ldown, lgain, rdown, qdown, head, chan, inverse, normed, pack
):
    half = tok.shape[0] // TP
    c = place()[2]
    normed[...] = scaled(tok[...].astype(f32), gain[...]).astype(bf16)
    start = pl.multiple_of(c * half, half)
    own = normed[pl.ds(start, half), :]
    latent = scaled(nn_dot(own, ldown[...]), lgain[...]).astype(bf16)
    raw = nt_dot(own, rdown[...])
    first = lax.axis_index("sp") * tok.shape[0] + start
    cos2, sin2 = turns(inverse, first, half)
    key = raw * cos2 + turned_half(raw) * sin2
    pair = jnp.concatenate([key[: half // 2], key[half // 2 :]], axis=1).astype(bf16)
    x = lax.axis_index("fs")
    tiles = []
    for j in range(2):
        for i in range(2):
            tiles.append(latent[i * ROW : (i + 1) * ROW, j * 128 : (j + 1) * 128])
    tiles.append(pair)
    tiles += [qdown[:, pl.ds(pl.multiple_of(c * 256 + h * 128, 128), 128)] for h in range(2)]
    tiles += [quarter_of(head, chan, x, h) for h in range(2)]
    for i in range(SIDE):
        for t, tile in enumerate(tiles):
            pack[i, t] = tile


def pack_kernel(value, gate, head, chan, pack):
    far = lax.rem(lax.axis_index("fs") + 2, FS)
    tiles = []
    for g in range(value.shape[1] // GROUP):
        lanes = slice(g * GROUP, (g + 1) * GROUP)
        tiles += [value[:, lanes], gate[:, lanes]]
    tiles += [quarter_of(head, chan, far, h) for h in range(2)]
    for i in range(SIDE):
        for t, tile in enumerate(tiles):
            pack[i, t] = tile


def attend_kernel(
    normed, mine, theirs, qgain, qup, kup, vup, inverse, head_out, logw,
    weight, lat, queries, keys, sa, sb, p, top, low, acc
):
    c = place()[2]
    blocks = SIDE * SIDE
    for src, kind in ((mine, c), (theirs, jnp.bitwise_xor(c, 1))):
        for b in range(SIDE):
            for o in range(SIDE):
                block = jnp.where(kind == 0, b * SIDE + o, o * SIDE + b)
                for h in range(2):
                    weight[kind * 2 + h, block] = src[b * SIDE + o, QUERY_AT + h]
    x = normed[...]
    for g in range(4):
        lat[:, g * 128 : (g + 1) * 128] = nn_dot(x, weight[g].reshape(blocks * ROW, 128))
    latent = scaled(lat[...], qgain[...]).astype(bf16)
    every = nn_dot(latent, qup[...])
    heads = kup.shape[1] // NOPE
    rows = normed.shape[0]
    cos2, sin2 = turns(inverse, lax.axis_index("sp") * rows, rows)
    for h in range(heads):
        lo = h * (NOPE + ROPE)
        plain = every[:, lo : lo + NOPE].astype(bf16)
        raw = every[:, lo + NOPE : lo + NOPE + ROPE]
        rot = raw * cos2 + turned_half(raw) * sin2
        rot = jnp.concatenate([rot, jnp.zeros_like(rot)], axis=1).astype(bf16)
        absorbed = nt_dot(plain, kup[:, h * NOPE : (h + 1) * NOPE]).astype(bf16)
        queries[h * rows : (h + 1) * rows, :KVR] = absorbed
        queries[h * rows : (h + 1) * rows, KVR:] = rot

    per = SIDE * 64
    base = 0
    for src in (mine, theirs):
        count = src.shape[0] // SIDE

        def fill(i, carry, src=src, base=base):
            part = src[pl.ds(i * SIDE, SIDE)]
            to = pl.ds(pl.multiple_of((base + i) * per, per), per)
            keys[to, 0:128] = part[:, 0:2].reshape(per, 128)
            keys[to, 128:256] = part[:, 2:4].reshape(per, 128)
            near = part[:, 4].astype(f32)
            far = pltpu.roll(near.reshape(per // 2, 128), 64, 1).reshape(SIDE, 32, 128)
            both = jnp.concatenate([near, far], axis=1).reshape(per, 128)
            keys[to, 256:384] = both.astype(bf16)
            return carry

        lax.fori_loop(0, count, fill, 0)
        base += count
    top[...] = jnp.full_like(top, far_below)
    low[...] = jnp.zeros_like(low)
    acc[...] = jnp.zeros_like(acc)
    factor = LOG2E * (NOPE + ROPE) ** (-0.5)
    wide = sa.shape[1]
    steps = keys.shape[0] // wide
    total_rows = heads * rows

    def span(j):
        return pl.ds(pl.multiple_of(j * wide, wide), wide)

    def score(j, s):
        s[...] = nt_dot(queries[...], keys[span(j), :])

    def soften(j, s):
        for r in range(0, total_rows, 32):
            at = slice(r, r + 32)
            v = s[at, :]
            most = v[:, 0:128]
            for i in range(1, wide // 128):
                most = jnp.maximum(most, v[:, i * 128 : (i + 1) * 128])
            old = top[at, :]
            new = jnp.maximum(old, jnp.max(most, axis=1, keepdims=True))
            fade = jnp.exp2((old - new) * factor)
            part = low[at, :] * fade
            for i in range(wide // 128):
                e = jnp.exp2((v[:, i * 128 : (i + 1) * 128] - new) * factor)
                part = part + e
                p[at, i * 128 : (i + 1) * 128] = e.astype(bf16)
            low[at, :] = part
            top[at, :] = new
            acc[at, 0:128] = acc[at, 0:128] * fade
            acc[at, 128:256] = acc[at, 128:256] * fade
        acc[...] += nn_dot(p[...], keys[span(j), 0:KVR])

    score(0, sa)

    def pair(i, carry):
        score(2 * i + 1, sb)
        soften(2 * i, sa)
        score(jnp.minimum(2 * i + 2, steps - 1), sa)
        soften(2 * i + 1, sb)
        return carry

    lax.fori_loop(0, steps // 2, pair, 0)
    for h in range(heads):
        at = slice(h * rows, (h + 1) * rows)
        total = jnp.sum(low[at, :], axis=1, keepdims=True)
        attended = (acc[at, :] / total).astype(bf16)
        out = nn_dot(attended, vup[:, h * VDIM : (h + 1) * VDIM])
        head_out[:, h * VDIM : (h + 1) * VDIM] = out.astype(bf16)
        logs = top[at, :] * (factor * LN2) + jnp.log(total)
        logw[h : h + 1, :] = jnp.transpose(logs)[0:1, :]


def edge_kernel(normed, before, after, gain, wide):
    rows = normed.shape[0]
    wide[0:EDGE, :] = scaled(before[...].astype(f32), gain[...]).astype(bf16)
    wide[EDGE : EDGE + rows, :] = normed[...]
    wide[EDGE + rows :, :] = scaled(after[...].astype(f32), gain[...]).astype(bf16)


def post_kernel(
    w_any, own_any, up_any, down_any, wide_any, taps, ggain, head_out,
    mine, other, w, wo, wide, taps_v, ggain_v, head_v, gated, outs, sems
):
    c = place()[2]
    x = lax.axis_index("fs")
    rows = head_out.shape[0]
    ch = gated.shape[1]
    groups = ch // GROUP

    def copies(core):
        made = []

        def add(src, to):
            made.append(pltpu.make_async_copy(src, to, sems.at[len(made)]))

        base = place()[core]

        def tiles(src, lo, count, to, relative=False):
            for j in range(SIDE):
                at = src.at[pl.ds(j * SIDE, SIDE), pl.ds(lo, count)]
                far = jnp.bitwise_and(base + (OFFSETS[j] + SIDE), SIDE - 1) if relative else j
                add(at, to.at[far] if core == 0 else to.at[:, far])

        tiles(w_any, 0, GLU_TILES, w, True)
        add(wide_any, wide)
        add(taps, taps_v)
        add(ggain, ggain_v)
        add(head_out, head_v)
        first = len(made)
        for step, src, lo in ((0, own_any, OUT_AT), (3, up_any, 0), (1, down_any, 0)):
            tiles(src, lo, 2, wo.at[lax.rem(x + step, FS)])
        tiles(w_any, GLU_TILES, 2, wo.at[lax.rem(x + 2, FS)], True)
        return made, first

    pending, first = copies(0)

    def launch(span):
        for core in range(TP):

            @pl.when(c == core)
            def _(core=core):
                for copy in copies(core)[0][span]:
                    copy.start()

    launch(slice(0, first))
    for copy in pending[:first]:
        copy.wait()
    launch(slice(first, None))
    full = wide[...]

    def pair_of(ref, t):
        return jnp.concatenate([ref[:, :, t + i].reshape(-1, 128) for i in range(2)], axis=1)

    for g in range(groups):
        both = nn_dot(full, pair_of(w, 2 * g))
        value = both[:, :GROUP] * jax.nn.sigmoid(both[:, GROUP:])
        gated[:, g * GROUP : (g + 1) * GROUP] = value.astype(bf16).astype(f32)
    mixed = []
    count = taps_v.shape[0]
    lo = EDGE - count // 2
    for g in range(groups):
        lanes = slice(g * GROUP, (g + 1) * GROUP)
        tap = taps_v[:, lanes].astype(f32)
        total = None
        for r in range(8):
            reach = [s for s in range(lo, lo + count) if s % 8 == r]
            top = reach[-1] - r
            shifted = gated[r : r + top + rows, lanes]
            for s in reach:
                term = shifted[s - r : s - r + rows] * tap[s - lo : s - lo + 1, :]
                total = term if total is None else total + term
        centred = total - jnp.mean(total, axis=-1, keepdims=True)
        spread = jnp.mean(centred * centred, axis=-1, keepdims=True)
        unit = centred * lax.rsqrt(spread + norm_eps) * ggain_v[lanes].astype(f32)[None, :]
        mixed.append((unit * jax.nn.sigmoid(unit)).astype(bf16))
    mix = jnp.concatenate([head_v[...]] + mixed, axis=1)
    for copy in pending[first:]:
        copy.wait()
    part = SIDE // TP
    sent = []
    for i, (out, which) in enumerate(((other, jnp.bitwise_xor(c, 1)), (mine, c))):
        total = None
        for q in range(FS):
            wq = pair_of(wo.at[q, pl.ds(which * part, part)], 0)
            term = nt_dot(mix[:, q * QUART : (q + 1) * QUART], wq)
            total = term if total is None else total + term
        outs[i] = total.astype(bf16)
        sent.append(pltpu.make_async_copy(outs.at[i], out, sems.at[len(pending) + i]))
        sent[i].start()
    for copy in sent:
        copy.wait()


def on_device(
    tokens,
    norm_gain,
    query_down,
    query_gain,
    latent_down,
    latent_gain,
    rope_down,
    query_up,
    key_up,
    value_up,
    glu_value,
    glu_gate,
    conv_taps,
    group_gain,
    head_proj,
    channel_proj,
):
    tok = tokens.shape[0]
    vmem = pl.BlockSpec(memory_space=pltpu.VMEM)
    hbm = pl.BlockSpec(memory_space=pltpu.HBM)
    first, second = line_groups(0), line_groups(1)
    head_t, chan_t = head_proj.T, channel_proj.T

    quarter = ROPE // 4
    inverse = rope_base ** (-jnp.arange(quarter, dtype=f32) / quarter)
    inverse = jnp.tile(inverse, 4)[None]
    normed, sent = pl.pallas_call(
        pre_kernel,
        name="pre",
        out_shape=(
            jax.ShapeDtypeStruct(tokens.shape, bf16),
            jax.ShapeDtypeStruct((SIDE, KEY_TILES, ROW, 128), bf16),
        ),
        in_specs=[vmem] * 9,
        out_specs=(vmem, vmem),
        cost_estimate=pl.CostEstimate(flops=int(2e9), bytes_accessed=3 * 2**20, transcendentals=0),
    )(tokens, norm_gain, latent_down, latent_gain, rope_down.T, query_down, head_t, chan_t, inverse)
    own = lax.all_to_all(sent, MESH_AXES, 0, 0, axis_index_groups=first, tiled=True)

    spread = lax.all_gather(own, MESH_AXES, axis_index_groups=second, axis=0, tiled=True)

    value, gate, own = lax.optimization_barrier((glu_value, glu_gate, own))
    sent = pl.pallas_call(
        pack_kernel,
        name="pack",
        out_shape=jax.ShapeDtypeStruct((SIDE, WEIGHT_TILES, ROW, 128), bf16),
        in_specs=[vmem] * 4,
        out_specs=vmem,
    )(value, gate, head_t, chan_t)
    near = lax.all_to_all(sent, MESH_AXES, 0, 0, axis_index_groups=first, tiled=True)
    weights = spread_line(near)

    swap = [(0, 1), (1, 0)]
    theirs = lax.ppermute(spread, "tp", swap)
    fourth = spread[:, OUT_AT:]
    up = lax.ppermute(fourth, "fs", [(i, (i + 1) % FS) for i in range(FS)])
    down = lax.ppermute(fourth, "fs", [((i + 1) % FS, i) for i in range(FS)])

    heads = key_up.shape[1] // NOPE
    many = heads * tok
    total_keys = 2 * SIDE * SIDE * 64
    chunk = 1024
    attend = pl.pallas_call(
        attend_kernel,
        name="attend",
        out_shape=(
            jax.ShapeDtypeStruct((tok, heads * VDIM), bf16),
            jax.ShapeDtypeStruct((heads, tok), f32),
        ),
        in_specs=[vmem] * 8,
        out_specs=(vmem, vmem),
        scratch_shapes=[
            pltpu.VMEM((4, SIDE * SIDE, ROW, 128), bf16),
            pltpu.VMEM((tok, 512), f32),
            pltpu.VMEM((many, KVR + 128), bf16),
            pltpu.VMEM((total_keys, KVR + 128), bf16),
            pltpu.VMEM((many, chunk), f32),
            pltpu.VMEM((many, chunk), f32),
            pltpu.VMEM((many, chunk), bf16),
            pltpu.VMEM((many, 128), f32),
            pltpu.VMEM((many, 128), f32),
            pltpu.VMEM((many, KVR), f32),
        ],
        cost_estimate=pl.CostEstimate(flops=int(8e9), bytes_accessed=8 * 2**20, transcendentals=0),
    )
    head_out, log_weight = attend(normed, spread, theirs, query_gain, query_up, key_up, value_up, inverse)
    sp_count = lax.axis_size("sp")
    forward = [(i, i + 1) for i in range(sp_count - 1)]
    backward = [(i + 1, i) for i in range(sp_count - 1)]
    before = lax.ppermute(tokens[tok - EDGE :], "sp", forward)
    after = lax.ppermute(tokens[:EDGE], "sp", backward)
    wide = pl.pallas_call(
        edge_kernel,
        name="edge",
        out_shape=jax.ShapeDtypeStruct((tok + 2 * EDGE, tokens.shape[1]), bf16),
        in_specs=[vmem] * 4,
        out_specs=vmem,
    )(normed, before, after, norm_gain)

    ch = glu_value.shape[1]
    half_out = tokens.shape[1] // TP
    mine, other = pl.pallas_call(
        post_kernel,
        name="post",
        out_shape=(jax.ShapeDtypeStruct((tok, half_out), bf16),) * 2,
        in_specs=[hbm] * 8,
        out_specs=(hbm, hbm),
        scratch_shapes=[
            pltpu.VMEM((SIDE, SIDE, GLU_TILES, ROW, 128), bf16),
            pltpu.VMEM((FS, SIDE, SIDE, 2, ROW, 128), bf16),
            pltpu.VMEM((tok + 2 * EDGE, tokens.shape[1]), bf16),
            pltpu.VMEM(conv_taps.shape, bf16),
            pltpu.VMEM(group_gain.shape, bf16),
            pltpu.VMEM(head_out.shape, bf16),
            pltpu.VMEM((tok + 2 * EDGE, ch), f32),
            pltpu.VMEM((TP, tok, half_out), bf16),
            pltpu.SemaphoreType.DMA((64,)),
        ],
        cost_estimate=pl.CostEstimate(flops=int(3e9), bytes_accessed=9 * 2**20, transcendentals=0),
    )(
        weights, spread, up, down, wide, conv_taps, group_gain, head_out
    )
    arrived = lax.ppermute(other, "tp", swap)
    mixed_out = (mine.astype(f32) + arrived.astype(f32)).astype(bf16)
    return (mixed_out, log_weight)


def solution(mesh):
    in_specs = (
        P(("fs", "sp"), None),
        P(),
        P("sp", None),
        P(),
        P(),
        P(),
        P(),
        P(None, "tp"),
        P(None, "tp"),
        P(None, "tp"),
        P("sp", "tp"),
        P("sp", "tp"),
        P(None, "tp"),
        P("tp"),
        P("tp", "sp"),
        P("tp", "sp"),
    )
    out_specs = (P(("fs", "sp"), "tp"), P("tp", ("fs", "sp")))
    return jax.shard_map(
        on_device, mesh=mesh, in_specs=in_specs, out_specs=out_specs, check_vma=False
    )
```

```python
import jax
import jax.numpy as jnp
import numpy as np
from jax import lax
from jax.experimental import pallas as pl
from jax.experimental.pallas import tpu as pltpu
from jax.sharding import PartitionSpec as P

NOPE = 128
ROPE = 64
VDIM = 128
KVR = 256
GROUP = 128
GRID_W = 64
EDGE = 16
SIDE = 8
FS = 4
TP = 2
ROW = 32
QUERY_AT = 5
OUT_AT = 7
KEY_TILES = 9
GLU_TILES = 8
WEIGHT_TILES = 10
QUART = 256
MESH_AXES = ("sp", "fs", "tp")

norm_eps = 1e-06
rope_base = 10000.0
far_below = -1e30
LOG2E = 1.4426950408889634
LN2 = 0.6931471805599453

f32 = jnp.float32
bf16 = jnp.bfloat16


def flat(z, y, x, c):
    return ((z * SIDE + y) * FS + x) * TP + c


def line_groups(phase):
    groups = []
    for x in range(FS):
        for c in range(TP):
            for o in range(SIDE):
                if (c == 0) == (phase == 0):
                    groups.append([flat(o, i, x, c) for i in range(SIDE)])
                else:
                    groups.append([flat(i, o, x, c) for i in range(SIDE)])
    return groups


def nt_dot(a, b):
    return lax.dot_general(a, b, (((1,), (1,)), ((), ())), preferred_element_type=f32)


def nn_dot(a, b):
    return jnp.dot(a, b, preferred_element_type=f32)


def scaled(values, gain):
    inv = lax.rsqrt(jnp.mean(values * values, axis=-1, keepdims=True) + norm_eps)
    return values * inv * gain.astype(f32)[None, :]


def turned_half(raw):
    return jnp.concatenate([raw[:, ROPE // 2 :], raw[:, : ROPE // 2]], axis=1)


def turns(inverse, first, count):
    spot = first + lax.broadcasted_iota(jnp.int32, (count, ROPE), 0)
    lane = lax.broadcasted_iota(jnp.int32, (count, ROPE), 1)
    row = lax.shift_right_logical(spot, GRID_W.bit_length() - 1)
    col = jnp.bitwise_and(spot, GRID_W - 1)
    on_row = jnp.bitwise_and(lane, ROPE // 2 - 1) < ROPE // 4
    angles = jnp.where(on_row, row, col).astype(f32) * inverse[...]
    sine = jnp.sin(angles)
    return jnp.cos(angles), jnp.where(lane < ROPE // 2, -sine, sine)


def place():
    sp = lax.axis_index("sp")
    return lax.div(sp, SIDE), lax.rem(sp, SIDE), lax.axis_index("tp")


def quarter_of(head, chan, q, h):
    at = pl.ds(pl.multiple_of(lax.rem(q, 2) * QUART + h * 128, 128), 128)
    return jnp.where(q < 2, head[:, at], chan[:, at])


def pre_kernel(
    tok, gain, ldown, lgain, rdown, qdown, head, chan, inverse, normed, pack
):
    half = tok.shape[0] // TP
    c = place()[2]
    normed[...] = scaled(tok[...].astype(f32), gain[...]).astype(bf16)
    start = pl.multiple_of(c * half, half)
    own = normed[pl.ds(start, half), :]
    latent = scaled(nn_dot(own, ldown[...]), lgain[...]).astype(bf16)
    raw = nt_dot(own, rdown[...])
    first = lax.axis_index("sp") * tok.shape[0] + start
    cos2, sin2 = turns(inverse, first, half)
    key = raw * cos2 + turned_half(raw) * sin2
    pair = jnp.concatenate([key[: half // 2], key[half // 2 :]], axis=1).astype(bf16)
    x = lax.axis_index("fs")
    tiles = []
    for j in range(2):
        for i in range(2):
            tiles.append(latent[i * ROW : (i + 1) * ROW, j * 128 : (j + 1) * 128])
    tiles.append(pair)
    tiles += [qdown[:, pl.ds(pl.multiple_of(c * 256 + h * 128, 128), 128)] for h in range(2)]
    tiles += [quarter_of(head, chan, x, h) for h in range(2)]
    for i in range(SIDE):
        for t, tile in enumerate(tiles):
            pack[i, t] = tile


def pack_kernel(value, gate, head, chan, pack):
    far = lax.rem(lax.axis_index("fs") + 2, FS)
    tiles = []
    for g in range(value.shape[1] // GROUP):
        lanes = slice(g * GROUP, (g + 1) * GROUP)
        tiles += [value[:, lanes], gate[:, lanes]]
    tiles += [quarter_of(head, chan, far, h) for h in range(2)]
    for i in range(SIDE):
        for t, tile in enumerate(tiles):
            pack[i, t] = tile


def attend_kernel(
    normed, mine, theirs, qgain, qup, kup, vup, inverse, head_out, logw,
    weight, lat, queries, keys, sa, sb, p, top, low, acc
):
    c = place()[2]
    blocks = SIDE * SIDE
    for src, kind in ((mine, c), (theirs, jnp.bitwise_xor(c, 1))):
        for b in range(SIDE):
            for o in range(SIDE):
                block = jnp.where(kind == 0, b * SIDE + o, o * SIDE + b)
                for h in range(2):
                    weight[kind * 2 + h, block] = src[b * SIDE + o, QUERY_AT + h]
    x = normed[...]
    for g in range(4):
        lat[:, g * 128 : (g + 1) * 128] = nn_dot(x, weight[g].reshape(blocks * ROW, 128))
    latent = scaled(lat[...], qgain[...]).astype(bf16)
    every = nn_dot(latent, qup[...])
    heads = kup.shape[1] // NOPE
    rows = normed.shape[0]
    cos2, sin2 = turns(inverse, lax.axis_index("sp") * rows, rows)
    for h in range(heads):
        lo = h * (NOPE + ROPE)
        plain = every[:, lo : lo + NOPE].astype(bf16)
        raw = every[:, lo + NOPE : lo + NOPE + ROPE]
        rot = raw * cos2 + turned_half(raw) * sin2
        rot = jnp.concatenate([rot, jnp.zeros_like(rot)], axis=1).astype(bf16)
        absorbed = nt_dot(plain, kup[:, h * NOPE : (h + 1) * NOPE]).astype(bf16)
        queries[h * rows : (h + 1) * rows, :KVR] = absorbed
        queries[h * rows : (h + 1) * rows, KVR:] = rot

    per = SIDE * 64
    base = 0
    for src in (mine, theirs):
        count = src.shape[0] // SIDE

        def fill(i, carry, src=src, base=base):
            part = src[pl.ds(i * SIDE, SIDE)]
            to = pl.ds(pl.multiple_of((base + i) * per, per), per)
            keys[to, 0:128] = part[:, 0:2].reshape(per, 128)
            keys[to, 128:256] = part[:, 2:4].reshape(per, 128)
            near = part[:, 4].astype(f32)
            far = pltpu.roll(near.reshape(per // 2, 128), 64, 1).reshape(SIDE, 32, 128)
            both = jnp.concatenate([near, far], axis=1).reshape(per, 128)
            keys[to, 256:384] = both.astype(bf16)
            return carry

        lax.fori_loop(0, count, fill, 0)
        base += count
    top[...] = jnp.full_like(top, far_below)
    low[...] = jnp.zeros_like(low)
    acc[...] = jnp.zeros_like(acc)
    factor = LOG2E * (NOPE + ROPE) ** (-0.5)
    wide = sa.shape[1]
    steps = keys.shape[0] // wide
    total_rows = heads * rows

    def span(j):
        return pl.ds(pl.multiple_of(j * wide, wide), wide)

    def score(j, s):
        s[...] = nt_dot(queries[...], keys[span(j), :])

    def soften(j, s):
        fades = []
        for r in range(0, total_rows, 32):
            at = slice(r, r + 32)
            v = s[at, :]
            most = v[:, 0:128]
            for i in range(1, wide // 128):
                most = jnp.maximum(most, v[:, i * 128 : (i + 1) * 128])
            old = top[at, :]
            new = jnp.maximum(old, jnp.max(most, axis=1, keepdims=True))
            fade = jnp.exp2((old - new) * factor)
            part = low[at, :] * fade
            for i in range(wide // 128):
                e = jnp.exp2((v[:, i * 128 : (i + 1) * 128] - new) * factor)
                part = part + e
                p[at, i * 128 : (i + 1) * 128] = e.astype(bf16)
            low[at, :] = part
            top[at, :] = new
            acc[at, 0:128] = acc[at, 0:128] * fade
            acc[at, 128:256] = acc[at, 128:256] * fade
        acc[...] += nn_dot(p[...], keys[span(j), 0:KVR])

    score(0, sa)

    def pair(i, carry):
        score(2 * i + 1, sb)
        soften(2 * i, sa)
        score(jnp.minimum(2 * i + 2, steps - 1), sa)
        soften(2 * i + 1, sb)
        return carry

    lax.fori_loop(0, steps // 2, pair, 0)
    for h in range(heads):
        at = slice(h * rows, (h + 1) * rows)
        total = jnp.sum(low[at, :], axis=1, keepdims=True)
        attended = (acc[at, :] / total).astype(bf16)
        out = nn_dot(attended, vup[:, h * VDIM : (h + 1) * VDIM])
        head_out[:, h * VDIM : (h + 1) * VDIM] = out.astype(bf16)
        logs = top[at, :] * (factor * LN2) + jnp.log(total)
        logw[h : h + 1, :] = jnp.transpose(logs)[0:1, :]


def edge_kernel(normed, before, after, gain, wide):
    rows = normed.shape[0]
    wide[0:EDGE, :] = scaled(before[...].astype(f32), gain[...]).astype(bf16)
    wide[EDGE : EDGE + rows, :] = normed[...]
    wide[EDGE + rows :, :] = scaled(after[...].astype(f32), gain[...]).astype(bf16)


def out_copies(core, which, w_any, own_any, up_any, down_any, wo, sems):
    x = lax.axis_index("fs")
    part = SIDE // TP
    made = []
    sources = ((0, own_any, OUT_AT), (3, up_any, 0), (1, down_any, 0), (2, w_any, GLU_TILES))
    for step, src, lo in sources:
        to = wo.at[lax.rem(x + step, FS)]
        for j in range(part if core == 0 else SIDE):
            if core == 0:
                at, spot = pl.ds((which * part + j) * SIDE, SIDE), to.at[j]
            else:
                at, spot = pl.ds(j * SIDE + which * part, part), to.at[:, j]
            made.append(pltpu.make_async_copy(src.at[at, pl.ds(lo, 2)], spot, sems.at[len(made)]))
    return made


def on_core(c, made, act):
    for core in range(TP):

        @pl.when(c == core)
        def _(core=core):
            for copy in made(core):
                act(copy)


def pair_of(ref, t):
    return jnp.concatenate([ref[:, :, t + i].reshape(-1, 128) for i in range(2)], axis=1)


def project(mix, wo):
    total = None
    for q in range(FS):
        term = nt_dot(mix[:, q * QUART : (q + 1) * QUART], pair_of(wo.at[q], 0))
        total = term if total is None else total + term
    return total.astype(bf16)


def start(copy):
    copy.start()


def wait(copy):
    copy.wait()


def post_kernel(
    w_any, own_any, up_any, down_any, wide_any, taps, ggain, head_out,
    other, conv, w, wo, wide, taps_v, ggain_v, head_v, gated, sems, out_sems
):
    c = place()[2]
    rows = head_out.shape[0]
    ch = gated.shape[1]
    groups = ch // GROUP

    def inputs(core):
        made = []

        def add(src, to):
            made.append(pltpu.make_async_copy(src, to, sems.at[len(made)]))

        for j in range(SIDE):
            at = w_any.at[pl.ds(j * SIDE, SIDE), pl.ds(0, GLU_TILES)]
            add(at, w.at[j] if core == 0 else w.at[:, j])
        add(wide_any, wide)
        add(taps, taps_v)
        add(ggain, ggain_v)
        add(head_out, head_v)
        return made

    def outputs(core):
        which = jnp.bitwise_xor(c, 1)
        return out_copies(core, which, w_any, own_any, up_any, down_any, wo, out_sems)

    on_core(c, inputs, start)
    on_core(c, outputs, start)
    on_core(c, inputs, wait)
    full = wide[...]
    for g in range(groups):
        both = nn_dot(full, pair_of(w, 2 * g))
        value = both[:, :GROUP] * jax.nn.sigmoid(both[:, GROUP:])
        gated[:, g * GROUP : (g + 1) * GROUP] = value.astype(bf16).astype(f32)
    count = taps_v.shape[0]
    lo = EDGE - count // 2
    for g in range(groups):
        lanes = slice(g * GROUP, (g + 1) * GROUP)
        tap = taps_v[:, lanes].astype(f32)
        total = None
        for r in range(8):
            reach = [s for s in range(lo, lo + count) if s % 8 == r]
            top = reach[-1] - r
            shifted = gated[r : r + top + rows, lanes]
            for s in reach:
                term = shifted[s - r : s - r + rows] * tap[s - lo : s - lo + 1, :]
                total = term if total is None else total + term
        centred = total - jnp.mean(total, axis=-1, keepdims=True)
        spread = jnp.mean(centred * centred, axis=-1, keepdims=True)
        unit = centred * lax.rsqrt(spread + norm_eps) * ggain_v[lanes].astype(f32)[None, :]
        conv[:, lanes] = (unit * jax.nn.sigmoid(unit)).astype(bf16)
    mix = jnp.concatenate([head_v[...], conv[...]], axis=1)
    on_core(c, outputs, wait)
    other[...] = project(mix, wo)


def own_kernel(head_out, conv, w_any, own_any, up_any, down_any, mine, wo, out_sems):
    c = place()[2]

    def outputs(core):
        return out_copies(core, c, w_any, own_any, up_any, down_any, wo, out_sems)

    on_core(c, outputs, start)
    mix = jnp.concatenate([head_out[...], conv[...]], axis=1)
    on_core(c, outputs, wait)
    mine[...] = project(mix, wo)


def per_device(
    tokens,
    norm_gain,
    query_down,
    query_gain,
    latent_down,
    latent_gain,
    rope_down,
    query_up,
    key_up,
    value_up,
    glu_value,
    glu_gate,
    conv_taps,
    group_gain,
    head_proj,
    channel_proj,
):
    tok = tokens.shape[0]
    vmem = pl.BlockSpec(memory_space=pltpu.VMEM)
    hbm = pl.BlockSpec(memory_space=pltpu.HBM)
    first, second = line_groups(0), line_groups(1)
    head_t, chan_t = head_proj.T, channel_proj.T

    quarter = ROPE // 4
    powers = rope_base ** (-np.arange(quarter) / quarter)
    inverse = jnp.asarray(np.tile(powers, 4)[None], f32)
    normed, sent = pl.pallas_call(
        pre_kernel,
        name="pre",
        out_shape=(
            jax.ShapeDtypeStruct(tokens.shape, bf16),
            jax.ShapeDtypeStruct((SIDE, KEY_TILES, ROW, 128), bf16),
        ),
        in_specs=[vmem] * 9,
        out_specs=(vmem, vmem),
        cost_estimate=pl.CostEstimate(flops=int(2e9), bytes_accessed=3 * 2**20, transcendentals=0),
    )(tokens, norm_gain, latent_down, latent_gain, rope_down.T, query_down, head_t, chan_t, inverse)
    own = lax.all_to_all(sent, MESH_AXES, 0, 0, axis_index_groups=first, tiled=True)

    spread = lax.all_gather(own, MESH_AXES, axis_index_groups=second, axis=0, tiled=True)

    value, gate, own = lax.optimization_barrier((glu_value, glu_gate, own))
    sent = pl.pallas_call(
        pack_kernel,
        name="pack",
        out_shape=jax.ShapeDtypeStruct((SIDE, WEIGHT_TILES, ROW, 128), bf16),
        in_specs=[vmem] * 4,
        out_specs=vmem,
    )(value, gate, head_t, chan_t)
    near = lax.all_to_all(sent, MESH_AXES, 0, 0, axis_index_groups=first, tiled=True)
    weights = lax.all_gather(near, MESH_AXES, axis_index_groups=second, axis=0, tiled=True)

    swap = [(0, 1), (1, 0)]
    theirs = lax.ppermute(spread, "tp", swap)
    fourth = spread[:, OUT_AT:]
    up = lax.ppermute(fourth, "fs", [(i, (i + 1) % FS) for i in range(FS)])
    down = lax.ppermute(fourth, "fs", [((i + 1) % FS, i) for i in range(FS)])

    heads = key_up.shape[1] // NOPE
    many = heads * tok
    total_keys = 2 * SIDE * SIDE * 64
    chunk = 1024
    head_out, log_weight = pl.pallas_call(
        attend_kernel,
        name="attend",
        out_shape=(
            jax.ShapeDtypeStruct((tok, heads * VDIM), bf16),
            jax.ShapeDtypeStruct((heads, tok), f32),
        ),
        in_specs=[vmem] * 8,
        out_specs=(vmem, vmem),
        scratch_shapes=[
            pltpu.VMEM((4, SIDE * SIDE, ROW, 128), bf16),
            pltpu.VMEM((tok, 512), f32),
            pltpu.VMEM((many, KVR + 128), bf16),
            pltpu.VMEM((total_keys, KVR + 128), bf16),
            pltpu.VMEM((many, chunk), f32),
            pltpu.VMEM((many, chunk), f32),
            pltpu.VMEM((many, chunk), bf16),
            pltpu.VMEM((many, 128), f32),
            pltpu.VMEM((many, 128), f32),
            pltpu.VMEM((many, KVR), f32),
        ],
        cost_estimate=pl.CostEstimate(flops=int(8e9), bytes_accessed=8 * 2**20, transcendentals=0),
    )(normed, spread, theirs, query_gain, query_up, key_up, value_up, inverse)

    sp_count = lax.axis_size("sp")
    forward = [(i, i + 1) for i in range(sp_count - 1)]
    backward = [(i + 1, i) for i in range(sp_count - 1)]
    last, front, head_out = lax.optimization_barrier(
        (tokens[tok - EDGE :], tokens[:EDGE], head_out)
    )
    before = lax.ppermute(last, "sp", forward)
    after = lax.ppermute(front, "sp", backward)
    wide = pl.pallas_call(
        edge_kernel,
        name="edge",
        out_shape=jax.ShapeDtypeStruct((tok + 2 * EDGE, tokens.shape[1]), bf16),
        in_specs=[vmem] * 4,
        out_specs=vmem,
    )(normed, before, after, norm_gain)

    ch = glu_value.shape[1]
    half_out = tokens.shape[1] // TP
    halves = pltpu.VMEM((FS, SIDE // TP, SIDE, 2, ROW, 128), bf16)
    out_sems = pltpu.SemaphoreType.DMA((FS * SIDE,))
    half_shape = jax.ShapeDtypeStruct((tok, half_out), bf16)
    other, conv = pl.pallas_call(
        post_kernel,
        name="post",
        out_shape=(half_shape, jax.ShapeDtypeStruct((tok, ch), bf16)),
        in_specs=[hbm] * 8,
        out_specs=(vmem, vmem),
        scratch_shapes=[
            pltpu.VMEM((SIDE, SIDE, GLU_TILES, ROW, 128), bf16),
            halves,
            pltpu.VMEM((tok + 2 * EDGE, tokens.shape[1]), bf16),
            pltpu.VMEM(conv_taps.shape, bf16),
            pltpu.VMEM(group_gain.shape, bf16),
            pltpu.VMEM(head_out.shape, bf16),
            pltpu.VMEM((tok + 2 * EDGE, ch), f32),
            pltpu.SemaphoreType.DMA((16,)),
            out_sems,
        ],
        cost_estimate=pl.CostEstimate(flops=int(3e9), bytes_accessed=9 * 2**20, transcendentals=0),
    )(weights, spread, up, down, wide, conv_taps, group_gain, head_out)
    arrived = lax.ppermute(other, "tp", swap)
    mine = pl.pallas_call(
        own_kernel,
        name="own",
        out_shape=half_shape,
        in_specs=[vmem] * 2 + [hbm] * 4,
        out_specs=vmem,
        scratch_shapes=[halves, out_sems],
        cost_estimate=pl.CostEstimate(flops=int(3e8), bytes_accessed=2**21, transcendentals=0),
    )(head_out, conv, weights, spread, up, down)
    mixed_out = (mine.astype(f32) + arrived.astype(f32)).astype(bf16)
    return (mixed_out, log_weight)


def solution(mesh):
    in_specs = (
        P(("fs", "sp"), None),
        P(),
        P("sp", None),
        P(),
        P(),
        P(),
        P(),
        P(None, "tp"),
        P(None, "tp"),
        P(None, "tp"),
        P("sp", "tp"),
        P("sp", "tp"),
        P(None, "tp"),
        P("tp"),
        P("tp", "sp"),
        P("tp", "sp"),
    )
    out_specs = (P(("fs", "sp"), "tp"), P("tp", ("fs", "sp")))
    return jax.shard_map(
        per_device, mesh=mesh, in_specs=in_specs, out_specs=out_specs, check_vma=False
    )
```

```python
import jax
import jax.numpy as jnp
import numpy as np
from jax import lax
from jax.experimental import pallas as pl
from jax.experimental.pallas import tpu as pltpu
from jax.sharding import PartitionSpec as P

NOPE = 128
ROPE = 64
VDIM = 128
KVR = 256
GROUP = 128
GRID_W = 64
EDGE = 16
SIDE = 8
FS = 4
TP = 2
ROW = 32
QUERY_AT = 5
OUT_AT = 7
KEY_TILES = 9
GLU_TILES = 8
WEIGHT_TILES = 10
QUART = 256
MESH_AXES = ("sp", "fs", "tp")

norm_eps = 1e-06
rope_base = 10000.0
far_below = -1e30
LOG2E = 1.4426950408889634
LN2 = 0.6931471805599453

f32 = jnp.float32
bf16 = jnp.bfloat16


def flat(z, y, x, c):
    return ((z * SIDE + y) * FS + x) * TP + c


def line_groups(phase):
    groups = []
    for x in range(FS):
        for c in range(TP):
            for o in range(SIDE):
                if (c == 0) == (phase == 0):
                    groups.append([flat(o, i, x, c) for i in range(SIDE)])
                else:
                    groups.append([flat(i, o, x, c) for i in range(SIDE)])
    return groups


def nt_dot(a, b):
    return lax.dot_general(a, b, (((1,), (1,)), ((), ())), preferred_element_type=f32)


def nn_dot(a, b):
    return jnp.dot(a, b, preferred_element_type=f32)


def scaled(values, gain):
    inv = lax.rsqrt(jnp.mean(values * values, axis=-1, keepdims=True) + norm_eps)
    return values * inv * gain.astype(f32)[None, :]


def turned_half(raw):
    return jnp.concatenate([raw[:, ROPE // 2 :], raw[:, : ROPE // 2]], axis=1)


def turns(inverse, first, count):
    spot = first + lax.broadcasted_iota(jnp.int32, (count, ROPE), 0)
    lane = lax.broadcasted_iota(jnp.int32, (count, ROPE), 1)
    row = lax.shift_right_logical(spot, GRID_W.bit_length() - 1)
    col = jnp.bitwise_and(spot, GRID_W - 1)
    on_row = jnp.bitwise_and(lane, ROPE // 2 - 1) < ROPE // 4
    angles = jnp.where(on_row, row, col).astype(f32) * inverse[...]
    sine = jnp.sin(angles)
    return jnp.cos(angles), jnp.where(lane < ROPE // 2, -sine, sine)


def place():
    sp = lax.axis_index("sp")
    return lax.div(sp, SIDE), lax.rem(sp, SIDE), lax.axis_index("tp")


def quarter_of(head, chan, q, h):
    at = pl.ds(pl.multiple_of(lax.rem(q, 2) * QUART + h * 128, 128), 128)
    return jnp.where(q < 2, head[:, at], chan[:, at])


def pre_kernel(
    tok, gain, ldown, lgain, rdown, qdown, head, chan, inverse, normed, pack
):
    half = tok.shape[0] // TP
    c = place()[2]
    normed[...] = scaled(tok[...].astype(f32), gain[...]).astype(bf16)
    start = pl.multiple_of(c * half, half)
    own = normed[pl.ds(start, half), :]
    latent = scaled(nn_dot(own, ldown[...]), lgain[...]).astype(bf16)
    raw = nt_dot(own, rdown[...])
    first = lax.axis_index("sp") * tok.shape[0] + start
    cos2, sin2 = turns(inverse, first, half)
    key = raw * cos2 + turned_half(raw) * sin2
    pair = jnp.concatenate([key[: half // 2], key[half // 2 :]], axis=1).astype(bf16)
    x = lax.axis_index("fs")
    tiles = []
    for j in range(2):
        for i in range(2):
            tiles.append(latent[i * ROW : (i + 1) * ROW, j * 128 : (j + 1) * 128])
    tiles.append(pair)
    tiles += [qdown[:, pl.ds(pl.multiple_of(c * 256 + h * 128, 128), 128)] for h in range(2)]
    tiles += [quarter_of(head, chan, x, h) for h in range(2)]
    for i in range(SIDE):
        for t, tile in enumerate(tiles):
            pack[i, t] = tile


def pack_kernel(value, gate, head, chan, pack):
    far = lax.rem(lax.axis_index("fs") + 2, FS)
    tiles = []
    for g in range(value.shape[1] // GROUP):
        lanes = slice(g * GROUP, (g + 1) * GROUP)
        tiles += [value[:, lanes], gate[:, lanes]]
    tiles += [quarter_of(head, chan, far, h) for h in range(2)]
    for i in range(SIDE):
        for t, tile in enumerate(tiles):
            pack[i, t] = tile


def attend_kernel(
    normed, mine, theirs, qgain, qup, kup, vup, inverse, head_out, logw,
    weight, lat, queries, keys, sa, sb, p, top, low, acc
):
    c = place()[2]
    blocks = SIDE * SIDE
    for src, kind in ((mine, c), (theirs, jnp.bitwise_xor(c, 1))):
        for b in range(SIDE):
            for o in range(SIDE):
                block = jnp.where(kind == 0, b * SIDE + o, o * SIDE + b)
                for h in range(2):
                    weight[kind * 2 + h, block] = src[b * SIDE + o, QUERY_AT + h]
    x = normed[...]
    for g in range(4):
        lat[:, g * 128 : (g + 1) * 128] = nn_dot(x, weight[g].reshape(blocks * ROW, 128))
    latent = scaled(lat[...], qgain[...]).astype(bf16)
    every = nn_dot(latent, qup[...])
    heads = kup.shape[1] // NOPE
    rows = normed.shape[0]
    cos2, sin2 = turns(inverse, lax.axis_index("sp") * rows, rows)
    for h in range(heads):
        lo = h * (NOPE + ROPE)
        plain = every[:, lo : lo + NOPE].astype(bf16)
        raw = every[:, lo + NOPE : lo + NOPE + ROPE]
        rot = raw * cos2 + turned_half(raw) * sin2
        rot = jnp.concatenate([rot, jnp.zeros_like(rot)], axis=1).astype(bf16)
        absorbed = nt_dot(plain, kup[:, h * NOPE : (h + 1) * NOPE]).astype(bf16)
        queries[h * rows : (h + 1) * rows, :KVR] = absorbed
        queries[h * rows : (h + 1) * rows, KVR:] = rot

    per = SIDE * 64
    base = 0
    for src in (mine, theirs):
        count = src.shape[0] // SIDE

        def fill(i, carry, src=src, base=base):
            part = src[pl.ds(i * SIDE, SIDE)]
            to = pl.ds(pl.multiple_of((base + i) * per, per), per)
            keys[to, 0:128] = part[:, 0:2].reshape(per, 128)
            keys[to, 128:256] = part[:, 2:4].reshape(per, 128)
            near = part[:, 4].astype(f32)
            far = pltpu.roll(near.reshape(per // 2, 128), 64, 1).reshape(SIDE, 32, 128)
            both = jnp.concatenate([near, far], axis=1).reshape(per, 128)
            keys[to, 256:384] = both.astype(bf16)
            return carry

        lax.fori_loop(0, count, fill, 0)
        base += count
    top[...] = jnp.full_like(top, far_below)
    low[...] = jnp.zeros_like(low)
    acc[...] = jnp.zeros_like(acc)
    factor = LOG2E * (NOPE + ROPE) ** (-0.5)
    wide = sa.shape[1]
    steps = keys.shape[0] // wide
    total_rows = heads * rows

    def span(j):
        return pl.ds(pl.multiple_of(j * wide, wide), wide)

    def score(j, s):
        s[...] = nt_dot(queries[...], keys[span(j), :])

    def soften(j, s):
        fades = []
        for r in range(0, total_rows, 32):
            at = slice(r, r + 32)
            v = s[at, :]
            most = v[:, 0:128]
            for i in range(1, wide // 128):
                most = jnp.maximum(most, v[:, i * 128 : (i + 1) * 128])
            old = top[at, :]
            new = jnp.maximum(old, jnp.max(most, axis=1, keepdims=True))
            fade = jnp.exp2((old - new) * factor)
            part = low[at, :] * fade
            for i in range(wide // 128):
                e = jnp.exp2((v[:, i * 128 : (i + 1) * 128] - new) * factor)
                part = part + e
                p[at, i * 128 : (i + 1) * 128] = e.astype(bf16)
            low[at, :] = part
            top[at, :] = new
            acc[at, 0:128] = acc[at, 0:128] * fade
            acc[at, 128:256] = acc[at, 128:256] * fade
        acc[...] += nn_dot(p[...], keys[span(j), 0:KVR])

    score(0, sa)

    def pair(i, carry):
        score(2 * i + 1, sb)
        soften(2 * i, sa)
        score(jnp.minimum(2 * i + 2, steps - 1), sa)
        soften(2 * i + 1, sb)
        return carry

    lax.fori_loop(0, steps // 2, pair, 0)
    for h in range(heads):
        at = slice(h * rows, (h + 1) * rows)
        total = jnp.sum(low[at, :], axis=1, keepdims=True)
        attended = (acc[at, :] / total).astype(bf16)
        out = nn_dot(attended, vup[:, h * VDIM : (h + 1) * VDIM])
        head_out[:, h * VDIM : (h + 1) * VDIM] = out.astype(bf16)
        logs = top[at, :] * (factor * LN2) + jnp.log(total)
        logw[h : h + 1, :] = jnp.transpose(logs)[0:1, :]


def edge_kernel(normed, before, after, gain, wide):
    rows = normed.shape[0]
    wide[0:EDGE, :] = scaled(before[...].astype(f32), gain[...]).astype(bf16)
    wide[EDGE : EDGE + rows, :] = normed[...]
    wide[EDGE + rows :, :] = scaled(after[...].astype(f32), gain[...]).astype(bf16)


def post_kernel(
    w_any, own_any, up_any, down_any, wide_any, taps, ggain, head_out,
    mine, other, w, wo, wide, taps_v, ggain_v, head_v, gated, outs, sems
):
    c = place()[2]
    x = lax.axis_index("fs")
    rows = head_out.shape[0]
    ch = gated.shape[1]
    groups = ch // GROUP

    def copies(core):
        made = []

        def add(src, to):
            made.append(pltpu.make_async_copy(src, to, sems.at[len(made)]))

        def tiles(src, lo, count, to):
            for j in range(SIDE):
                at = src.at[pl.ds(j * SIDE, SIDE), pl.ds(lo, count)]
                add(at, to.at[j] if core == 0 else to.at[:, j])

        tiles(w_any, 0, GLU_TILES, w)
        add(wide_any, wide)
        add(taps, taps_v)
        add(ggain, ggain_v)
        add(head_out, head_v)
        first = len(made)
        for step, src, lo in ((0, own_any, OUT_AT), (3, up_any, 0), (1, down_any, 0)):
            tiles(src, lo, 2, wo.at[lax.rem(x + step, FS)])
        tiles(w_any, GLU_TILES, 2, wo.at[lax.rem(x + 2, FS)])
        return made, first

    pending, first = copies(0)

    def launch(span):
        for core in range(TP):

            @pl.when(c == core)
            def _(core=core):
                for copy in copies(core)[0][span]:
                    copy.start()

    launch(slice(0, first))
    for copy in pending[:first]:
        copy.wait()
    launch(slice(first, None))
    full = wide[...]

    def pair_of(ref, t):
        return jnp.concatenate([ref[:, :, t + i].reshape(-1, 128) for i in range(2)], axis=1)

    for g in range(groups):
        both = nn_dot(full, pair_of(w, 2 * g))
        value = both[:, :GROUP] * jax.nn.sigmoid(both[:, GROUP:])
        gated[:, g * GROUP : (g + 1) * GROUP] = value.astype(bf16).astype(f32)
    mixed = []
    count = taps_v.shape[0]
    lo = EDGE - count // 2
    for g in range(groups):
        lanes = slice(g * GROUP, (g + 1) * GROUP)
        tap = taps_v[:, lanes].astype(f32)
        total = None
        for r in range(8):
            reach = [s for s in range(lo, lo + count) if s % 8 == r]
            top = reach[-1] - r
            shifted = gated[r : r + top + rows, lanes]
            for s in reach:
                term = shifted[s - r : s - r + rows] * tap[s - lo : s - lo + 1, :]
                total = term if total is None else total + term
        centred = total - jnp.mean(total, axis=-1, keepdims=True)
        spread = jnp.mean(centred * centred, axis=-1, keepdims=True)
        unit = centred * lax.rsqrt(spread + norm_eps) * ggain_v[lanes].astype(f32)[None, :]
        mixed.append((unit * jax.nn.sigmoid(unit)).astype(bf16))
    mix = jnp.concatenate([head_v[...]] + mixed, axis=1)
    for copy in pending[first:]:
        copy.wait()
    part = SIDE // TP
    sent = []
    for i, (out, which) in enumerate(((other, jnp.bitwise_xor(c, 1)), (mine, c))):
        total = None
        for q in range(FS):
            wq = pair_of(wo.at[q, pl.ds(which * part, part)], 0)
            term = nt_dot(mix[:, q * QUART : (q + 1) * QUART], wq)
            total = term if total is None else total + term
        outs[i] = total.astype(bf16)
        sent.append(pltpu.make_async_copy(outs.at[i], out, sems.at[len(pending) + i]))
        sent[i].start()
    for copy in sent:
        copy.wait()


def per_device(
    tokens,
    norm_gain,
    query_down,
    query_gain,
    latent_down,
    latent_gain,
    rope_down,
    query_up,
    key_up,
    value_up,
    glu_value,
    glu_gate,
    conv_taps,
    group_gain,
    head_proj,
    channel_proj,
):
    tok = tokens.shape[0]
    vmem = pl.BlockSpec(memory_space=pltpu.VMEM)
    hbm = pl.BlockSpec(memory_space=pltpu.HBM)
    first, second = line_groups(0), line_groups(1)
    head_t, chan_t = head_proj.T, channel_proj.T

    quarter = ROPE // 4
    powers = rope_base ** (-np.arange(quarter) / quarter)
    inverse = jnp.asarray(np.tile(powers, 4)[None], f32)
    normed, sent = pl.pallas_call(
        pre_kernel,
        name="pre",
        out_shape=(
            jax.ShapeDtypeStruct(tokens.shape, bf16),
            jax.ShapeDtypeStruct((SIDE, KEY_TILES, ROW, 128), bf16),
        ),
        in_specs=[vmem] * 9,
        out_specs=(vmem, vmem),
        cost_estimate=pl.CostEstimate(flops=int(2e9), bytes_accessed=3 * 2**20, transcendentals=0),
    )(tokens, norm_gain, latent_down, latent_gain, rope_down.T, query_down, head_t, chan_t, inverse)
    own = lax.all_to_all(sent, MESH_AXES, 0, 0, axis_index_groups=first, tiled=True)

    spread = lax.all_gather(own, MESH_AXES, axis_index_groups=second, axis=0, tiled=True)

    value, gate, own = lax.optimization_barrier((glu_value, glu_gate, own))
    sent = pl.pallas_call(
        pack_kernel,
        name="pack",
        out_shape=jax.ShapeDtypeStruct((SIDE, WEIGHT_TILES, ROW, 128), bf16),
        in_specs=[vmem] * 4,
        out_specs=vmem,
    )(value, gate, head_t, chan_t)
    near = lax.all_to_all(sent, MESH_AXES, 0, 0, axis_index_groups=first, tiled=True)
    weights = lax.all_gather(near, MESH_AXES, axis_index_groups=second, axis=0, tiled=True)

    swap = [(0, 1), (1, 0)]
    theirs = lax.ppermute(spread, "tp", swap)
    fourth = spread[:, OUT_AT:]
    up = lax.ppermute(fourth, "fs", [(i, (i + 1) % FS) for i in range(FS)])
    down = lax.ppermute(fourth, "fs", [((i + 1) % FS, i) for i in range(FS)])

    heads = key_up.shape[1] // NOPE
    many = heads * tok
    total_keys = 2 * SIDE * SIDE * 64
    chunk = 1024
    head_out, log_weight = pl.pallas_call(
        attend_kernel,
        name="attend",
        out_shape=(
            jax.ShapeDtypeStruct((tok, heads * VDIM), bf16),
            jax.ShapeDtypeStruct((heads, tok), f32),
        ),
        in_specs=[vmem] * 8,
        out_specs=(vmem, vmem),
        scratch_shapes=[
            pltpu.VMEM((4, SIDE * SIDE, ROW, 128), bf16),
            pltpu.VMEM((tok, 512), f32),
            pltpu.VMEM((many, KVR + 128), bf16),
            pltpu.VMEM((total_keys, KVR + 128), bf16),
            pltpu.VMEM((many, chunk), f32),
            pltpu.VMEM((many, chunk), f32),
            pltpu.VMEM((many, chunk), bf16),
            pltpu.VMEM((many, 128), f32),
            pltpu.VMEM((many, 128), f32),
            pltpu.VMEM((many, KVR), f32),
        ],
        cost_estimate=pl.CostEstimate(flops=int(8e9), bytes_accessed=8 * 2**20, transcendentals=0),
    )(normed, spread, theirs, query_gain, query_up, key_up, value_up, inverse)

    sp_count = lax.axis_size("sp")
    forward = [(i, i + 1) for i in range(sp_count - 1)]
    backward = [(i + 1, i) for i in range(sp_count - 1)]
    last, front, head_out = lax.optimization_barrier(
        (tokens[tok - EDGE :], tokens[:EDGE], head_out)
    )
    before = lax.ppermute(last, "sp", forward)
    after = lax.ppermute(front, "sp", backward)
    wide = pl.pallas_call(
        edge_kernel,
        name="edge",
        out_shape=jax.ShapeDtypeStruct((tok + 2 * EDGE, tokens.shape[1]), bf16),
        in_specs=[vmem] * 4,
        out_specs=vmem,
    )(normed, before, after, norm_gain)

    ch = glu_value.shape[1]
    half_out = tokens.shape[1] // TP
    mine, other = pl.pallas_call(
        post_kernel,
        name="post",
        out_shape=(jax.ShapeDtypeStruct((tok, half_out), bf16),) * 2,
        in_specs=[hbm] * 8,
        out_specs=(hbm, hbm),
        scratch_shapes=[
            pltpu.VMEM((SIDE, SIDE, GLU_TILES, ROW, 128), bf16),
            pltpu.VMEM((FS, SIDE, SIDE, 2, ROW, 128), bf16),
            pltpu.VMEM((tok + 2 * EDGE, tokens.shape[1]), bf16),
            pltpu.VMEM(conv_taps.shape, bf16),
            pltpu.VMEM(group_gain.shape, bf16),
            pltpu.VMEM(head_out.shape, bf16),
            pltpu.VMEM((tok + 2 * EDGE, ch), f32),
            pltpu.VMEM((TP, tok, half_out), bf16),
            pltpu.SemaphoreType.DMA((64,)),
        ],
        cost_estimate=pl.CostEstimate(flops=int(3e9), bytes_accessed=9 * 2**20, transcendentals=0),
    )(
        weights, spread, up, down, wide, conv_taps, group_gain, head_out
    )
    arrived = lax.ppermute(other, "tp", swap)
    mixed_out = (mine.astype(f32) + arrived.astype(f32)).astype(bf16)
    return (mixed_out, log_weight)


def solution(mesh):
    in_specs = (
        P(("fs", "sp"), None),
        P(),
        P("sp", None),
        P(),
        P(),
        P(),
        P(),
        P(None, "tp"),
        P(None, "tp"),
        P(None, "tp"),
        P("sp", "tp"),
        P("sp", "tp"),
        P(None, "tp"),
        P("tp"),
        P("tp", "sp"),
        P("tp", "sp"),
    )
    out_specs = (P(("fs", "sp"), "tp"), P("tp", ("fs", "sp")))
    return jax.shard_map(
        per_device, mesh=mesh, in_specs=in_specs, out_specs=out_specs, check_vma=False
    )
```
